32 devices in a mesh: sp: 8 (over z, x), tp: 4 (over y, core).
Axes of the slice: x: 2, y: 2, z: 4, core: 2. Of those that a mesh axis runs over, the one named last changes fastest.
Arguments:
- residual_in: bfloat16 [1536, 2048], P('sp', 'tp'), may hold values from -6 to 6
- query_rows: bfloat16 [1536, 1024], P('sp', 'tp'), may hold values from -8 to 8
- key_rows: bfloat16 [1536, 1024], P('sp', 'tp'), may hold values from -8 to 8
- value_rows: bfloat16 [1536, 1024], P('sp', 'tp'), may hold values from -6 to 6
- map_weight: float32 [16], P('tp'), may hold values from 0.3 to 0.8
- head_gain: float32 [64], replicated, may hold values from 0.1 to 1.9
- out_proj: bfloat16 [1024, 2048], P(None, 'tp'), may hold values from -0.1875 to 0.1875
- norm_gain: float32 [2048], replicated, may hold values from 0.1 to 1.9
- route_ids: int32 [1536, 2], P('sp'), may hold values from 0 to 7, all different within a row; in each aligned block of 192 rows (0 to 191, 192 to 383, ...) at most 60 rows name the same one
- route_weights: float32 [1536, 2], P('sp'), may hold values from 0.2 to 1.2
- expert_gate: bfloat16 [8, 1024, 2048], P('sp', 'tp'), may hold values from -0.125 to 0.125
- expert_up: bfloat16 [8, 1024, 2048], P('sp', 'tp'), may hold values from -0.125 to 0.125
- expert_down: bfloat16 [8, 1024, 2048], P('sp', None, 'tp'), may hold values from -0.1875 to 0.1875
- shared_gate: bfloat16 [1024, 2048], P('tp'), may hold values from -0.125 to 0.125
- shared_up: bfloat16 [1024, 2048], P('tp'), may hold values from -0.125 to 0.125
- shared_down: bfloat16 [1024, 2048], P(None, 'tp'), may hold values from -0.1875 to 0.1875
Outputs:
- mixed_out: bfloat16 [1536, 2048], P('sp', 'tp')
The draws below stay inside these ranges and needn't reach their ends.
Inputs may be any that keep to these rules, and one draw needn't show every extreme that they name: `route_ids`: each row names 2 different experts. Among the rows held by one index of sp no expert is named more than 60 times, and in every draw some expert is named exactly 60 times by the rows of some index of sp.
All inputs are finite; a program needn't handle non-finite values.
Results may differ from the reference program's by a relative error of at most 0.0095.
Values may be sent and summed in bfloat16 or wider, within the bound.
A program may use at most 64 MiB of HBM per device.

```python
import math
from functools import partial
import jax
import jax.numpy as jnp
import numpy as np
from jax import lax

D = 2048
H = 16
HD = 64
FE = 1024
TOPK = 2
SEQ_DEV = 192
TOKENS = 1536
EXPERTS = 8
CAPACITY = 60
N_SP = 8


def query_key_pair(key):
    query_key = jax.random.fold_in(key, 11)
    second_key = jax.random.fold_in(key, 12)
    full_shape = (TOKENS, H * HD)
    queries = jnp.clip(jax.random.normal(query_key, full_shape, jnp.float32) * 1.3, -8.0, 8.0)
    key_vals = jnp.clip(jax.random.normal(second_key, full_shape, jnp.float32) * 1.3, -8.0, 8.0)
    return (queries, key_vals)


def draw_query_rows(key, part):
    return query_key_pair(key)[0].astype(jnp.bfloat16)


def draw_key_rows(key, part):
    return query_key_pair(key)[1].astype(jnp.bfloat16)


def block_scale(rng, extent, pieces, low, high):
    def one(dim, shards_of):
        heights = jax.random.uniform(jax.random.fold_in(jax.random.fold_in(rng, 6), dim), (shards_of,), jnp.float32, low / len(pieces), high / len(pieces))
        return jnp.repeat(jnp.exp(heights), extent[dim] // shards_of).reshape((-1,) + (1,) * (len(extent) - dim - 1))

    loudness = one(*pieces[0])
    for cut in pieces[1:]:
        loudness = loudness * one(*cut)
    return loudness


def deal_out(rng, own, number, rows, number_of, top, reach, slope):
    ranking = jax.random.permutation(rng, number_of)
    packed, usual = shares(number_of, rows * top, reach, slope, True), shares(number_of, rows * top, reach, slope, False)
    places = jnp.arange(number_of)

    def named(lengths, rotation):
        used = int((lengths > 0).sum())
        fixed = max(1, used // 4)
        passed = fixed + (places - fixed + rotation * (used - fixed)) % max(1, number_of - fixed)
        return jnp.zeros((number_of,), jnp.int32).at[ranking[jnp.where(places < fixed, places, passed)]].set(jnp.asarray(lengths, jnp.int32))

    lengths = jnp.where(number % 4 == 0, named(packed, number // 4), named(usual, number - number // 4 - 1))
    mixed = jax.random.permutation(jax.random.fold_in(own, 3), number_of)
    donor, receiver = mixed[0:number_of // 2 * 2:2], mixed[1:number_of // 2 * 2:2]
    slack = jnp.minimum(lengths[donor] - 1, reach - lengths[receiver]) // 2
    slack = jnp.where((donor == ranking[0]) | (receiver == ranking[0]) | (lengths[receiver] == 0), 0, jnp.maximum(slack, 0))
    passed = jax.random.randint(jax.random.fold_in(own, 4), (number_of // 2,), 0, 1 << 20) % (slack + 1)
    lengths = lengths.at[donor].add(-passed).at[receiver].add(passed)
    items = jnp.searchsorted(jnp.cumsum(lengths), jnp.arange(rows * top), side="right").astype(jnp.int32)
    listing = items.reshape(top, rows).T
    listing = listing[jax.random.permutation(jax.random.fold_in(own, 1), rows)]
    rotation = jax.random.randint(jax.random.fold_in(own, 2), (rows, 1), 0, top)
    return jnp.take_along_axis(listing, (jnp.arange(top)[None, :] + rotation) % top, axis=1)


def shares(amount, total, most, skew, full):
    loads = [(1 << 20) // math.isqrt(grade ** skew) + 1 for grade in range(1, amount + 1)]
    largest = most if full else min(most, max(-(-total // amount), total * loads[0] // sum(loads)))
    least = 1 if total - largest >= amount - 1 else 0
    given, rest = [largest] + [least] * (amount - 1), total - largest - least * (amount - 1)
    while rest > 0:
        movable = [i for i in range(1, amount) if given[i] < largest] or [i for i in range(1, amount) if given[i] < most]
        mass, remaining = sum([loads[i] for i in movable]), rest
        for i in movable:
            extra = min(most - given[i], max(1, remaining * loads[i] // mass), rest)
            given[i] = given[i] + extra
            rest = rest - extra
    return np.array(given)


def gaussian(rng, extent, spread, reach, cuts=(), kind=jnp.bfloat16):
    entries = spread * jax.random.normal(rng, extent, jnp.float32)
    if cuts:
        entries = entries * block_scale(rng, extent, cuts, -0.22, 0.18)
    return jnp.clip(entries, -reach, reach).astype(kind)


def setup_inputs(seed: int = 0) -> dict:
    seeds = jax.random.split(jax.random.key(seed), 17)
    residual_in = gaussian(seeds[0], (TOKENS, D), 1.0, 6.0, ((0, 8), (1, 4)))
    query_rows = draw_query_rows(jax.random.fold_in(seeds[16], 71), 0)
    key_rows = draw_key_rows(jax.random.fold_in(seeds[16], 71), 0)
    value_rows = gaussian(seeds[3], (TOKENS, H * HD), 1.0, 6.0, ((0, 8), (1, 4)))
    map_weight = jnp.clip(0.3 + 0.5 * jax.random.uniform(seeds[4], (H,), jnp.float32) ** block_scale(seeds[4], (H,), ((0, 4),), -0.2, 0.2), 0.3, 0.8)
    head_gain = jnp.clip(1.0 + 0.18 * jax.random.normal(seeds[5], (HD,), jnp.float32), 0.1, 1.9)
    out_proj = gaussian(seeds[6], (H * HD, D), (H * HD) ** -0.5, 0.1875, ((1, 4),))
    norm_gain = jnp.clip(1.0 + 0.18 * jax.random.normal(seeds[7], (D,), jnp.float32), 0.1, 1.9)
    route_ids_keys = jax.random.split(jax.random.fold_in(seeds[8], 1), TOKENS // SEQ_DEV)
    route_ids_turns = jax.random.permutation(jax.random.fold_in(seeds[8], 3), TOKENS // SEQ_DEV)
    route_ids = jax.vmap(lambda own, number: deal_out(jax.random.fold_in(seeds[8], 2), own, number, SEQ_DEV, EXPERTS, TOPK, CAPACITY, 2))(route_ids_keys, route_ids_turns).reshape((TOKENS, TOPK))
    route_weights = jnp.clip(0.2 + 1 * jax.random.uniform(seeds[9], (TOKENS, TOPK), jnp.float32) ** block_scale(seeds[9], (TOKENS, TOPK), ((0, 8),), -0.2, 0.2), 0.2, 1.2)
    expert_gate = gaussian(seeds[10], (EXPERTS, FE, D), D ** -0.5, 0.125, ((0, 8), (1, 4)))
    expert_up = gaussian(seeds[11], (EXPERTS, FE, D), D ** -0.5, 0.125, ((0, 8), (1, 4)))
    expert_down = gaussian(seeds[12], (EXPERTS, FE, D), FE ** -0.5, 0.1875, ((0, 8), (2, 4)))
    shared_gate = gaussian(seeds[13], (FE, D), D ** -0.5, 0.125, ((0, 4),))
    shared_up = gaussian(seeds[14], (FE, D), D ** -0.5, 0.125, ((0, 4),))
    shared_down = gaussian(seeds[15], (FE, D), FE ** -0.5, 0.1875, ((1, 4),))
    return {"residual_in": residual_in, "query_rows": query_rows, "key_rows": key_rows, "value_rows": value_rows, "map_weight": map_weight, "head_gain": head_gain, "out_proj": out_proj, "norm_gain": norm_gain, "route_ids": route_ids, "route_weights": route_weights, "expert_gate": expert_gate, "expert_up": expert_up, "expert_down": expert_down, "shared_gate": shared_gate, "shared_up": shared_up, "shared_down": shared_down}


epsilon = 1e-06
masked_score = -1e+30

def rms_scale(values, gain_vec):
    squares = lax.optimization_barrier(jnp.mean(values * values, axis=-1, keepdims=True))
    return values * lax.rsqrt(squares + epsilon) * gain_vec

def block_slots(route_block, experts_all, capacity):
    flat_ids = route_block.reshape(-1)
    one_hot = (flat_ids[:, None] == jnp.arange(experts_all, dtype=jnp.int32)[None, :]).astype(jnp.int32)
    earlier = jnp.cumsum(one_hot, axis=0) - one_hot
    position = lax.optimization_barrier(jnp.sum(earlier * one_hot, axis=1))
    return (flat_ids * capacity + position).astype(jnp.int32).reshape(route_block.shape)

def reference(residual_in, query_rows, key_rows, value_rows, map_weight, head_gain, out_proj, norm_gain, route_ids, route_weights, expert_gate, expert_up, expert_down, shared_gate, shared_up, shared_down):
    half_dim = HD // 2
    block_len = min(256, TOKENS)
    block_count = TOKENS // block_len
    key_heads = key_rows.reshape(TOKENS, H, 2, half_dim).astype(jnp.float32)
    value_heads = value_rows.reshape(TOKENS, H, HD).astype(jnp.float32)
    query_blocks = query_rows.reshape(block_count, block_len, H, 2, half_dim)
    key_pos = jnp.arange(TOKENS, dtype=jnp.int32)

    def attend(operands):
        query_block, block_index = operands
        query_pos = block_index * block_len + jnp.arange(block_len, dtype=jnp.int32)
        scores = jnp.einsum('qhmd,khmd->mhqk', query_block.astype(jnp.float32), key_heads) * half_dim ** (-0.5)
        visible = key_pos[None, :] <= query_pos[:, None]
        scores = jnp.where(visible, scores, masked_score)
        row_max = lax.optimization_barrier(jnp.max(scores, axis=-1, keepdims=True))
        expo = jnp.where(visible, jnp.exp(scores - row_max), 0.0)
        totals = lax.optimization_barrier(jnp.sum(expo, axis=-1))
        rounded = lax.optimization_barrier(expo.astype(jnp.bfloat16)).astype(jnp.float32)
        summed = jnp.einsum('mhqk,khd->mhqd', rounded, value_heads) / totals[..., None]
        return summed[0] - map_weight[:, None, None] * summed[1]
    parts = lax.map(attend, (query_blocks, jnp.arange(block_count, dtype=jnp.int32)))
    head_out = rms_scale(parts, head_gain).astype(jnp.bfloat16)
    head_out = jnp.transpose(head_out, (0, 2, 1, 3)).reshape(TOKENS, H * HD)
    attn = jnp.dot(head_out, out_proj, preferred_element_type=jnp.float32)
    hidden_state = (residual_in.astype(jnp.float32) + attn).astype(jnp.bfloat16)
    normed = rms_scale(hidden_state.astype(jnp.float32), norm_gain).astype(jnp.bfloat16)
    shared_hidden = (jax.nn.silu(jnp.dot(normed, shared_gate.T, preferred_element_type=jnp.float32)) * jnp.dot(normed, shared_up.T, preferred_element_type=jnp.float32)).astype(jnp.bfloat16)
    shared_out = jnp.dot(shared_hidden, shared_down, preferred_element_type=jnp.float32)
    slot_ids = jax.vmap(partial(block_slots, experts_all=EXPERTS, capacity=CAPACITY))(route_ids.reshape(N_SP, SEQ_DEV, TOPK))
    group_ids = jnp.broadcast_to(jnp.arange(N_SP, dtype=jnp.int32)[:, None, None], slot_ids.shape)
    token_ids = group_ids * SEQ_DEV + jnp.broadcast_to(jnp.arange(SEQ_DEV, dtype=jnp.int32)[None, :, None], slot_ids.shape)
    table = jnp.full((N_SP, EXPERTS * CAPACITY), TOKENS, jnp.int32).at[group_ids, slot_ids].set(token_ids)
    table = jnp.transpose(table.reshape(N_SP, EXPERTS, CAPACITY), (1, 0, 2))
    padded = jnp.concatenate([normed, jnp.zeros((1, D), jnp.bfloat16)], axis=0)

    def run_expert(operands):
        gate_w, up_w, down_w, rows_index = operands
        gathered = padded[rows_index.reshape(-1)]
        hidden_part = (jax.nn.silu(jnp.dot(gathered, gate_w.T, preferred_element_type=jnp.float32)) * jnp.dot(gathered, up_w.T, preferred_element_type=jnp.float32)).astype(jnp.bfloat16)
        return jnp.dot(hidden_part, down_w, preferred_element_type=jnp.float32).astype(jnp.bfloat16)
    results = lax.map(run_expert, (expert_gate, expert_up, expert_down, table))
    results = results.reshape(EXPERTS * N_SP * CAPACITY, D)
    expert_of = slot_ids // CAPACITY
    position = slot_ids % CAPACITY
    flat_index = ((expert_of * N_SP + group_ids) * CAPACITY + position).astype(jnp.int32).reshape(TOKENS, TOPK)
    picked = results[flat_index].astype(jnp.float32)
    routed = lax.optimization_barrier(jnp.sum(picked * route_weights[:, :, None], axis=1))
    return (hidden_state.astype(jnp.float32) + shared_out + routed).astype(jnp.bfloat16)
```

```python
import functools

import jax
import jax.numpy as jnp
from jax import lax
from jax.experimental import pallas as pl
from jax.experimental.pallas import tpu as pltpu
from jax.sharding import PartitionSpec as P

epsilon = 1e-06
masked_score = -1e30
MESH = pl.DeviceIdType.MESH


def rms_scale(values, gain_vec):
    squares = jnp.mean(values * values, axis=-1, keepdims=True)
    return values * lax.rsqrt(squares + epsilon) * gain_vec


def block_slots(route_block, experts_all, capacity):
    flat_ids = route_block.reshape(-1)
    one_hot = (flat_ids[:, None] == jnp.arange(experts_all, dtype=jnp.int32)[None, :]).astype(
        jnp.int32
    )
    earlier = jnp.cumsum(one_hot, axis=0) - one_hot
    position = jnp.sum(earlier * one_hot, axis=1)
    return (flat_ids * capacity + position).reshape(route_block.shape)


def body(
    residual_in,
    query_rows,
    key_rows,
    value_rows,
    map_weight,
    head_gain,
    out_proj,
    norm_gain,
    route_ids,
    route_weights,
    expert_gate,
    expert_up,
    expert_down,
    shared_gate,
    shared_up,
    shared_down,
):
    seq_dev = residual_in.shape[0]
    col_dev = residual_in.shape[1]
    heads_here = map_weight.shape[0]
    head_dim = head_gain.shape[0]
    half_dim = head_dim // 2
    topk_count = route_ids.shape[1]
    exp_here = expert_gate.shape[0]
    experts_all = exp_here * lax.axis_size("sp")
    capacity = 5 * seq_dev * topk_count // (4 * experts_all)
    score_scale = half_dim ** (-0.5)
    query_pos = lax.axis_index("sp") * seq_dev + jnp.arange(seq_dev, dtype=jnp.int32)
    query_heads = query_rows.reshape(seq_dev, heads_here, 2, half_dim)
    key_piece = lax.all_gather(key_rows, "sp", axis=0, tiled=True)
    value_piece = lax.all_gather(value_rows, "sp", axis=0, tiled=True)
    piece_len = key_piece.shape[0]
    key_heads = key_piece.reshape(piece_len, heads_here, 2, half_dim)
    value_heads = value_piece.reshape(piece_len, heads_here, head_dim)
    scores = (
        jnp.einsum("qhmd,khmd->mhqk", query_heads, key_heads, preferred_element_type=jnp.float32)
        * score_scale
    )
    key_pos = jnp.arange(piece_len, dtype=jnp.int32)
    visible = key_pos[None, :] <= query_pos[:, None]
    scores = jnp.where(visible, scores, masked_score)
    run_max = jnp.full((2, heads_here, seq_dev), masked_score, jnp.float32)
    new_max = jnp.maximum(run_max, jnp.max(scores, axis=-1))
    expo = jnp.where(visible, jnp.exp(scores - new_max[..., None]), 0.0)
    new_sum = jnp.sum(expo, axis=-1)
    product = jnp.einsum(
        "mhqk,khd->mhqd", expo.astype(jnp.bfloat16), value_heads, preferred_element_type=jnp.float32
    )
    summed = product / new_sum[..., None]
    diff_out = summed[0] - map_weight[:, None, None] * summed[1]
    head_out = rms_scale(diff_out, head_gain).astype(jnp.bfloat16)
    head_out = jnp.transpose(head_out, (1, 0, 2)).reshape(seq_dev, heads_here * head_dim)
    attn = jnp.dot(
        lax.all_gather(head_out, "tp", axis=1, tiled=True),
        out_proj,
        preferred_element_type=jnp.float32,
    )
    hidden_state = (residual_in.astype(jnp.float32) + attn).astype(jnp.bfloat16)
    full_rows = lax.all_gather(hidden_state, "tp", axis=1, tiled=True)
    normed = rms_scale(full_rows.astype(jnp.float32), norm_gain).astype(jnp.bfloat16)
    shared_gate_part = jnp.einsum(
        "rd,fd->rf", normed, shared_gate, preferred_element_type=jnp.float32
    )
    shared_up_part = jnp.einsum("rd,fd->rf", normed, shared_up, preferred_element_type=jnp.float32)
    shared_hidden = (jax.nn.silu(shared_gate_part) * shared_up_part).astype(jnp.bfloat16)
    slot_ids = block_slots(route_ids, experts_all, capacity)
    token_of = jnp.repeat(jnp.arange(seq_dev, dtype=jnp.int32), topk_count)
    slot_token = (
        jnp.full((experts_all * capacity,), seq_dev, jnp.int32)
        .at[slot_ids.reshape(-1)]
        .set(token_of)
    )
    own_cols = lax.dynamic_slice_in_dim(normed, lax.axis_index("tp") * col_dev, col_dev, 1)
    padded = jnp.concatenate([own_cols, jnp.zeros((1, col_dev), jnp.bfloat16)], axis=0)
    outgoing = jnp.take(padded, slot_token, axis=0).reshape(experts_all, capacity, col_dev)
    arrived = lax.all_to_all(outgoing, "sp", split_axis=0, concat_axis=1, tiled=True)
    arrived_rows = arrived.shape[1]
    pieces = lax.all_gather(arrived, "tp", axis=2, tiled=True)
    gate_add = jnp.einsum("erd,efd->erf", pieces, expert_gate, preferred_element_type=jnp.float32)
    up_add = jnp.einsum("erd,efd->erf", pieces, expert_up, preferred_element_type=jnp.float32)
    expert_hidden = (jax.nn.silu(gate_add) * up_add).astype(jnp.bfloat16)
    expert_flat = expert_hidden.reshape(exp_here * arrived_rows, expert_hidden.shape[2])
    pieces = (
        lax.all_gather(shared_hidden, "tp", axis=1, tiled=True),
        lax.all_gather(expert_flat, "tp", axis=1, tiled=True),
    )
    piece_width = pieces[0].shape[1]
    routed_piece = pieces[1].reshape(exp_here, arrived_rows, piece_width)
    shared_add = jnp.dot(pieces[0], shared_down, preferred_element_type=jnp.float32)
    expert_add = jnp.einsum(
        "erf,efd->erd", routed_piece, expert_down, preferred_element_type=jnp.float32
    )
    returned_rows = lax.all_to_all(
        expert_add.astype(jnp.bfloat16), "sp", split_axis=1, concat_axis=0, tiled=True
    )
    returned_flat = returned_rows.reshape(experts_all * capacity, col_dev)
    picked = (
        jnp.take(returned_flat, slot_ids.reshape(-1), axis=0)
        .reshape(seq_dev, topk_count, col_dev)
        .astype(jnp.float32)
    )
    routed = jnp.sum(picked * route_weights[:, :, None], axis=1)
    return (hidden_state.astype(jnp.float32) + shared_add + routed).astype(jnp.bfloat16)


def lane_iota(rows):
    return lax.broadcasted_iota(jnp.int32, (rows, 128), 1)


def roll_half(values):
    return pltpu.roll(values, 64, 1)


def contract_last(a, b):
    return lax.dot_general(a, b, (((1,), (1,)), ((), ())), preferred_element_type=jnp.float32)


def layer_kernel(
    n_sp,
    n_tp,
    q_in,
    k_in,
    v_in,
    res_in,
    map_w,
    head_g,
    norm_g,
    ids_in,
    route_w,
    out_proj,
    exp_gate,
    exp_up,
    exp_down,
    sh_gate,
    sh_up,
    sh_down,
    out_ref,
    w_out,
    w_gate,
    w_up,
    w_down,
    w_sgate,
    w_sup,
    w_sdown,
    kv_out,
    q_out,
    kv_buf,
    q_buf,
    o_out,
    ho_buf,
    hid_buf,
    disp_out,
    arr_buf,
    sh_buf,
    eh_buf,
    res_out,
    ret_buf,
    spread_buf,
    pick_buf,
    weight_buf,
    w_sem,
    a_send,
    kv_recv,
    q_recv,
    o_send,
    o_recv,
    d_send,
    d_recv,
    r_send,
    r_recv,
    g_send,
    g_recv,
    peer_out,
    p_send,
    p_recv,
    shared_sum,
):
    me_s = lax.axis_index("sp")
    me_t = lax.axis_index("tp")
    sib = me_t + 1 - 2 * lax.rem(me_t, 2)
    peers = n_tp // 2 - 1
    rows = res_in.shape[0]
    col_dev = res_in.shape[1]
    half = rows // 2
    quarter = rows // 4
    cap = arr_buf.shape[2]
    half_dim = 32
    piece_far = 3 + 2 * n_sp
    bf16 = jnp.bfloat16
    f32 = jnp.float32

    def across(k):
        other = me_s
        for b in range(n_sp.bit_length() - 1):
            if k >> b & 1:
                bit = lax.rem(me_s // (1 << b), 2)
                other = other + (1 << b) * (1 - 2 * bit)
        return other

    loads = []
    for i, (src, dst) in enumerate(
        (
            (out_proj, w_out),
            (sh_gate, w_sgate),
            (sh_up, w_sup),
            (exp_gate.at[0], w_gate),
            (exp_up.at[0], w_up),
            (exp_down.at[0], w_down),
            (sh_down, w_sdown),
        )
    ):
        copy = pltpu.make_async_copy(src, dst, w_sem.at[i])
        copy.start()
        loads.append(copy)

    barrier = pltpu.get_barrier_semaphore()
    for d in range(1, n_sp):
        pl.semaphore_signal(
            barrier, inc=1, device_id={"sp": lax.rem(me_s + d, n_sp)}, device_id_type=MESH
        )
    for d in range(1, n_tp):
        pl.semaphore_signal(
            barrier, inc=1, device_id={"tp": lax.rem(me_t + d, n_tp)}, device_id_type=MESH
        )

    sends = []

    def send(src, dst, ssem, rsem, device):
        copy = pltpu.make_async_remote_copy(
            src_ref=src,
            dst_ref=dst,
            send_sem=ssem,
            recv_sem=rsem,
            device_id=device,
            device_id_type=MESH,
        )
        copy.start()
        return copy

    def wait_recv(ref, ssem, rsem, device):
        pltpu.make_async_remote_copy(
            src_ref=ref,
            dst_ref=ref,
            send_sem=ssem,
            recv_sem=rsem,
            device_id=device,
            device_id_type=MESH,
        ).wait_recv()

    n_gs = 1 + 2 * peers

    def gather_start(piece, get):
        for k in range(1, peers + 1):
            other = lax.rem(me_t + 2 * k, n_tp)
            sends.append(
                send(
                    get(me_t),
                    get(me_t),
                    g_send.at[piece * n_gs + k],
                    g_recv.at[piece * n_tp + me_t],
                    {"tp": other},
                )
            )
        sends.append(
            send(
                get(me_t),
                get(me_t),
                g_send.at[piece * n_gs],
                g_recv.at[piece * n_tp + me_t],
                {"tp": sib},
            )
        )

    def gather_relay(piece, get):
        for k in range(1, peers + 1):
            other = lax.rem(me_t + 2 * k, n_tp)
            wait_recv(
                get(other), g_send.at[piece * n_gs], g_recv.at[piece * n_tp + other], {"tp": sib}
            )
            sends.append(
                send(
                    get(other),
                    get(other),
                    g_send.at[piece * n_gs + peers + k],
                    g_recv.at[piece * n_tp + other],
                    {"tp": sib},
                )
            )

    def gather_finish(piece, get):
        for k in range(peers + 1):
            other = lax.rem(sib + 2 * k, n_tp)
            wait_recv(
                get(other), g_send.at[piece * n_gs], g_recv.at[piece * n_tp + other], {"tp": sib}
            )

    low_rows = lane_iota(rows) < 64
    low_quarter = lane_iota(quarter) < 64
    for j in range(n_sp // 4):
        pair = slice(j * 128, (j + 1) * 128)
        keys = k_in[:, pair].astype(f32)
        vals = v_in[:, pair].astype(f32)
        kv_out[2 * j] = jnp.where(low_rows, keys, roll_half(vals)).astype(bf16)
        kv_out[2 * j + 1] = jnp.where(low_rows, roll_half(keys), vals).astype(bf16)
        for p in range(2):
            first = q_in[p * half : p * half + quarter, pair].astype(f32)
            second = q_in[p * half + quarter : (p + 1) * half, pair].astype(f32)
            q_out[4 * j + p] = jnp.where(low_quarter, first, roll_half(second)).astype(bf16)
            q_out[4 * j + 2 + p] = jnp.where(low_quarter, roll_half(first), second).astype(bf16)

    pl.semaphore_wait(barrier, n_sp + n_tp - 2)

    for d in (6, 7, 4, 5, 2, 3, 1):
        dst = across(d)
        if d % 2 == 0 or d == 1:
            sends.append(
                send(
                    kv_out.at[dst // 2],
                    kv_buf.at[me_s],
                    a_send.at[2 * d],
                    kv_recv.at[me_s],
                    {"sp": dst},
                )
            )
    for d in (6, 7, 4, 5, 2, 3, 1):
        dst = across(d)
        sends.append(
            send(
                q_out.at[dst], q_buf.at[me_s], a_send.at[2 * d + 1], q_recv.at[me_s], {"sp": dst}
            )
        )
    kv_buf[me_s] = kv_out[me_s // 2]
    q_buf[me_s] = q_out[me_s]

    eye = lax.broadcasted_iota(jnp.int32, (rows, rows), 0)
    eye_lane = lax.broadcasted_iota(jnp.int32, (rows, rows), 1)
    same = eye == eye_lane
    before_col = eye_lane < eye
    before_row = eye < eye_lane

    def as_column(row):
        return jnp.sum(jnp.where(same, row, 0.0), axis=1, keepdims=True)

    ids_row = [jnp.bitwise_xor(ids_in[c : c + 1, :], me_s).astype(f32) for c in range(2)]
    ids_col = [as_column(row) for row in ids_row]
    weight_col = [as_column(route_w[c : c + 1, :]) for c in range(2)]
    slot_row = []
    slot_col = []
    for c in range(2):
        hit = (ids_row[0] == ids_col[c]) | (ids_row[1] == ids_col[c])
        count = jnp.sum(jnp.where(hit & before_col, 1.0, 0.0), axis=1, keepdims=True)
        slot_col.append(ids_col[c] * cap + count)
        hit = (ids_col[0] == ids_row[c]) | (ids_col[1] == ids_row[c])
        count = jnp.sum(jnp.where(hit & before_row, 1.0, 0.0), axis=0, keepdims=True)
        slot_row.append(ids_row[c] * cap + count)
    slots = n_sp * cap
    slot_iota = lax.broadcasted_iota(jnp.int32, (slots, rows), 0).astype(f32)
    chosen = (slot_iota == slot_row[0]) | (slot_iota == slot_row[1])
    spread_buf[...] = jnp.where(chosen, 1.0, 0.0).astype(bf16)
    col_iota = lax.broadcasted_iota(jnp.int32, (rows, slots), 1).astype(f32)
    for c in range(2):
        pick_buf[c] = jnp.where(col_iota == slot_col[c], 1.0, 0.0).astype(bf16)
        weight_buf[c] = jnp.broadcast_to(weight_col[c], (rows, 128))
    head_lane = lax.broadcasted_iota(jnp.int32, map_w.shape, 1)
    map_here = jnp.sum(
        jnp.where(head_lane == me_s // 2, map_w[...], 0.0), axis=1, keepdims=True
    )
    gain_here = jnp.concatenate([jnp.zeros((1, 64), f32), head_g[...]], axis=1)

    parity = lax.rem(me_s, 2)
    lane_q = lane_iota(quarter)
    scale = half_dim ** (-0.5)
    row_in = lax.broadcasted_iota(jnp.int32, (half, rows), 0) + parity * half
    visible_half = lax.broadcasted_iota(jnp.int32, (half, rows), 1) <= row_in
    visible = jnp.concatenate([visible_half.astype(f32)] * 2, axis=0) > 0.5
    high_lanes = lane_iota(half) >= 64
    zero_q = jnp.zeros((quarter, 128), f32)
    first_map = lane_q < 32
    second_map = (lane_q >= 32) & (lane_q < 64)
    batch = n_sp // 2
    for d in (6, 4, 2):
        src = across(d)
        wait_recv(kv_buf.at[src], a_send.at[0], kv_recv.at[src], {"sp": src})
        sends.append(
            send(
                kv_buf.at[src],
                kv_buf.at[src],
                a_send.at[2 * d + 2],
                kv_recv.at[src],
                {"sp": across(1)},
            )
        )
    for s in range(n_sp):

        @pl.when(parity != s % 2)
        def _():
            wait_recv(kv_buf.at[s], a_send.at[0], kv_recv.at[s], {"sp": across(1)})

        @pl.when(me_s != s)
        def _():
            wait_recv(q_buf.at[s], a_send.at[1], q_recv.at[s], {"sp": s})

    def attend(start):
        steps = range(start, start + batch)
        queries = {}
        for s in steps:
            packed = q_buf[s].astype(f32)
            rolled = roll_half(packed)
            queries[s] = jnp.concatenate(
                [
                    jnp.where(first_map, packed, zero_q),
                    jnp.where(first_map, rolled, zero_q),
                    jnp.where(second_map, packed, zero_q),
                    jnp.where(second_map, rolled, zero_q),
                ],
                axis=0,
            ).astype(bf16)
        keys = {s: kv_buf[0 : s + 1].reshape((s + 1) * rows, 128) for s in steps}
        scores = {}
        for s in steps:
            raw = contract_last(queries[s], keys[s]) * scale
            diag = jnp.where(visible, raw[:, s * rows :], masked_score)
            scores[s] = jnp.concatenate([raw[:, : s * rows], diag], axis=1) if s else diag
        row_max = {s: jnp.max(scores[s], axis=1, keepdims=True) for s in steps}
        expo = {s: jnp.exp(scores[s] - row_max[s]) for s in steps}
        total = {s: jnp.sum(expo[s], axis=1, keepdims=True) for s in steps}
        acc = {
            s: jnp.dot(expo[s].astype(bf16), keys[s], preferred_element_type=f32) for s in steps
        }
        diff = {}
        for s in steps:
            summed = acc[s] / total[s]
            raw = summed[0:half] - map_here * summed[half:rows]
            diff[s] = jnp.where(high_lanes, raw, 0.0)
        for s in steps:
            squares = jnp.sum(diff[s] * diff[s], axis=1, keepdims=True) * (1.0 / 64.0)
            head = diff[s] * lax.rsqrt(squares + epsilon) * gain_here
            o_out[s] = (roll_half(head[0:quarter]) + head[quarter:half]).astype(bf16)

        for s in steps:

            @pl.when(me_s != s)
            def _():
                send(
                    o_out.at[s],
                    ho_buf.at[me_t, me_s],
                    o_send.at[s],
                    o_recv.at[me_s],
                    {"sp": s},
                )

            @pl.when(me_s == s)
            def _():
                ho_buf[me_t, s] = o_out[s]

    upper = me_s // batch

    @pl.when(upper == 1)
    def _():
        attend(0)
        attend(batch)

    @pl.when(upper == 0)
    def _():
        attend(batch)
        attend(0)

    split = n_sp // 2
    base = me_s // split * split

    def get_near(t):
        return ho_buf.at[t, pl.ds(base, split)]

    def get_far(t):
        return ho_buf.at[t, pl.ds(split - base, split)]

    for d in (4, 5, 6, 7, 1, 2, 3):
        other = across(d)
        wait_recv(ho_buf.at[me_t, other], o_send.at[d], o_recv.at[other], {"sp": other})
        if d == n_sp - 1:
            gather_start(piece_far, get_far)
    gather_start(0, get_near)
    for piece, get in ((piece_far, get_far), (0, get_near)):
        gather_relay(piece, get)
    for piece, get in ((piece_far, get_far), (0, get_near)):
        gather_finish(piece, get)

    blocks = []
    for p in range(2):
        for u in range(2):
            parts = []
            for t in range(n_tp):
                for j in range(n_sp // 4):
                    even = ho_buf[t, 4 * j + p].astype(f32)
                    odd = ho_buf[t, 4 * j + 2 + p].astype(f32)
                    if u == 0:
                        part = jnp.where(low_quarter, even, roll_half(odd))
                    else:
                        part = jnp.where(low_quarter, roll_half(even), odd)
                    parts.append(part.astype(bf16))
            blocks.append(jnp.concatenate(parts, axis=1))
    heads = jnp.concatenate(blocks, axis=0)
    loads[0].wait()
    attn = jnp.dot(heads, w_out[...], preferred_element_type=f32)
    hidden = (res_in[...].astype(f32) + attn).astype(bf16)
    hid_buf[me_t] = hidden

    def get_hid(t):
        return hid_buf.at[t]

    gather_start(1, get_hid)

    near = n_sp // 2

    def spread(lo, hi, cols):
        picked = jnp.dot(spread_buf[lo * cap : hi * cap], cols, preferred_element_type=f32)
        return picked.astype(bf16).reshape(hi - lo, cap, col_dev)

    inner = lax.rem(me_s // 2 + upper, 2)

    def slot_at(d):
        return d if d < near else near + 2 * inner + 1 - d % 2

    def offset_of(e):
        if e < near:
            return e
        return (6 - 2 * inner if e < 6 else 4 + 2 * inner) + 1 - e % 2

    def source(e):
        if e < near:
            return across(e)
        side = me_s % 2 if e % 2 else 1 - me_s % 2
        return 2 * (3 * (1 - upper) if e < 6 else 2 - upper) + side

    def dispatch(d):
        e = slot_at(d)
        sends.append(
            send(
                disp_out.at[d], arr_buf.at[me_t, e], d_send.at[d], d_recv.at[e], {"sp": across(d)}
            )
        )

    def dispatch_peer(d, k):
        other = lax.rem(me_t + 2 * k, n_tp)
        i = (k - 1) * near + d
        return send(
            peer_out.at[i], arr_buf.at[other, d], p_send.at[i], p_recv.at[i], {"sp": across(d)}
        )

    def get_arr(d):
        return lambda t: arr_buf.at[t, d]

    def normalise(pieces):
        full = [piece.astype(f32) for piece in pieces]
        squares = sum(jnp.sum(piece * piece, axis=1, keepdims=True) for piece in full)
        factor = lax.rsqrt(squares * (1.0 / (n_tp * col_dev)) + epsilon)
        return jnp.concatenate(
            [
                (piece * factor * norm_g[:, t * col_dev : (t + 1) * col_dev]).astype(bf16)
                for t, piece in enumerate(full)
            ],
            axis=1,
        )

    def gated(normed, gate, up):
        gate_part = contract_last(normed, gate[...])
        up_part = contract_last(normed, up[...])
        return (gate_part / (1.0 + jnp.exp(-gate_part)) * up_part).astype(bf16)

    def arrive(d):
        wait_recv(arr_buf.at[me_t, d], d_send.at[d], d_recv.at[d], {"sp": source(d)})
        gather_start(2 + d, get_arr(d))

    def relay(d):
        gather_relay(2 + d, get_arr(d))

    def arrive_near(d):
        piece = 2 + d
        get = get_arr(d)
        wait_recv(get(me_t), d_send.at[d], d_recv.at[d], {"sp": across(d)})
        sends.append(
            send(
                get(me_t),
                get(me_t),
                g_send.at[piece * n_gs],
                g_recv.at[piece * n_tp + me_t],
                {"tp": sib},
            )
        )

    def arrive_peer(d):
        piece = 2 + d
        get = get_arr(d)
        for k in range(1, peers + 1):
            other = lax.rem(me_t + 2 * k, n_tp)
            i = (k - 1) * near + d
            wait_recv(get(other), p_send.at[i], p_recv.at[i], {"sp": across(d)})
            sends.append(
                send(
                    get(other),
                    get(other),
                    g_send.at[piece * n_gs + peers + k],
                    g_recv.at[piece * n_tp + other],
                    {"tp": sib},
                )
            )

    def get_sh(t):
        return sh_buf.at[t]

    def get_eh(lo, hi):
        return lambda t: eh_buf.at[t, pl.ds(lo, hi - lo)]

    piece_sh = 2 + n_sp
    piece_eh = 3 + n_sp

    def expert_up(lo, hi):
        for d in range(lo, hi):
            if d:
                gather_finish(2 + d, get_arr(d))
        count = (hi - lo) * cap
        normed = normalise([arr_buf[t, lo:hi].reshape(count, col_dev) for t in range(n_tp)])
        hidden_units = gated(normed, w_gate, w_up)
        eh_buf[me_t, lo:hi] = hidden_units.reshape(hi - lo, cap, hidden_units.shape[1])

    def start_eh(lo, hi):
        gather_start(piece_eh + lo, get_eh(lo, hi))

    def relay_eh(lo, hi):
        gather_relay(piece_eh + lo, get_eh(lo, hi))

    def expert_out(lo, hi):
        gather_finish(piece_eh + lo, get_eh(lo, hi))
        count = (hi - lo) * cap
        joined = jnp.concatenate(
            [eh_buf[t, lo:hi].reshape(count, eh_buf.shape[3]) for t in range(n_tp)], axis=1
        )
        result = jnp.dot(joined, w_down[...], preferred_element_type=f32).astype(bf16)
        res_out[lo:hi] = result.reshape(hi - lo, cap, col_dev)
        for d in range(lo, hi):
            if d == 0:
                ret_buf[0] = res_out[0]
            else:
                sends.append(
                    send(
                        res_out.at[d],
                        ret_buf.at[offset_of(d)],
                        r_send.at[d],
                        r_recv.at[offset_of(d)],
                        {"sp": source(d)},
                    )
                )

    def shared_up():
        normed_own = normalise([hid_buf[t] for t in range(n_tp)])
        sh_buf[me_t] = gated(normed_own, w_sgate, w_sup)

    def shared_down():
        shared_all = jnp.concatenate([sh_buf[t] for t in range(n_tp)], axis=1)
        shared_sum[...] = hid_buf[me_t].astype(f32) + jnp.dot(
            shared_all, w_sdown[...], preferred_element_type=f32
        )

    def own_rows():
        for t in range(n_tp):
            arr_buf[t, 0] = jnp.dot(
                spread_buf[0:cap], hid_buf[t], preferred_element_type=f32
            ).astype(bf16)

    def wait_loads():
        for copy in loads[1:]:
            copy.wait()

    def send_own():
        disp_out[near:n_sp] = spread(near, n_sp, hidden)
        for d in (4, 6, 5, 7):
            dispatch(d)
        disp_out[1:near] = spread(1, near, hidden)
        for d in range(1, near):
            dispatch(d)

    def peer_cols():
        for k in range(1, peers + 1):
            other = lax.rem(me_t + 2 * k, n_tp)
            peer_out[(k - 1) * near + 1 : k * near] = spread(1, near, hid_buf[other])
            for d in range(1, near):
                sends.append(dispatch_peer(d, k))

    send_own()
    arrive(5)
    gather_relay(1, get_hid)
    peer_cols()
    gather_finish(1, get_hid)
    arrive(4)
    relay(5)
    wait_loads()
    shared_up()
    expert_up(5, 6)
    start_eh(5, 6)
    relay(4)
    own_rows()
    arrive(7)
    arrive_near(1)
    arrive_peer(1)
    expert_up(4, 5)
    start_eh(4, 5)
    relay_eh(5, 6)
    arrive(6)
    gather_start(piece_sh, get_sh)
    relay(7)
    expert_up(0, 2)
    expert_out(5, 6)
    expert_up(7, 8)
    start_eh(7, 8)
    relay_eh(4, 5)
    arrive_near(2)
    arrive_near(3)
    arrive_peer(2)
    arrive_peer(3)
    relay(6)
    expert_out(4, 5)
    start_eh(0, 2)
    expert_up(6, 7)
    start_eh(6, 7)
    relay_eh(7, 8)
    expert_up(2, 4)
    start_eh(2, 4)
    expert_out(7, 8)
    relay_eh(0, 2)
    gather_relay(piece_sh, get_sh)
    relay_eh(6, 7)
    expert_out(0, 2)
    expert_out(6, 7)
    relay_eh(2, 4)
    gather_finish(piece_sh, get_sh)
    shared_down()
    expert_out(2, 4)
    result = shared_sum[...]
    for d in range(1, n_sp):
        wait_recv(ret_buf.at[d], r_send.at[d], r_recv.at[d], {"sp": across(d)})
    returned = ret_buf[...].reshape(slots, col_dev)
    for c in range(2):
        picked = jnp.dot(pick_buf[c], returned, preferred_element_type=f32)
        result = result + weight_buf[c][:, 0:1] * picked
    out_ref[...] = result.astype(out_ref.dtype)

    for copy in sends:
        copy.wait_send()
    for s in range(n_sp):

        @pl.when(me_s != s)
        def _():
            pltpu.make_async_remote_copy(
                src_ref=o_out.at[s],
                dst_ref=ho_buf.at[me_t, me_s],
                send_sem=o_send.at[s],
                recv_sem=o_recv.at[me_s],
                device_id={"sp": s},
                device_id_type=MESH,
            ).wait_send()


def fused_body(
    residual_in,
    query_rows,
    key_rows,
    value_rows,
    map_weight,
    head_gain,
    out_proj,
    norm_gain,
    route_ids,
    route_weights,
    expert_gate,
    expert_up,
    expert_down,
    shared_gate,
    shared_up,
    shared_down,
):
    n_sp = lax.axis_size("sp")
    n_tp = lax.axis_size("tp")
    rows, col_dev = residual_in.shape
    topk = route_ids.shape[1]
    capacity = 5 * rows * topk // (4 * n_sp)
    cap = (capacity + 15) // 16 * 16
    hid_units = shared_gate.shape[0]
    bf16 = jnp.bfloat16
    pieces = 4 + 2 * n_sp
    peer_slots = (n_tp // 2 - 1) * (n_sp // 2)
    n_gs = 1 + 2 * (n_tp // 2 - 1)
    dma = pltpu.SemaphoreType.DMA
    vmem = pl.BlockSpec(memory_space=pltpu.VMEM)
    hbm = pl.BlockSpec(memory_space=pl.ANY)
    return pl.pallas_call(
        functools.partial(layer_kernel, n_sp, n_tp),
        out_shape=jax.ShapeDtypeStruct((rows, col_dev), bf16),
        in_specs=[vmem] * 9 + [hbm] * 7,
        out_specs=vmem,
        scratch_shapes=[
            pltpu.VMEM(out_proj.shape, bf16),
            pltpu.VMEM(expert_gate.shape[1:], bf16),
            pltpu.VMEM(expert_up.shape[1:], bf16),
            pltpu.VMEM(expert_down.shape[1:], bf16),
            pltpu.VMEM(shared_gate.shape, bf16),
            pltpu.VMEM(shared_up.shape, bf16),
            pltpu.VMEM(shared_down.shape, bf16),
            pltpu.VMEM((n_sp // 2, rows, 128), bf16),
            pltpu.VMEM((n_sp, rows // 4, 128), bf16),
            pltpu.VMEM((n_sp, rows, 128), bf16),
            pltpu.VMEM((n_sp, rows // 4, 128), bf16),
            pltpu.VMEM((n_sp, rows // 4, 128), bf16),
            pltpu.VMEM((n_tp, n_sp, rows // 4, 128), bf16),
            pltpu.VMEM((n_tp, rows, col_dev), bf16),
            pltpu.VMEM((n_sp, cap, col_dev), bf16),
            pltpu.VMEM((n_tp, n_sp, cap, col_dev), bf16),
            pltpu.VMEM((n_tp, rows, hid_units), bf16),
            pltpu.VMEM((n_tp, n_sp, cap, hid_units), bf16),
            pltpu.VMEM((n_sp, cap, col_dev), bf16),
            pltpu.VMEM((n_sp, cap, col_dev), bf16),
            pltpu.VMEM((n_sp * cap, rows), bf16),
            pltpu.VMEM((2, rows, n_sp * cap), bf16),
            pltpu.VMEM((2, rows, 128), jnp.float32),
            dma((7,)),
            dma((2 * n_sp,)),
            dma((n_sp,)),
            dma((n_sp,)),
            dma((n_sp,)),
            dma((n_sp,)),
            dma((n_sp,)),
            dma((n_sp,)),
            dma((n_sp,)),
            dma((n_sp,)),
            dma((pieces * n_gs,)),
            dma((pieces * n_tp,)),
            pltpu.VMEM((peer_slots, cap, col_dev), bf16),
            dma((peer_slots,)),
            dma((peer_slots,)),
            pltpu.VMEM((rows, col_dev), jnp.float32),
        ],
        compiler_params=pltpu.CompilerParams(collective_id=0, has_side_effects=True),
    )(
        query_rows,
        key_rows,
        value_rows,
        residual_in,
        map_weight[None, :],
        head_gain[None, :],
        norm_gain[None, :],
        route_ids.T,
        route_weights.T,
        out_proj,
        expert_gate,
        expert_up,
        expert_down,
        shared_gate,
        shared_up,
        shared_down,
    )


def layer(*args):
    residual_in, map_weight, head_gain, route_ids = args[0], args[4], args[5], args[8]
    fits = (
        2 * map_weight.shape[0] == lax.axis_size("sp") == 8
        and map_weight.shape[0] % 2 == 0
        and head_gain.shape[0] == 64
        and route_ids.shape[1] == 2
        and args[10].shape[0] == 1
        and residual_in.shape[0] % 64 == 0
        and residual_in.shape[1] % 128 == 0
        and args[13].shape[0] % 128 == 0
        and lax.axis_size("tp") in (4, 8)
    )
    return (fused_body if fits else body)(*args)


def solution(mesh):
    in_specs = (
        P("sp", "tp"),
        P("sp", "tp"),
        P("sp", "tp"),
        P("sp", "tp"),
        P("tp"),
        P(),
        P(None, "tp"),
        P(),
        P("sp", None),
        P("sp", None),
        P("sp", "tp", None),
        P("sp", "tp", None),
        P("sp", None, "tp"),
        P("tp", None),
        P("tp", None),
        P(None, "tp"),
    )
    out_specs = P("sp", "tp")
    return jax.shard_map(layer, mesh=mesh, in_specs=in_specs, out_specs=out_specs, check_vma=False)
```

```python
import functools

import jax
import jax.numpy as jnp
from jax import lax
from jax.experimental import pallas as pl
from jax.experimental.pallas import tpu as pltpu
from jax.sharding import PartitionSpec as P

epsilon = 1e-06
masked_score = -1e30
MESH = pl.DeviceIdType.MESH


def rms_scale(values, gain_vec):
    squares = jnp.mean(values * values, axis=-1, keepdims=True)
    return values * lax.rsqrt(squares + epsilon) * gain_vec


def block_slots(route_block, experts_all, capacity):
    flat_ids = route_block.reshape(-1)
    one_hot = (flat_ids[:, None] == jnp.arange(experts_all, dtype=jnp.int32)[None, :]).astype(
        jnp.int32
    )
    earlier = jnp.cumsum(one_hot, axis=0) - one_hot
    position = jnp.sum(earlier * one_hot, axis=1)
    return (flat_ids * capacity + position).reshape(route_block.shape)


def body(
    residual_in,
    query_rows,
    key_rows,
    value_rows,
    map_weight,
    head_gain,
    out_proj,
    norm_gain,
    route_ids,
    route_weights,
    expert_gate,
    expert_up,
    expert_down,
    shared_gate,
    shared_up,
    shared_down,
):
    seq_dev = residual_in.shape[0]
    col_dev = residual_in.shape[1]
    heads_here = map_weight.shape[0]
    head_dim = head_gain.shape[0]
    half_dim = head_dim // 2
    topk_count = route_ids.shape[1]
    exp_here = expert_gate.shape[0]
    experts_all = exp_here * lax.axis_size("sp")
    capacity = 5 * seq_dev * topk_count // (4 * experts_all)
    score_scale = half_dim ** (-0.5)
    query_pos = lax.axis_index("sp") * seq_dev + jnp.arange(seq_dev, dtype=jnp.int32)
    query_heads = query_rows.reshape(seq_dev, heads_here, 2, half_dim)
    key_piece = lax.all_gather(key_rows, "sp", axis=0, tiled=True)
    value_piece = lax.all_gather(value_rows, "sp", axis=0, tiled=True)
    piece_len = key_piece.shape[0]
    key_heads = key_piece.reshape(piece_len, heads_here, 2, half_dim)
    value_heads = value_piece.reshape(piece_len, heads_here, head_dim)
    scores = (
        jnp.einsum("qhmd,khmd->mhqk", query_heads, key_heads, preferred_element_type=jnp.float32)
        * score_scale
    )
    key_pos = jnp.arange(piece_len, dtype=jnp.int32)
    visible = key_pos[None, :] <= query_pos[:, None]
    scores = jnp.where(visible, scores, masked_score)
    run_max = jnp.full((2, heads_here, seq_dev), masked_score, jnp.float32)
    new_max = jnp.maximum(run_max, jnp.max(scores, axis=-1))
    expo = jnp.where(visible, jnp.exp(scores - new_max[..., None]), 0.0)
    new_sum = jnp.sum(expo, axis=-1)
    product = jnp.einsum(
        "mhqk,khd->mhqd", expo.astype(jnp.bfloat16), value_heads, preferred_element_type=jnp.float32
    )
    summed = product / new_sum[..., None]
    diff_out = summed[0] - map_weight[:, None, None] * summed[1]
    head_out = rms_scale(diff_out, head_gain).astype(jnp.bfloat16)
    head_out = jnp.transpose(head_out, (1, 0, 2)).reshape(seq_dev, heads_here * head_dim)
    attn = jnp.dot(
        lax.all_gather(head_out, "tp", axis=1, tiled=True),
        out_proj,
        preferred_element_type=jnp.float32,
    )
    hidden_state = (residual_in.astype(jnp.float32) + attn).astype(jnp.bfloat16)
    full_rows = lax.all_gather(hidden_state, "tp", axis=1, tiled=True)
    normed = rms_scale(full_rows.astype(jnp.float32), norm_gain).astype(jnp.bfloat16)
    shared_gate_part = jnp.einsum(
        "rd,fd->rf", normed, shared_gate, preferred_element_type=jnp.float32
    )
    shared_up_part = jnp.einsum("rd,fd->rf", normed, shared_up, preferred_element_type=jnp.float32)
    shared_hidden = (jax.nn.silu(shared_gate_part) * shared_up_part).astype(jnp.bfloat16)
    slot_ids = block_slots(route_ids, experts_all, capacity)
    token_of = jnp.repeat(jnp.arange(seq_dev, dtype=jnp.int32), topk_count)
    slot_token = (
        jnp.full((experts_all * capacity,), seq_dev, jnp.int32)
        .at[slot_ids.reshape(-1)]
        .set(token_of)
    )
    own_cols = lax.dynamic_slice_in_dim(normed, lax.axis_index("tp") * col_dev, col_dev, 1)
    padded = jnp.concatenate([own_cols, jnp.zeros((1, col_dev), jnp.bfloat16)], axis=0)
    outgoing = jnp.take(padded, slot_token, axis=0).reshape(experts_all, capacity, col_dev)
    arrived = lax.all_to_all(outgoing, "sp", split_axis=0, concat_axis=1, tiled=True)
    arrived_rows = arrived.shape[1]
    pieces = lax.all_gather(arrived, "tp", axis=2, tiled=True)
    gate_add = jnp.einsum("erd,efd->erf", pieces, expert_gate, preferred_element_type=jnp.float32)
    up_add = jnp.einsum("erd,efd->erf", pieces, expert_up, preferred_element_type=jnp.float32)
    expert_hidden = (jax.nn.silu(gate_add) * up_add).astype(jnp.bfloat16)
    expert_flat = expert_hidden.reshape(exp_here * arrived_rows, expert_hidden.shape[2])
    pieces = (
        lax.all_gather(shared_hidden, "tp", axis=1, tiled=True),
        lax.all_gather(expert_flat, "tp", axis=1, tiled=True),
    )
    piece_width = pieces[0].shape[1]
    routed_piece = pieces[1].reshape(exp_here, arrived_rows, piece_width)
    shared_add = jnp.dot(pieces[0], shared_down, preferred_element_type=jnp.float32)
    expert_add = jnp.einsum(
        "erf,efd->erd", routed_piece, expert_down, preferred_element_type=jnp.float32
    )
    returned_rows = lax.all_to_all(
        expert_add.astype(jnp.bfloat16), "sp", split_axis=1, concat_axis=0, tiled=True
    )
    returned_flat = returned_rows.reshape(experts_all * capacity, col_dev)
    picked = (
        jnp.take(returned_flat, slot_ids.reshape(-1), axis=0)
        .reshape(seq_dev, topk_count, col_dev)
        .astype(jnp.float32)
    )
    routed = jnp.sum(picked * route_weights[:, :, None], axis=1)
    return (hidden_state.astype(jnp.float32) + shared_add + routed).astype(jnp.bfloat16)


def lane_iota(rows):
    return lax.broadcasted_iota(jnp.int32, (rows, 128), 1)


def roll_half(values):
    return pltpu.roll(values, 64, 1)


def contract_last(a, b):
    return lax.dot_general(a, b, (((1,), (1,)), ((), ())), preferred_element_type=jnp.float32)


def layer_kernel(
    n_sp,
    n_tp,
    q_hbm,
    k_hbm,
    v_hbm,
    res_hbm,
    map_w_hbm,
    head_g_hbm,
    norm_g_hbm,
    ids_hbm,
    route_w_hbm,
    out_proj,
    exp_gate,
    exp_up,
    exp_down,
    sh_gate,
    sh_up,
    sh_down,
    out_ref,
    w_out,
    w_gate,
    w_up,
    w_down,
    w_sgate,
    w_sup,
    w_sdown,
    kv_out,
    q_out,
    kv_buf,
    q_buf,
    o_out,
    ho_buf,
    hid_buf,
    disp_out,
    arr_buf,
    sh_buf,
    eh_buf,
    res_out,
    ret_buf,
    spread_buf,
    pick_buf,
    weight_buf,
    w_sem,
    a_send,
    q_send,
    kv_recv,
    q_recv,
    o_send,
    o_recv,
    d_send,
    d_recv,
    r_send,
    r_recv,
    g_send,
    g_recv,
    peer_out,
    p_send,
    p_recv,
    shared_sum,
    q_in,
    k_in,
    v_in,
    res_in,
    map_w,
    head_g,
    norm_g,
    ids_in,
    route_w,
    in_sem,
):
    me_s = lax.axis_index("sp")
    me_t = lax.axis_index("tp")
    sib = me_t + 1 - 2 * lax.rem(me_t, 2)
    peers = n_tp // 2 - 1
    rows = res_in.shape[0]
    col_dev = res_in.shape[1]
    half = rows // 2
    quarter = rows // 4
    cap = arr_buf.shape[2]
    half_dim = 32
    piece_far = 3 + 2 * n_sp
    bf16 = jnp.bfloat16
    f32 = jnp.float32

    def across(k):
        other = me_s
        for b in range(n_sp.bit_length() - 1):
            if k >> b & 1:
                bit = lax.rem(me_s // (1 << b), 2)
                other = other + (1 << b) * (1 - 2 * bit)
        return other

    barrier = pltpu.get_barrier_semaphore()
    for d in range(1, n_sp):
        pl.semaphore_signal(
            barrier, inc=1, device_id={"sp": lax.rem(me_s + d, n_sp)}, device_id_type=MESH
        )
    for d in range(1, n_tp):
        pl.semaphore_signal(
            barrier, inc=1, device_id={"tp": lax.rem(me_t + d, n_tp)}, device_id_type=MESH
        )

    inputs = []
    for i, (src, dst) in enumerate(
        (
            (q_hbm, q_in),
            (k_hbm, k_in),
            (v_hbm, v_in),
            (res_hbm, res_in),
            (map_w_hbm, map_w),
            (head_g_hbm, head_g),
            (norm_g_hbm, norm_g),
            (ids_hbm, ids_in),
            (route_w_hbm, route_w),
        )
    ):
        copy = pltpu.make_async_copy(src, dst, in_sem.at[i])
        copy.start()
        inputs.append(copy)

    loads = []
    for i, (src, dst) in enumerate(
        (
            (out_proj, w_out),
            (sh_gate, w_sgate),
            (sh_up, w_sup),
            (exp_gate.at[0], w_gate),
            (exp_up.at[0], w_up),
            (exp_down.at[0], w_down),
            (sh_down, w_sdown),
        )
    ):
        copy = pltpu.make_async_copy(src, dst, w_sem.at[i])
        copy.start()
        loads.append(copy)

    sends = []

    def send(src, dst, ssem, rsem, device):
        copy = pltpu.make_async_remote_copy(
            src_ref=src,
            dst_ref=dst,
            send_sem=ssem,
            recv_sem=rsem,
            device_id=device,
            device_id_type=MESH,
        )
        copy.start()
        return copy

    def wait_recv(ref, ssem, rsem, device):
        pltpu.make_async_remote_copy(
            src_ref=ref,
            dst_ref=ref,
            send_sem=ssem,
            recv_sem=rsem,
            device_id=device,
            device_id_type=MESH,
        ).wait_recv()

    n_gs = 1 + 2 * peers

    def gather_start(piece, get):
        for k in range(1, peers + 1):
            other = lax.rem(me_t + 2 * k, n_tp)
            sends.append(
                send(
                    get(me_t),
                    get(me_t),
                    g_send.at[piece * n_gs + k],
                    g_recv.at[piece * n_tp + me_t],
                    {"tp": other},
                )
            )
        sends.append(
            send(
                get(me_t),
                get(me_t),
                g_send.at[piece * n_gs],
                g_recv.at[piece * n_tp + me_t],
                {"tp": sib},
            )
        )

    def gather_relay(piece, get):
        for k in range(1, peers + 1):
            other = lax.rem(me_t + 2 * k, n_tp)
            wait_recv(
                get(other), g_send.at[piece * n_gs], g_recv.at[piece * n_tp + other], {"tp": sib}
            )
            sends.append(
                send(
                    get(other),
                    get(other),
                    g_send.at[piece * n_gs + peers + k],
                    g_recv.at[piece * n_tp + other],
                    {"tp": sib},
                )
            )

    def gather_finish(piece, get):
        for k in range(peers + 1):
            other = lax.rem(sib + 2 * k, n_tp)
            wait_recv(
                get(other), g_send.at[piece * n_gs], g_recv.at[piece * n_tp + other], {"tp": sib}
            )

    for copy in inputs[:3]:
        copy.wait()
    low_rows = lane_iota(rows) < 64
    low_quarter = lane_iota(quarter) < 64
    for j in range(n_sp // 4):
        pair = slice(j * 128, (j + 1) * 128)
        keys = k_in[:, pair].astype(f32)
        vals = v_in[:, pair].astype(f32)
        kv_out[2 * j] = jnp.where(low_rows, keys, roll_half(vals)).astype(bf16)
        kv_out[2 * j + 1] = jnp.where(low_rows, roll_half(keys), vals).astype(bf16)
        for p in range(2):
            first = q_in[p * half : p * half + quarter, pair].astype(f32)
            second = q_in[p * half + quarter : (p + 1) * half, pair].astype(f32)
            q_out[4 * j + p] = jnp.where(low_quarter, first, roll_half(second)).astype(bf16)
            q_out[4 * j + 2 + p] = jnp.where(low_quarter, roll_half(first), second).astype(bf16)

    pl.semaphore_wait(barrier, n_sp + n_tp - 2)

    for d in (6, 7, 4, 5, 2, 3, 1):
        dst = across(d)
        if d % 2 == 0 or d == 1:
            sends.append(
                send(
                    kv_out.at[dst // 2],
                    kv_buf.at[me_s],
                    a_send.at[d],
                    kv_recv.at[me_s],
                    {"sp": dst},
                )
            )
    def send_queries(ds):
        for d in ds:
            dst = across(d)
            send(
                q_out.at[dst], q_buf.at[me_s], q_send.at[d], q_recv.at[me_s], {"sp": dst}
            )

    upper = me_s // (n_sp // 2)
    inner = lax.rem(me_s // 2 + upper, 2)

    @pl.when(inner == 1)
    def _():
        send_queries((6, 7, 4, 5))

    send_queries((2, 3, 1))
    kv_buf[me_s] = kv_out[me_s // 2]
    q_buf[me_s] = q_out[me_s]

    for copy in inputs[3:]:
        copy.wait()
    eye = lax.broadcasted_iota(jnp.int32, (rows, rows), 0)
    eye_lane = lax.broadcasted_iota(jnp.int32, (rows, rows), 1)
    same = eye == eye_lane
    before_col = eye_lane < eye
    before_row = eye < eye_lane

    def as_column(row):
        return jnp.sum(jnp.where(same, row, 0.0), axis=1, keepdims=True)

    ids_row = [jnp.bitwise_xor(ids_in[c : c + 1, :], me_s).astype(f32) for c in range(2)]
    ids_col = [as_column(row) for row in ids_row]
    weight_col = [as_column(route_w[c : c + 1, :]) for c in range(2)]
    slot_row = []
    slot_col = []
    for c in range(2):
        hit = (ids_row[0] == ids_col[c]) | (ids_row[1] == ids_col[c])
        count = jnp.sum(jnp.where(hit & before_col, 1.0, 0.0), axis=1, keepdims=True)
        slot_col.append(ids_col[c] * cap + count)
        hit = (ids_col[0] == ids_row[c]) | (ids_col[1] == ids_row[c])
        count = jnp.sum(jnp.where(hit & before_row, 1.0, 0.0), axis=0, keepdims=True)
        slot_row.append(ids_row[c] * cap + count)
    slots = n_sp * cap
    slot_iota = lax.broadcasted_iota(jnp.int32, (slots, rows), 0).astype(f32)
    chosen = (slot_iota == slot_row[0]) | (slot_iota == slot_row[1])
    spread_buf[...] = jnp.where(chosen, 1.0, 0.0).astype(bf16)
    col_iota = lax.broadcasted_iota(jnp.int32, (rows, slots), 1).astype(f32)
    for c in range(2):
        pick_buf[c] = jnp.where(col_iota == slot_col[c], 1.0, 0.0).astype(bf16)
        weight_buf[c] = jnp.broadcast_to(weight_col[c], (rows, 128))
    head_lane = lax.broadcasted_iota(jnp.int32, map_w.shape, 1)
    map_here = jnp.sum(
        jnp.where(head_lane == me_s // 2, map_w[...], 0.0), axis=1, keepdims=True
    )
    gain_here = jnp.concatenate([jnp.zeros((1, 64), f32), head_g[...]], axis=1)

    parity = lax.rem(me_s, 2)
    lane_q = lane_iota(quarter)
    scale = half_dim ** (-0.5)
    row_in = lax.broadcasted_iota(jnp.int32, (half, rows), 0) + parity * half
    visible_half = lax.broadcasted_iota(jnp.int32, (half, rows), 1) <= row_in
    visible = jnp.concatenate([visible_half.astype(f32)] * 2, axis=0) > 0.5
    high_lanes = lane_iota(half) >= 64
    zero_q = jnp.zeros((quarter, 128), f32)
    first_map = lane_q < 32
    second_map = (lane_q >= 32) & (lane_q < 64)
    batch = n_sp // 2
    for d in (6, 4, 2):
        src = across(d)
        wait_recv(kv_buf.at[src], a_send.at[0], kv_recv.at[src], {"sp": src})
        sends.append(
            send(
                kv_buf.at[src],
                kv_buf.at[src],
                a_send.at[d + 1],
                kv_recv.at[src],
                {"sp": across(1)},
            )
        )
        if d == 6:

            @pl.when(inner == 0)
            def _():
                send_queries((6, 7, 4, 5))

    for s in range(n_sp):

        @pl.when(parity != s % 2)
        def _():
            wait_recv(kv_buf.at[s], a_send.at[0], kv_recv.at[s], {"sp": across(1)})

        @pl.when(me_s != s)
        def _():
            wait_recv(q_buf.at[s], q_send.at[0], q_recv.at[s], {"sp": s})

    def attend(start):
        steps = range(start, start + batch)
        queries = {}
        for s in steps:
            packed = q_buf[s].astype(f32)
            rolled = roll_half(packed)
            queries[s] = jnp.concatenate(
                [
                    jnp.where(first_map, packed, zero_q),
                    jnp.where(first_map, rolled, zero_q),
                    jnp.where(second_map, packed, zero_q),
                    jnp.where(second_map, rolled, zero_q),
                ],
                axis=0,
            ).astype(bf16)
        keys = {s: kv_buf[0 : s + 1].reshape((s + 1) * rows, 128) for s in steps}
        scores = {}
        for s in steps:
            raw = contract_last(queries[s], keys[s]) * scale
            diag = jnp.where(visible, raw[:, s * rows :], masked_score)
            scores[s] = jnp.concatenate([raw[:, : s * rows], diag], axis=1) if s else diag
        row_max = {s: jnp.max(scores[s], axis=1, keepdims=True) for s in steps}
        expo = {s: jnp.exp(scores[s] - row_max[s]) for s in steps}
        total = {s: jnp.sum(expo[s], axis=1, keepdims=True) for s in steps}
        acc = {
            s: jnp.dot(expo[s].astype(bf16), keys[s], preferred_element_type=f32) for s in steps
        }
        diff = {}
        for s in steps:
            summed = acc[s] / total[s]
            raw = summed[0:half] - map_here * summed[half:rows]
            diff[s] = jnp.where(high_lanes, raw, 0.0)
        for s in steps:
            squares = jnp.sum(diff[s] * diff[s], axis=1, keepdims=True) * (1.0 / 64.0)
            head = diff[s] * lax.rsqrt(squares + epsilon) * gain_here
            o_out[s] = (roll_half(head[0:quarter]) + head[quarter:half]).astype(bf16)

        for s in steps:

            @pl.when(me_s != s)
            def _():
                send(
                    o_out.at[s],
                    ho_buf.at[me_t, me_s],
                    o_send.at[s],
                    o_recv.at[me_s],
                    {"sp": s},
                )

            @pl.when(me_s == s)
            def _():
                ho_buf[me_t, s] = o_out[s]


    @pl.when(upper == 1)
    def _():
        attend(0)
        attend(batch)

    @pl.when(upper == 0)
    def _():
        attend(batch)
        attend(0)

    split = n_sp // 2
    base = me_s // split * split

    def get_near(t):
        return ho_buf.at[t, pl.ds(base, split)]

    def get_far(t):
        return ho_buf.at[t, pl.ds(split - base, split)]

    for d in (4, 5, 6, 7, 1, 2, 3):
        other = across(d)
        wait_recv(ho_buf.at[me_t, other], o_send.at[d], o_recv.at[other], {"sp": other})
        if d == n_sp - 1:
            gather_start(piece_far, get_far)
    gather_start(0, get_near)
    for piece, get in ((piece_far, get_far), (0, get_near)):
        gather_relay(piece, get)
    for piece, get in ((piece_far, get_far), (0, get_near)):
        gather_finish(piece, get)

    blocks = []
    for p in range(2):
        for u in range(2):
            parts = []
            for t in range(n_tp):
                for j in range(n_sp // 4):
                    even = ho_buf[t, 4 * j + p].astype(f32)
                    odd = ho_buf[t, 4 * j + 2 + p].astype(f32)
                    if u == 0:
                        part = jnp.where(low_quarter, even, roll_half(odd))
                    else:
                        part = jnp.where(low_quarter, roll_half(even), odd)
                    parts.append(part.astype(bf16))
            blocks.append(jnp.concatenate(parts, axis=1))
    heads = jnp.concatenate(blocks, axis=0)
    loads[0].wait()
    attn = jnp.dot(heads, w_out[...], preferred_element_type=f32)
    hidden = (res_in[...].astype(f32) + attn).astype(bf16)
    hid_buf[me_t] = hidden

    def get_hid(t):
        return hid_buf.at[t]

    gather_start(1, get_hid)

    near = n_sp // 2

    def spread(lo, hi, cols):
        picked = jnp.dot(spread_buf[lo * cap : hi * cap], cols, preferred_element_type=f32)
        return picked.astype(bf16).reshape(hi - lo, cap, col_dev)

    def slot_at(d):
        return d if d < near else near + 2 * inner + 1 - d % 2

    def offset_of(e):
        if e < near:
            return e
        return (6 - 2 * inner if e < 6 else 4 + 2 * inner) + 1 - e % 2

    def source(e):
        if e < near:
            return across(e)
        side = me_s % 2 if e % 2 else 1 - me_s % 2
        return 2 * (3 * (1 - upper) if e < 6 else 2 - upper) + side

    def dispatch(d):
        e = slot_at(d)
        sends.append(
            send(
                disp_out.at[d], arr_buf.at[me_t, e], d_send.at[d], d_recv.at[e], {"sp": across(d)}
            )
        )

    def dispatch_peer(d, k):
        other = lax.rem(me_t + 2 * k, n_tp)
        i = (k - 1) * near + d
        return send(
            peer_out.at[i], arr_buf.at[other, d], p_send.at[i], p_recv.at[i], {"sp": across(d)}
        )

    def get_arr(d):
        return lambda t: arr_buf.at[t, d]

    def normalise(pieces):
        full = [piece.astype(f32) for piece in pieces]
        squares = sum(jnp.sum(piece * piece, axis=1, keepdims=True) for piece in full)
        factor = lax.rsqrt(squares * (1.0 / (n_tp * col_dev)) + epsilon)
        return jnp.concatenate(
            [
                (piece * factor * norm_g[:, t * col_dev : (t + 1) * col_dev]).astype(bf16)
                for t, piece in enumerate(full)
            ],
            axis=1,
        )

    def gated(normed, gate, up):
        gate_part = contract_last(normed, gate[...])
        up_part = contract_last(normed, up[...])
        return (gate_part / (1.0 + jnp.exp(-gate_part)) * up_part).astype(bf16)

    def arrive(d):
        wait_recv(arr_buf.at[me_t, d], d_send.at[d], d_recv.at[d], {"sp": source(d)})
        gather_start(2 + d, get_arr(d))

    def relay(d):
        gather_relay(2 + d, get_arr(d))

    def arrive_near(d):
        piece = 2 + d
        get = get_arr(d)
        wait_recv(get(me_t), d_send.at[d], d_recv.at[d], {"sp": across(d)})
        sends.append(
            send(
                get(me_t),
                get(me_t),
                g_send.at[piece * n_gs],
                g_recv.at[piece * n_tp + me_t],
                {"tp": sib},
            )
        )

    def arrive_peer(d):
        piece = 2 + d
        get = get_arr(d)
        for k in range(1, peers + 1):
            other = lax.rem(me_t + 2 * k, n_tp)
            i = (k - 1) * near + d
            wait_recv(get(other), p_send.at[i], p_recv.at[i], {"sp": across(d)})
            sends.append(
                send(
                    get(other),
                    get(other),
                    g_send.at[piece * n_gs + peers + k],
                    g_recv.at[piece * n_tp + other],
                    {"tp": sib},
                )
            )

    def get_sh(t):
        return sh_buf.at[t]

    def get_eh(lo, hi):
        return lambda t: eh_buf.at[t, pl.ds(lo, hi - lo)]

    piece_sh = 2 + n_sp
    piece_eh = 3 + n_sp

    def expert_up(lo, hi):
        for d in range(lo, hi):
            if d:
                gather_finish(2 + d, get_arr(d))
        count = (hi - lo) * cap
        normed = normalise([arr_buf[t, lo:hi].reshape(count, col_dev) for t in range(n_tp)])
        hidden_units = gated(normed, w_gate, w_up)
        eh_buf[me_t, lo:hi] = hidden_units.reshape(hi - lo, cap, hidden_units.shape[1])

    def start_eh(lo, hi):
        gather_start(piece_eh + lo, get_eh(lo, hi))

    def relay_eh(lo, hi):
        gather_relay(piece_eh + lo, get_eh(lo, hi))

    def expert_out(lo, hi):
        gather_finish(piece_eh + lo, get_eh(lo, hi))
        count = (hi - lo) * cap
        joined = jnp.concatenate(
            [eh_buf[t, lo:hi].reshape(count, eh_buf.shape[3]) for t in range(n_tp)], axis=1
        )
        result = jnp.dot(joined, w_down[...], preferred_element_type=f32).astype(bf16)
        res_out[lo:hi] = result.reshape(hi - lo, cap, col_dev)
        for d in range(lo, hi):
            if d == 0:
                ret_buf[0] = res_out[0]
            else:
                sends.append(
                    send(
                        res_out.at[d],
                        ret_buf.at[offset_of(d)],
                        r_send.at[d],
                        r_recv.at[offset_of(d)],
                        {"sp": source(d)},
                    )
                )

    def shared_up():
        normed_own = normalise([hid_buf[t] for t in range(n_tp)])
        sh_buf[me_t] = gated(normed_own, w_sgate, w_sup)

    def shared_down():
        shared_all = jnp.concatenate([sh_buf[t] for t in range(n_tp)], axis=1)
        shared_sum[...] = hid_buf[me_t].astype(f32) + jnp.dot(
            shared_all, w_sdown[...], preferred_element_type=f32
        )

    def own_rows():
        for t in range(n_tp):
            arr_buf[t, 0] = jnp.dot(
                spread_buf[0:cap], hid_buf[t], preferred_element_type=f32
            ).astype(bf16)

    def wait_loads():
        for copy in loads[1:]:
            copy.wait()

    def send_own():
        disp_out[near:n_sp] = spread(near, n_sp, hidden)
        for d in (4, 6, 5, 7):
            dispatch(d)
        disp_out[1:near] = spread(1, near, hidden)
        for d in range(1, near):
            dispatch(d)

    def peer_cols():
        for k in range(1, peers + 1):
            other = lax.rem(me_t + 2 * k, n_tp)
            peer_out[(k - 1) * near + 1 : k * near] = spread(1, near, hid_buf[other])
            for d in range(1, near):
                sends.append(dispatch_peer(d, k))

    send_own()
    arrive(5)
    gather_relay(1, get_hid)
    peer_cols()
    gather_finish(1, get_hid)
    arrive(4)
    relay(5)
    wait_loads()
    shared_up()
    expert_up(5, 6)
    start_eh(5, 6)
    relay(4)
    own_rows()
    arrive(7)
    arrive_near(1)
    arrive_peer(1)
    expert_up(4, 5)
    start_eh(4, 5)
    relay_eh(5, 6)
    arrive(6)
    gather_start(piece_sh, get_sh)
    relay(7)
    expert_up(0, 2)
    expert_out(5, 6)
    expert_up(7, 8)
    start_eh(7, 8)
    relay_eh(4, 5)
    arrive_near(2)
    arrive_near(3)
    arrive_peer(2)
    arrive_peer(3)
    relay(6)
    expert_out(4, 5)
    start_eh(0, 2)
    expert_up(6, 7)
    start_eh(6, 7)
    relay_eh(7, 8)
    expert_up(2, 4)
    start_eh(2, 4)
    expert_out(7, 8)
    relay_eh(0, 2)
    gather_relay(piece_sh, get_sh)
    relay_eh(6, 7)
    expert_out(0, 2)
    expert_out(6, 7)
    relay_eh(2, 4)
    gather_finish(piece_sh, get_sh)
    shared_down()
    expert_out(2, 4)
    result = shared_sum[...]
    for d in range(1, n_sp):
        wait_recv(ret_buf.at[d], r_send.at[d], r_recv.at[d], {"sp": across(d)})
    returned = ret_buf[...].reshape(slots, col_dev)
    for c in range(2):
        picked = jnp.dot(pick_buf[c], returned, preferred_element_type=f32)
        result = result + weight_buf[c][:, 0:1] * picked
    out_ref[...] = result.astype(out_ref.dtype)

    for copy in sends:
        copy.wait_send()
    for d in range(1, n_sp):
        pltpu.make_async_remote_copy(
            src_ref=q_out.at[d],
            dst_ref=q_buf.at[me_s],
            send_sem=q_send.at[d],
            recv_sem=q_recv.at[me_s],
            device_id={"sp": across(d)},
            device_id_type=MESH,
        ).wait_send()
    for s in range(n_sp):

        @pl.when(me_s != s)
        def _():
            pltpu.make_async_remote_copy(
                src_ref=o_out.at[s],
                dst_ref=ho_buf.at[me_t, me_s],
                send_sem=o_send.at[s],
                recv_sem=o_recv.at[me_s],
                device_id={"sp": s},
                device_id_type=MESH,
            ).wait_send()


def fused_body(
    residual_in,
    query_rows,
    key_rows,
    value_rows,
    map_weight,
    head_gain,
    out_proj,
    norm_gain,
    route_ids,
    route_weights,
    expert_gate,
    expert_up,
    expert_down,
    shared_gate,
    shared_up,
    shared_down,
):
    n_sp = lax.axis_size("sp")
    n_tp = lax.axis_size("tp")
    rows, col_dev = residual_in.shape
    topk = route_ids.shape[1]
    capacity = 5 * rows * topk // (4 * n_sp)
    cap = (capacity + 15) // 16 * 16
    hid_units = shared_gate.shape[0]
    bf16 = jnp.bfloat16
    pieces = 4 + 2 * n_sp
    peer_slots = (n_tp // 2 - 1) * (n_sp // 2)
    n_gs = 1 + 2 * (n_tp // 2 - 1)
    dma = pltpu.SemaphoreType.DMA
    vmem = pl.BlockSpec(memory_space=pltpu.VMEM)
    hbm = pl.BlockSpec(memory_space=pl.ANY)
    return pl.pallas_call(
        functools.partial(layer_kernel, n_sp, n_tp),
        out_shape=pltpu.VMEM((rows, col_dev), bf16),
        in_specs=[hbm] * 16,
        out_specs=vmem,
        scratch_shapes=[
            pltpu.VMEM(out_proj.shape, bf16),
            pltpu.VMEM(expert_gate.shape[1:], bf16),
            pltpu.VMEM(expert_up.shape[1:], bf16),
            pltpu.VMEM(expert_down.shape[1:], bf16),
            pltpu.VMEM(shared_gate.shape, bf16),
            pltpu.VMEM(shared_up.shape, bf16),
            pltpu.VMEM(shared_down.shape, bf16),
            pltpu.VMEM((n_sp // 2, rows, 128), bf16),
            pltpu.VMEM((n_sp, rows // 4, 128), bf16),
            pltpu.VMEM((n_sp, rows, 128), bf16),
            pltpu.VMEM((n_sp, rows // 4, 128), bf16),
            pltpu.VMEM((n_sp, rows // 4, 128), bf16),
            pltpu.VMEM((n_tp, n_sp, rows // 4, 128), bf16),
            pltpu.VMEM((n_tp, rows, col_dev), bf16),
            pltpu.VMEM((n_sp, cap, col_dev), bf16),
            pltpu.VMEM((n_tp, n_sp, cap, col_dev), bf16),
            pltpu.VMEM((n_tp, rows, hid_units), bf16),
            pltpu.VMEM((n_tp, n_sp, cap, hid_units), bf16),
            pltpu.VMEM((n_sp, cap, col_dev), bf16),
            pltpu.VMEM((n_sp, cap, col_dev), bf16),
            pltpu.VMEM((n_sp * cap, rows), bf16),
            pltpu.VMEM((2, rows, n_sp * cap), bf16),
            pltpu.VMEM((2, rows, 128), jnp.float32),
            dma((7,)),
            dma((n_sp,)),
            dma((n_sp,)),
            dma((n_sp,)),
            dma((n_sp,)),
            dma((n_sp,)),
            dma((n_sp,)),
            dma((n_sp,)),
            dma((n_sp,)),
            dma((n_sp,)),
            dma((n_sp,)),
            dma((pieces * n_gs,)),
            dma((pieces * n_tp,)),
            pltpu.VMEM((peer_slots, cap, col_dev), bf16),
            dma((peer_slots,)),
            dma((peer_slots,)),
            pltpu.VMEM((rows, col_dev), jnp.float32),
            pltpu.VMEM(query_rows.shape, bf16),
            pltpu.VMEM(key_rows.shape, bf16),
            pltpu.VMEM(value_rows.shape, bf16),
            pltpu.VMEM(residual_in.shape, bf16),
            pltpu.VMEM((1,) + map_weight.shape, jnp.float32),
            pltpu.VMEM((1,) + head_gain.shape, jnp.float32),
            pltpu.VMEM((1,) + norm_gain.shape, jnp.float32),
            pltpu.VMEM((topk, rows), jnp.int32),
            pltpu.VMEM((topk, rows), jnp.float32),
            dma((9,)),
        ],
        compiler_params=pltpu.CompilerParams(collective_id=0, has_side_effects=True),
    )(
        query_rows,
        key_rows,
        value_rows,
        residual_in,
        map_weight[None, :],
        head_gain[None, :],
        norm_gain[None, :],
        route_ids.T,
        route_weights.T,
        out_proj,
        expert_gate,
        expert_up,
        expert_down,
        shared_gate,
        shared_up,
        shared_down,
    )


def layer(*args):
    residual_in, map_weight, head_gain, route_ids = args[0], args[4], args[5], args[8]
    fits = (
        2 * map_weight.shape[0] == lax.axis_size("sp") == 8
        and map_weight.shape[0] % 2 == 0
        and head_gain.shape[0] == 64
        and route_ids.shape[1] == 2
        and args[10].shape[0] == 1
        and residual_in.shape[0] % 64 == 0
        and residual_in.shape[1] % 128 == 0
        and args[13].shape[0] % 128 == 0
        and lax.axis_size("tp") in (4, 8)
    )
    return (fused_body if fits else body)(*args)


def solution(mesh):
    in_specs = (
        P("sp", "tp"),
        P("sp", "tp"),
        P("sp", "tp"),
        P("sp", "tp"),
        P("tp"),
        P(),
        P(None, "tp"),
        P(),
        P("sp", None),
        P("sp", None),
        P("sp", "tp", None),
        P("sp", "tp", None),
        P("sp", None, "tp"),
        P("tp", None),
        P("tp", None),
        P(None, "tp"),
    )
    out_specs = P("sp", "tp")
    return jax.shard_map(layer, mesh=mesh, in_specs=in_specs, out_specs=out_specs, check_vma=False)
```

```python
import functools

import jax
import jax.numpy as jnp
from jax import lax
from jax.experimental import pallas as pl
from jax.experimental.pallas import tpu as pltpu
from jax.sharding import PartitionSpec as P

epsilon = 1e-06
masked_score = -1e30
MESH = pl.DeviceIdType.MESH


def rms_scale(values, gain_vec):
    squares = jnp.mean(values * values, axis=-1, keepdims=True)
    return values * lax.rsqrt(squares + epsilon) * gain_vec


def block_slots(route_block, experts_all, capacity):
    flat_ids = route_block.reshape(-1)
    one_hot = (flat_ids[:, None] == jnp.arange(experts_all, dtype=jnp.int32)[None, :]).astype(
        jnp.int32
    )
    earlier = jnp.cumsum(one_hot, axis=0) - one_hot
    position = jnp.sum(earlier * one_hot, axis=1)
    return (flat_ids * capacity + position).reshape(route_block.shape)


def body(
    residual_in,
    query_rows,
    key_rows,
    value_rows,
    map_weight,
    head_gain,
    out_proj,
    norm_gain,
    route_ids,
    route_weights,
    expert_gate,
    expert_up,
    expert_down,
    shared_gate,
    shared_up,
    shared_down,
):
    seq_dev = residual_in.shape[0]
    col_dev = residual_in.shape[1]
    heads_here = map_weight.shape[0]
    head_dim = head_gain.shape[0]
    half_dim = head_dim // 2
    topk_count = route_ids.shape[1]
    exp_here = expert_gate.shape[0]
    experts_all = exp_here * lax.axis_size("sp")
    capacity = 5 * seq_dev * topk_count // (4 * experts_all)
    score_scale = half_dim ** (-0.5)
    query_pos = lax.axis_index("sp") * seq_dev + jnp.arange(seq_dev, dtype=jnp.int32)
    query_heads = query_rows.reshape(seq_dev, heads_here, 2, half_dim)
    key_piece = lax.all_gather(key_rows, "sp", axis=0, tiled=True)
    value_piece = lax.all_gather(value_rows, "sp", axis=0, tiled=True)
    piece_len = key_piece.shape[0]
    key_heads = key_piece.reshape(piece_len, heads_here, 2, half_dim)
    value_heads = value_piece.reshape(piece_len, heads_here, head_dim)
    scores = (
        jnp.einsum("qhmd,khmd->mhqk", query_heads, key_heads, preferred_element_type=jnp.float32)
        * score_scale
    )
    key_pos = jnp.arange(piece_len, dtype=jnp.int32)
    visible = key_pos[None, :] <= query_pos[:, None]
    scores = jnp.where(visible, scores, masked_score)
    run_max = jnp.full((2, heads_here, seq_dev), masked_score, jnp.float32)
    new_max = jnp.maximum(run_max, jnp.max(scores, axis=-1))
    expo = jnp.where(visible, jnp.exp(scores - new_max[..., None]), 0.0)
    new_sum = jnp.sum(expo, axis=-1)
    product = jnp.einsum(
        "mhqk,khd->mhqd", expo.astype(jnp.bfloat16), value_heads, preferred_element_type=jnp.float32
    )
    summed = product / new_sum[..., None]
    diff_out = summed[0] - map_weight[:, None, None] * summed[1]
    head_out = rms_scale(diff_out, head_gain).astype(jnp.bfloat16)
    head_out = jnp.transpose(head_out, (1, 0, 2)).reshape(seq_dev, heads_here * head_dim)
    attn = jnp.dot(
        lax.all_gather(head_out, "tp", axis=1, tiled=True),
        out_proj,
        preferred_element_type=jnp.float32,
    )
    hidden_state = (residual_in.astype(jnp.float32) + attn).astype(jnp.bfloat16)
    full_rows = lax.all_gather(hidden_state, "tp", axis=1, tiled=True)
    normed = rms_scale(full_rows.astype(jnp.float32), norm_gain).astype(jnp.bfloat16)
    shared_gate_part = jnp.einsum(
        "rd,fd->rf", normed, shared_gate, preferred_element_type=jnp.float32
    )
    shared_up_part = jnp.einsum("rd,fd->rf", normed, shared_up, preferred_element_type=jnp.float32)
    shared_hidden = (jax.nn.silu(shared_gate_part) * shared_up_part).astype(jnp.bfloat16)
    slot_ids = block_slots(route_ids, experts_all, capacity)
    token_of = jnp.repeat(jnp.arange(seq_dev, dtype=jnp.int32), topk_count)
    slot_token = (
        jnp.full((experts_all * capacity,), seq_dev, jnp.int32)
        .at[slot_ids.reshape(-1)]
        .set(token_of)
    )
    own_cols = lax.dynamic_slice_in_dim(normed, lax.axis_index("tp") * col_dev, col_dev, 1)
    padded = jnp.concatenate([own_cols, jnp.zeros((1, col_dev), jnp.bfloat16)], axis=0)
    outgoing = jnp.take(padded, slot_token, axis=0).reshape(experts_all, capacity, col_dev)
    arrived = lax.all_to_all(outgoing, "sp", split_axis=0, concat_axis=1, tiled=True)
    arrived_rows = arrived.shape[1]
    pieces = lax.all_gather(arrived, "tp", axis=2, tiled=True)
    gate_add = jnp.einsum("erd,efd->erf", pieces, expert_gate, preferred_element_type=jnp.float32)
    up_add = jnp.einsum("erd,efd->erf", pieces, expert_up, preferred_element_type=jnp.float32)
    expert_hidden = (jax.nn.silu(gate_add) * up_add).astype(jnp.bfloat16)
    expert_flat = expert_hidden.reshape(exp_here * arrived_rows, expert_hidden.shape[2])
    pieces = (
        lax.all_gather(shared_hidden, "tp", axis=1, tiled=True),
        lax.all_gather(expert_flat, "tp", axis=1, tiled=True),
    )
    piece_width = pieces[0].shape[1]
    routed_piece = pieces[1].reshape(exp_here, arrived_rows, piece_width)
    shared_add = jnp.dot(pieces[0], shared_down, preferred_element_type=jnp.float32)
    expert_add = jnp.einsum(
        "erf,efd->erd", routed_piece, expert_down, preferred_element_type=jnp.float32
    )
    returned_rows = lax.all_to_all(
        expert_add.astype(jnp.bfloat16), "sp", split_axis=1, concat_axis=0, tiled=True
    )
    returned_flat = returned_rows.reshape(experts_all * capacity, col_dev)
    picked = (
        jnp.take(returned_flat, slot_ids.reshape(-1), axis=0)
        .reshape(seq_dev, topk_count, col_dev)
        .astype(jnp.float32)
    )
    routed = jnp.sum(picked * route_weights[:, :, None], axis=1)
    return (hidden_state.astype(jnp.float32) + shared_add + routed).astype(jnp.bfloat16)


def lane_iota(rows):
    return lax.broadcasted_iota(jnp.int32, (rows, 128), 1)


def roll_half(values):
    return pltpu.roll(values, 64, 1)


def contract_last(a, b):
    return lax.dot_general(a, b, (((1,), (1,)), ((), ())), preferred_element_type=jnp.float32)


def layer_kernel(
    n_sp,
    n_tp,
    q_hbm,
    k_hbm,
    v_hbm,
    res_hbm,
    map_w_hbm,
    head_g_hbm,
    norm_g_hbm,
    ids_hbm,
    route_w_hbm,
    out_proj,
    exp_gate,
    exp_up,
    exp_down,
    sh_gate,
    sh_up,
    sh_down,
    out_ref,
    w_out,
    w_gate,
    w_up,
    w_down,
    w_sgate,
    w_sup,
    w_sdown,
    kv_out,
    q_out,
    kv_buf,
    q_buf,
    o_out,
    ho_buf,
    hid_buf,
    disp_out,
    arr_buf,
    sh_buf,
    eh_buf,
    res_out,
    ret_buf,
    spread_buf,
    pick_buf,
    weight_buf,
    w_sem,
    a_send,
    q_send,
    kv_recv,
    q_recv,
    o_send,
    o_recv,
    d_send,
    d_recv,
    r_send,
    r_recv,
    g_send,
    g_recv,
    peer_out,
    p_send,
    p_recv,
    shared_sum,
    q_in,
    k_in,
    v_in,
    res_in,
    map_w,
    head_g,
    norm_g,
    ids_in,
    route_w,
    in_sem,
    t_gate,
    t_up,
    t_sgate,
    t_sup,
):
    me_s = lax.axis_index("sp")
    me_t = lax.axis_index("tp")
    sib = me_t + 1 - 2 * lax.rem(me_t, 2)
    peers = n_tp // 2 - 1
    rows = res_in.shape[0]
    col_dev = res_in.shape[1]
    half = rows // 2
    quarter = rows // 4
    cap = arr_buf.shape[2]
    half_dim = 32
    piece_far = 3 + 2 * n_sp
    bf16 = jnp.bfloat16
    f32 = jnp.float32

    def across(k):
        other = me_s
        for b in range(n_sp.bit_length() - 1):
            if k >> b & 1:
                bit = lax.rem(me_s // (1 << b), 2)
                other = other + (1 << b) * (1 - 2 * bit)
        return other

    barrier = pltpu.get_barrier_semaphore()
    for d in range(1, n_sp):
        pl.semaphore_signal(
            barrier, inc=1, device_id={"sp": lax.rem(me_s + d, n_sp)}, device_id_type=MESH
        )
    for d in range(1, n_tp):
        pl.semaphore_signal(
            barrier, inc=1, device_id={"tp": lax.rem(me_t + d, n_tp)}, device_id_type=MESH
        )

    inputs = []
    for i, (src, dst) in enumerate(
        (
            (q_hbm, q_in),
            (k_hbm, k_in),
            (v_hbm, v_in),
            (res_hbm, res_in),
            (map_w_hbm, map_w),
            (head_g_hbm, head_g),
            (norm_g_hbm, norm_g),
            (ids_hbm, ids_in),
            (route_w_hbm, route_w),
        )
    ):
        copy = pltpu.make_async_copy(src, dst, in_sem.at[i])
        copy.start()
        inputs.append(copy)

    loads = []
    for i, (src, dst) in enumerate(
        (
            (out_proj, w_out),
            (sh_gate, w_sgate),
            (sh_up, w_sup),
            (exp_gate.at[0], w_gate),
            (exp_up.at[0], w_up),
            (exp_down.at[0], w_down),
            (sh_down, w_sdown),
        )
    ):
        copy = pltpu.make_async_copy(src, dst, w_sem.at[i])
        copy.start()
        loads.append(copy)

    sends = []

    def send(src, dst, ssem, rsem, device):
        copy = pltpu.make_async_remote_copy(
            src_ref=src,
            dst_ref=dst,
            send_sem=ssem,
            recv_sem=rsem,
            device_id=device,
            device_id_type=MESH,
        )
        copy.start()
        return copy

    def wait_recv(ref, ssem, rsem, device):
        pltpu.make_async_remote_copy(
            src_ref=ref,
            dst_ref=ref,
            send_sem=ssem,
            recv_sem=rsem,
            device_id=device,
            device_id_type=MESH,
        ).wait_recv()

    n_gs = 1 + 2 * peers

    def gather_start(piece, get):
        for k in range(1, peers + 1):
            other = lax.rem(me_t + 2 * k, n_tp)
            sends.append(
                send(
                    get(me_t),
                    get(me_t),
                    g_send.at[piece * n_gs + k],
                    g_recv.at[piece * n_tp + me_t],
                    {"tp": other},
                )
            )
        sends.append(
            send(
                get(me_t),
                get(me_t),
                g_send.at[piece * n_gs],
                g_recv.at[piece * n_tp + me_t],
                {"tp": sib},
            )
        )

    def gather_relay(piece, get):
        for k in range(1, peers + 1):
            other = lax.rem(me_t + 2 * k, n_tp)
            wait_recv(
                get(other), g_send.at[piece * n_gs], g_recv.at[piece * n_tp + other], {"tp": sib}
            )
            sends.append(
                send(
                    get(other),
                    get(other),
                    g_send.at[piece * n_gs + peers + k],
                    g_recv.at[piece * n_tp + other],
                    {"tp": sib},
                )
            )

    def gather_finish(piece, get):
        for k in range(peers + 1):
            other = lax.rem(sib + 2 * k, n_tp)
            wait_recv(
                get(other), g_send.at[piece * n_gs], g_recv.at[piece * n_tp + other], {"tp": sib}
            )

    for copy in inputs[:3]:
        copy.wait()
    low_rows = lane_iota(rows) < 64
    low_quarter = lane_iota(quarter) < 64
    for j in range(n_sp // 4):
        pair = slice(j * 128, (j + 1) * 128)
        keys = k_in[:, pair].astype(f32)
        vals = v_in[:, pair].astype(f32)
        kv_out[2 * j] = jnp.where(low_rows, keys, roll_half(vals)).astype(bf16)
        kv_out[2 * j + 1] = jnp.where(low_rows, roll_half(keys), vals).astype(bf16)
        for p in range(2):
            first = q_in[p * half : p * half + quarter, pair].astype(f32)
            second = q_in[p * half + quarter : (p + 1) * half, pair].astype(f32)
            q_out[4 * j + p] = jnp.where(low_quarter, first, roll_half(second)).astype(bf16)
            q_out[4 * j + 2 + p] = jnp.where(low_quarter, roll_half(first), second).astype(bf16)

    pl.semaphore_wait(barrier, n_sp + n_tp - 2)

    for d in (6, 7, 4, 5, 2, 3, 1):
        dst = across(d)
        if d % 2 == 0 or d == 1:
            sends.append(
                send(
                    kv_out.at[dst // 2],
                    kv_buf.at[me_s],
                    a_send.at[d],
                    kv_recv.at[me_s],
                    {"sp": dst},
                )
            )
    def send_queries(ds):
        for d in ds:
            dst = across(d)
            send(
                q_out.at[dst], q_buf.at[me_s], q_send.at[d], q_recv.at[me_s], {"sp": dst}
            )

    upper = me_s // (n_sp // 2)
    inner = lax.rem(me_s // 2 + upper, 2)

    @pl.when(inner == 1)
    def _():
        send_queries((6, 7, 4, 5))

    send_queries((2, 3, 1))
    kv_buf[me_s] = kv_out[me_s // 2]
    q_buf[me_s] = q_out[me_s]

    for copy in inputs[3:]:
        copy.wait()
    eye = lax.broadcasted_iota(jnp.int32, (rows, rows), 0)
    eye_lane = lax.broadcasted_iota(jnp.int32, (rows, rows), 1)
    same = eye == eye_lane
    before_col = eye_lane < eye
    before_row = eye < eye_lane

    def as_column(row):
        return jnp.sum(jnp.where(same, row, 0.0), axis=1, keepdims=True)

    ids_row = [jnp.bitwise_xor(ids_in[c : c + 1, :], me_s).astype(f32) for c in range(2)]
    ids_col = [as_column(row) for row in ids_row]
    weight_col = [as_column(route_w[c : c + 1, :]) for c in range(2)]
    slot_row = []
    slot_col = []
    for c in range(2):
        hit = (ids_row[0] == ids_col[c]) | (ids_row[1] == ids_col[c])
        count = jnp.sum(jnp.where(hit & before_col, 1.0, 0.0), axis=1, keepdims=True)
        slot_col.append(ids_col[c] * cap + count)
        hit = (ids_col[0] == ids_row[c]) | (ids_col[1] == ids_row[c])
        count = jnp.sum(jnp.where(hit & before_row, 1.0, 0.0), axis=0, keepdims=True)
        slot_row.append(ids_row[c] * cap + count)
    slots = n_sp * cap
    slot_iota = lax.broadcasted_iota(jnp.int32, (slots, rows), 0).astype(f32)
    chosen = (slot_iota == slot_row[0]) | (slot_iota == slot_row[1])
    spread_buf[...] = jnp.where(chosen, 1.0, 0.0).astype(bf16)
    col_iota = lax.broadcasted_iota(jnp.int32, (rows, slots), 1).astype(f32)
    for c in range(2):
        pick_buf[c] = jnp.where(col_iota == slot_col[c], 1.0, 0.0).astype(bf16)
        weight_buf[c] = jnp.broadcast_to(weight_col[c], (rows, 128))
    head_lane = lax.broadcasted_iota(jnp.int32, map_w.shape, 1)
    map_here = jnp.sum(
        jnp.where(head_lane == me_s // 2, map_w[...], 0.0), axis=1, keepdims=True
    )
    gain_here = jnp.concatenate([jnp.zeros((1, 64), f32), head_g[...]], axis=1)

    parity = lax.rem(me_s, 2)
    lane_q = lane_iota(quarter)
    scale = half_dim ** (-0.5)
    row_in = lax.broadcasted_iota(jnp.int32, (half, rows), 0) + parity * half
    visible_half = lax.broadcasted_iota(jnp.int32, (half, rows), 1) <= row_in
    visible = jnp.concatenate([visible_half.astype(f32)] * 2, axis=0) > 0.5
    high_lanes = lane_iota(half) >= 64
    zero_q = jnp.zeros((quarter, 128), f32)
    first_map = lane_q < 32
    second_map = (lane_q >= 32) & (lane_q < 64)
    batch = n_sp // 2
    for d in (6, 4, 2):
        src = across(d)
        wait_recv(kv_buf.at[src], a_send.at[0], kv_recv.at[src], {"sp": src})
        sends.append(
            send(
                kv_buf.at[src],
                kv_buf.at[src],
                a_send.at[d + 1],
                kv_recv.at[src],
                {"sp": across(1)},
            )
        )
        if d == 6:

            @pl.when(inner == 0)
            def _():
                send_queries((6, 7, 4, 5))

    for i, (src, dst) in ((3, (w_gate, t_gate)), (4, (w_up, t_up))):
        loads[i].wait()
        dst[...] = src[...].T
    for s in range(n_sp):

        @pl.when(parity != s % 2)
        def _():
            wait_recv(kv_buf.at[s], a_send.at[0], kv_recv.at[s], {"sp": across(1)})

        @pl.when(me_s != s)
        def _():
            wait_recv(q_buf.at[s], q_send.at[0], q_recv.at[s], {"sp": s})

    def send_rows(s, k, start=True):
        copy = pltpu.make_async_remote_copy(
            src_ref=o_out.at[s],
            dst_ref=ho_buf.at[me_t, me_s],
            send_sem=o_send.at[k * n_sp + s],
            recv_sem=o_recv.at[k * n_sp + me_s],
            device_id={"sp": s, "tp": lax.rem(me_t + 2 * k, n_tp)},
            device_id_type=MESH,
        )
        if start:
            copy.start()
        else:
            copy.wait_send()

    def attend(start):
        steps = range(start, start + batch)
        queries = {}
        for s in steps:
            packed = q_buf[s].astype(f32)
            rolled = roll_half(packed)
            queries[s] = jnp.concatenate(
                [
                    jnp.where(first_map, packed, zero_q),
                    jnp.where(first_map, rolled, zero_q),
                    jnp.where(second_map, packed, zero_q),
                    jnp.where(second_map, rolled, zero_q),
                ],
                axis=0,
            ).astype(bf16)
        keys = {s: kv_buf[0 : s + 1].reshape((s + 1) * rows, 128) for s in steps}
        scores = {}
        for s in steps:
            raw = contract_last(queries[s], keys[s]) * scale
            diag = jnp.where(visible, raw[:, s * rows :], masked_score)
            scores[s] = jnp.concatenate([raw[:, : s * rows], diag], axis=1) if s else diag
        row_max = {s: jnp.max(scores[s], axis=1, keepdims=True) for s in steps}
        expo = {s: jnp.exp(scores[s] - row_max[s]) for s in steps}
        total = {s: jnp.sum(expo[s], axis=1, keepdims=True) for s in steps}
        acc = {
            s: jnp.dot(expo[s].astype(bf16), keys[s], preferred_element_type=f32) for s in steps
        }
        diff = {}
        for s in steps:
            summed = acc[s] / total[s]
            raw = summed[0:half] - map_here * summed[half:rows]
            diff[s] = jnp.where(high_lanes, raw, 0.0)
        for s in steps:
            squares = jnp.sum(diff[s] * diff[s], axis=1, keepdims=True) * (1.0 / 64.0)
            head = diff[s] * lax.rsqrt(squares + epsilon) * gain_here
            o_out[s] = (roll_half(head[0:quarter]) + head[quarter:half]).astype(bf16)

        for s in steps:

            @pl.when(me_s != s)
            def _():
                for k in range(peers + 1):
                    send_rows(s, k)

            @pl.when(me_s == s)
            def _():
                ho_buf[me_t, s] = o_out[s]


    @pl.when(upper == 1)
    def _():
        attend(0)
        attend(batch)

    @pl.when(upper == 0)
    def _():
        attend(batch)
        attend(0)

    split = n_sp // 2
    base = me_s // split * split

    def get_near(t):
        return ho_buf.at[t, pl.ds(base, split)]

    def get_far(t):
        return ho_buf.at[t, pl.ds(split - base, split)]

    for i, (src, dst) in ((1, (w_sgate, t_sgate)), (2, (w_sup, t_sup))):
        loads[i].wait()
        dst[...] = src[...].T
    for k in range(1, peers + 1):
        sends.append(
            send(
                ho_buf.at[me_t, me_s],
                ho_buf.at[me_t, me_s],
                g_send.at[k],
                o_recv.at[k * n_sp + me_s],
                {"tp": lax.rem(me_t + 2 * k, n_tp)},
            )
        )

    def wait_rows(d, k):
        other = across(d) if d else me_s
        from_t = lax.rem(me_t + 2 * k, n_tp)
        wait_recv(
            ho_buf.at[from_t, other],
            o_send.at[0],
            o_recv.at[k * n_sp + other],
            {"sp": other, "tp": from_t},
        )

    def pass_on(piece, get, k):
        from_t = lax.rem(me_t + 2 * k, n_tp)
        sends.append(
            send(
                get(from_t),
                get(from_t),
                g_send.at[piece * n_gs + (peers + k if k else 0)],
                g_recv.at[piece * n_tp + from_t],
                {"tp": sib},
            )
        )

    for k in range(peers + 1):
        for d in range(split, n_sp):
            wait_rows(d, k)
        pass_on(piece_far, get_far, k)
    for k in range(peers + 1):
        for d in range(0 if k else 1, split):
            wait_rows(d, k)
        pass_on(0, get_near, k)
    gather_finish(piece_far, get_far)
    gather_finish(0, get_near)

    blocks = []
    for p in range(2):
        for u in range(2):
            parts = []
            for t in range(n_tp):
                for j in range(n_sp // 4):
                    even = ho_buf[t, 4 * j + p].astype(f32)
                    odd = ho_buf[t, 4 * j + 2 + p].astype(f32)
                    if u == 0:
                        part = jnp.where(low_quarter, even, roll_half(odd))
                    else:
                        part = jnp.where(low_quarter, roll_half(even), odd)
                    parts.append(part.astype(bf16))
            blocks.append(jnp.concatenate(parts, axis=1))
    heads = jnp.concatenate(blocks, axis=0)
    loads[0].wait()
    attn = jnp.dot(heads, w_out[...], preferred_element_type=f32)
    hidden = (res_in[...].astype(f32) + attn).astype(bf16)
    hid_buf[me_t] = hidden

    def get_hid(t):
        return hid_buf.at[t]

    gather_start(1, get_hid)

    near = n_sp // 2

    def spread(lo, hi, cols):
        picked = jnp.dot(spread_buf[lo * cap : hi * cap], cols, preferred_element_type=f32)
        return picked.astype(bf16).reshape(hi - lo, cap, col_dev)

    def slot_at(d):
        return d if d < near else near + 2 * inner + 1 - d % 2

    def offset_of(e):
        if e < near:
            return e
        return (6 - 2 * inner if e < 6 else 4 + 2 * inner) + 1 - e % 2

    def source(e):
        if e < near:
            return across(e)
        side = me_s % 2 if e % 2 else 1 - me_s % 2
        return 2 * (3 * (1 - upper) if e < 6 else 2 - upper) + side

    def dispatch(d):
        e = slot_at(d)
        sends.append(
            send(
                disp_out.at[d], arr_buf.at[me_t, e], d_send.at[d], d_recv.at[e], {"sp": across(d)}
            )
        )

    def dispatch_peer(d, k):
        other = lax.rem(me_t + 2 * k, n_tp)
        i = (k - 1) * near + d
        return send(
            peer_out.at[i], arr_buf.at[other, d], p_send.at[i], p_recv.at[i], {"sp": across(d)}
        )

    def get_arr(d):
        return lambda t: arr_buf.at[t, d]

    def normalise(pieces):
        full = [piece.astype(f32) for piece in pieces]
        squares = sum(jnp.sum(piece * piece, axis=1, keepdims=True) for piece in full)
        factor = lax.rsqrt(squares * (1.0 / (n_tp * col_dev)) + epsilon)
        return jnp.concatenate(
            [
                (piece * factor * norm_g[:, t * col_dev : (t + 1) * col_dev]).astype(bf16)
                for t, piece in enumerate(full)
            ],
            axis=1,
        )

    def gated(normed, gate, up):
        gate_part = jnp.dot(normed, gate[...], preferred_element_type=f32)
        up_part = jnp.dot(normed, up[...], preferred_element_type=f32)
        return (gate_part / (1.0 + jnp.exp(-gate_part)) * up_part).astype(bf16)

    def arrive(d):
        wait_recv(arr_buf.at[me_t, d], d_send.at[d], d_recv.at[d], {"sp": source(d)})
        gather_start(2 + d, get_arr(d))

    def relay(d):
        gather_relay(2 + d, get_arr(d))

    def arrive_near(d):
        piece = 2 + d
        get = get_arr(d)
        wait_recv(get(me_t), d_send.at[d], d_recv.at[d], {"sp": across(d)})
        sends.append(
            send(
                get(me_t),
                get(me_t),
                g_send.at[piece * n_gs],
                g_recv.at[piece * n_tp + me_t],
                {"tp": sib},
            )
        )

    def arrive_peer(d):
        piece = 2 + d
        get = get_arr(d)
        for k in range(1, peers + 1):
            other = lax.rem(me_t + 2 * k, n_tp)
            i = (k - 1) * near + d
            wait_recv(get(other), p_send.at[i], p_recv.at[i], {"sp": across(d)})
            sends.append(
                send(
                    get(other),
                    get(other),
                    g_send.at[piece * n_gs + peers + k],
                    g_recv.at[piece * n_tp + other],
                    {"tp": sib},
                )
            )

    def get_sh(t):
        return sh_buf.at[t]

    def get_eh(lo, hi):
        return lambda t: eh_buf.at[t, pl.ds(lo, hi - lo)]

    piece_sh = 2 + n_sp
    piece_eh = 3 + n_sp

    def expert_up(lo, hi):
        for d in range(lo, hi):
            if d:
                gather_finish(2 + d, get_arr(d))
        count = (hi - lo) * cap
        normed = normalise([arr_buf[t, lo:hi].reshape(count, col_dev) for t in range(n_tp)])
        hidden_units = gated(normed, t_gate, t_up)
        eh_buf[me_t, lo:hi] = hidden_units.reshape(hi - lo, cap, hidden_units.shape[1])

    def start_eh(lo, hi):
        gather_start(piece_eh + lo, get_eh(lo, hi))

    def relay_eh(lo, hi):
        gather_relay(piece_eh + lo, get_eh(lo, hi))

    def expert_out(lo, hi):
        gather_finish(piece_eh + lo, get_eh(lo, hi))
        count = (hi - lo) * cap
        joined = jnp.concatenate(
            [eh_buf[t, lo:hi].reshape(count, eh_buf.shape[3]) for t in range(n_tp)], axis=1
        )
        result = jnp.dot(joined, w_down[...], preferred_element_type=f32).astype(bf16)
        res_out[lo:hi] = result.reshape(hi - lo, cap, col_dev)
        for d in range(lo, hi):
            if d == 0:
                ret_buf[0] = res_out[0]
            else:
                sends.append(
                    send(
                        res_out.at[d],
                        ret_buf.at[offset_of(d)],
                        r_send.at[d],
                        r_recv.at[offset_of(d)],
                        {"sp": source(d)},
                    )
                )

    def shared_up():
        normed_own = normalise([hid_buf[t] for t in range(n_tp)])
        sh_buf[me_t] = gated(normed_own, t_sgate, t_sup)

    def shared_down():
        shared_all = jnp.concatenate([sh_buf[t] for t in range(n_tp)], axis=1)
        shared_sum[...] = hid_buf[me_t].astype(f32) + jnp.dot(
            shared_all, w_sdown[...], preferred_element_type=f32
        )

    def own_rows():
        for t in range(n_tp):
            arr_buf[t, 0] = jnp.dot(
                spread_buf[0:cap], hid_buf[t], preferred_element_type=f32
            ).astype(bf16)

    def wait_loads():
        for copy in loads[5:]:
            copy.wait()

    def send_own():
        disp_out[near:n_sp] = spread(near, n_sp, hidden)
        for d in (4, 6, 5, 7):
            dispatch(d)
        disp_out[1:near] = spread(1, near, hidden)
        for d in range(1, near):
            dispatch(d)

    def peer_cols():
        for k in range(1, peers + 1):
            other = lax.rem(me_t + 2 * k, n_tp)
            peer_out[(k - 1) * near + 1 : k * near] = spread(1, near, hid_buf[other])
            for d in range(1, near):
                sends.append(dispatch_peer(d, k))

    send_own()
    arrive(5)
    gather_relay(1, get_hid)
    peer_cols()
    gather_finish(1, get_hid)
    arrive(4)
    relay(5)
    wait_loads()
    shared_up()
    expert_up(5, 6)
    start_eh(5, 6)
    own_rows()
    relay(4)
    arrive(7)
    expert_up(4, 5)
    start_eh(4, 5)
    relay_eh(5, 6)
    arrive(6)
    arrive_near(1)
    arrive_near(2)
    arrive_near(3)
    arrive_peer(1)
    expert_out(5, 6)
    arrive_peer(2)
    arrive_peer(3)
    relay(7)
    expert_up(0, 2)
    start_eh(0, 2)
    relay_eh(4, 5)
    expert_up(7, 8)
    start_eh(7, 8)
    expert_out(4, 5)
    relay(6)
    expert_up(2, 4)
    start_eh(2, 4)
    expert_up(6, 7)
    start_eh(6, 7)
    gather_start(piece_sh, get_sh)
    relay_eh(0, 2)
    relay_eh(7, 8)
    expert_out(0, 2)
    expert_out(7, 8)
    relay_eh(2, 4)
    relay_eh(6, 7)
    expert_out(2, 4)
    expert_out(6, 7)
    gather_relay(piece_sh, get_sh)
    gather_finish(piece_sh, get_sh)
    shared_down()
    result = shared_sum[...]
    for d in range(1, n_sp):
        wait_recv(ret_buf.at[d], r_send.at[d], r_recv.at[d], {"sp": across(d)})
    returned = ret_buf[...].reshape(slots, col_dev)
    for c in range(2):
        picked = jnp.dot(pick_buf[c], returned, preferred_element_type=f32)
        result = result + weight_buf[c][:, 0:1] * picked
    out_ref[...] = result.astype(out_ref.dtype)

    for copy in sends:
        copy.wait_send()
    for d in range(1, n_sp):
        pltpu.make_async_remote_copy(
            src_ref=q_out.at[d],
            dst_ref=q_buf.at[me_s],
            send_sem=q_send.at[d],
            recv_sem=q_recv.at[me_s],
            device_id={"sp": across(d)},
            device_id_type=MESH,
        ).wait_send()
    for s in range(n_sp):

        @pl.when(me_s != s)
        def _():
            for k in range(peers + 1):
                send_rows(s, k, start=False)


def fused_body(
    residual_in,
    query_rows,
    key_rows,
    value_rows,
    map_weight,
    head_gain,
    out_proj,
    norm_gain,
    route_ids,
    route_weights,
    expert_gate,
    expert_up,
    expert_down,
    shared_gate,
    shared_up,
    shared_down,
):
    n_sp = lax.axis_size("sp")
    n_tp = lax.axis_size("tp")
    rows, col_dev = residual_in.shape
    topk = route_ids.shape[1]
    capacity = 5 * rows * topk // (4 * n_sp)
    cap = (capacity + 15) // 16 * 16
    hid_units = shared_gate.shape[0]
    bf16 = jnp.bfloat16
    pieces = 4 + 2 * n_sp
    peer_slots = (n_tp // 2 - 1) * (n_sp // 2)
    n_gs = 1 + 2 * (n_tp // 2 - 1)
    dma = pltpu.SemaphoreType.DMA
    vmem = pl.BlockSpec(memory_space=pltpu.VMEM)
    hbm = pl.BlockSpec(memory_space=pl.ANY)
    return pl.pallas_call(
        functools.partial(layer_kernel, n_sp, n_tp),
        out_shape=pltpu.VMEM((rows, col_dev), bf16),
        in_specs=[hbm] * 16,
        out_specs=vmem,
        scratch_shapes=[
            pltpu.VMEM(out_proj.shape, bf16),
            pltpu.VMEM(expert_gate.shape[1:], bf16),
            pltpu.VMEM(expert_up.shape[1:], bf16),
            pltpu.VMEM(expert_down.shape[1:], bf16),
            pltpu.VMEM(shared_gate.shape, bf16),
            pltpu.VMEM(shared_up.shape, bf16),
            pltpu.VMEM(shared_down.shape, bf16),
            pltpu.VMEM((n_sp // 2, rows, 128), bf16),
            pltpu.VMEM((n_sp, rows // 4, 128), bf16),
            pltpu.VMEM((n_sp, rows, 128), bf16),
            pltpu.VMEM((n_sp, rows // 4, 128), bf16),
            pltpu.VMEM((n_sp, rows // 4, 128), bf16),
            pltpu.VMEM((n_tp, n_sp, rows // 4, 128), bf16),
            pltpu.VMEM((n_tp, rows, col_dev), bf16),
            pltpu.VMEM((n_sp, cap, col_dev), bf16),
            pltpu.VMEM((n_tp, n_sp, cap, col_dev), bf16),
            pltpu.VMEM((n_tp, rows, hid_units), bf16),
            pltpu.VMEM((n_tp, n_sp, cap, hid_units), bf16),
            pltpu.VMEM((n_sp, cap, col_dev), bf16),
            pltpu.VMEM((n_sp, cap, col_dev), bf16),
            pltpu.VMEM((n_sp * cap, rows), bf16),
            pltpu.VMEM((2, rows, n_sp * cap), bf16),
            pltpu.VMEM((2, rows, 128), jnp.float32),
            dma((7,)),
            dma((n_sp,)),
            dma((n_sp,)),
            dma((n_sp,)),
            dma((n_sp,)),
            dma((n_tp // 2 * n_sp,)),
            dma((n_tp // 2 * n_sp,)),
            dma((n_sp,)),
            dma((n_sp,)),
            dma((n_sp,)),
            dma((n_sp,)),
            dma((pieces * n_gs,)),
            dma((pieces * n_tp,)),
            pltpu.VMEM((peer_slots, cap, col_dev), bf16),
            dma((peer_slots,)),
            dma((peer_slots,)),
            pltpu.VMEM((rows, col_dev), jnp.float32),
            pltpu.VMEM(query_rows.shape, bf16),
            pltpu.VMEM(key_rows.shape, bf16),
            pltpu.VMEM(value_rows.shape, bf16),
            pltpu.VMEM(residual_in.shape, bf16),
            pltpu.VMEM((1,) + map_weight.shape, jnp.float32),
            pltpu.VMEM((1,) + head_gain.shape, jnp.float32),
            pltpu.VMEM((1,) + norm_gain.shape, jnp.float32),
            pltpu.VMEM((topk, rows), jnp.int32),
            pltpu.VMEM((topk, rows), jnp.float32),
            dma((9,)),
            pltpu.VMEM(expert_gate.shape[:0:-1], bf16),
            pltpu.VMEM(expert_up.shape[:0:-1], bf16),
            pltpu.VMEM(shared_gate.shape[::-1], bf16),
            pltpu.VMEM(shared_up.shape[::-1], bf16),
        ],
        compiler_params=pltpu.CompilerParams(collective_id=0, has_side_effects=True),
    )(
        query_rows,
        key_rows,
        value_rows,
        residual_in,
        map_weight[None, :],
        head_gain[None, :],
        norm_gain[None, :],
        route_ids.T,
        route_weights.T,
        out_proj,
        expert_gate,
        expert_up,
        expert_down,
        shared_gate,
        shared_up,
        shared_down,
    )


def layer(*args):
    residual_in, map_weight, head_gain, route_ids = args[0], args[4], args[5], args[8]
    fits = (
        2 * map_weight.shape[0] == lax.axis_size("sp") == 8
        and map_weight.shape[0] % 2 == 0
        and head_gain.shape[0] == 64
        and route_ids.shape[1] == 2
        and args[10].shape[0] == 1
        and residual_in.shape[0] % 64 == 0
        and residual_in.shape[1] % 128 == 0
        and args[13].shape[0] % 128 == 0
        and lax.axis_size("tp") in (4, 8)
    )
    return (fused_body if fits else body)(*args)


def solution(mesh):
    in_specs = (
        P("sp", "tp"),
        P("sp", "tp"),
        P("sp", "tp"),
        P("sp", "tp"),
        P("tp"),
        P(),
        P(None, "tp"),
        P(),
        P("sp", None),
        P("sp", None),
        P("sp", "tp", None),
        P("sp", "tp", None),
        P("sp", None, "tp"),
        P("tp", None),
        P("tp", None),
        P(None, "tp"),
    )
    out_specs = P("sp", "tp")
    return jax.shard_map(layer, mesh=mesh, in_specs=in_specs, out_specs=out_specs, check_vma=False)
```

```python
import functools

import jax
import jax.numpy as jnp
from jax import lax
from jax.experimental import pallas as pl
from jax.experimental.pallas import tpu as pltpu
from jax.sharding import PartitionSpec as P

epsilon = 1e-06
masked_score = -1e30
log2_e = 1.4426950408889634
MESH = pl.DeviceIdType.MESH


def rms_scale(values, gain_vec):
    squares = jnp.mean(values * values, axis=-1, keepdims=True)
    return values * lax.rsqrt(squares + epsilon) * gain_vec


def block_slots(route_block, experts_all, capacity):
    flat_ids = route_block.reshape(-1)
    one_hot = (flat_ids[:, None] == jnp.arange(experts_all, dtype=jnp.int32)[None, :]).astype(
        jnp.int32
    )
    earlier = jnp.cumsum(one_hot, axis=0) - one_hot
    position = jnp.sum(earlier * one_hot, axis=1)
    return (flat_ids * capacity + position).reshape(route_block.shape)


def body(
    residual_in,
    query_rows,
    key_rows,
    value_rows,
    map_weight,
    head_gain,
    out_proj,
    norm_gain,
    route_ids,
    route_weights,
    expert_gate,
    expert_up,
    expert_down,
    shared_gate,
    shared_up,
    shared_down,
):
    seq_dev = residual_in.shape[0]
    col_dev = residual_in.shape[1]
    heads_here = map_weight.shape[0]
    head_dim = head_gain.shape[0]
    half_dim = head_dim // 2
    topk_count = route_ids.shape[1]
    exp_here = expert_gate.shape[0]
    experts_all = exp_here * lax.axis_size("sp")
    capacity = 5 * seq_dev * topk_count // (4 * experts_all)
    score_scale = half_dim ** (-0.5)
    query_pos = lax.axis_index("sp") * seq_dev + jnp.arange(seq_dev, dtype=jnp.int32)
    query_heads = query_rows.reshape(seq_dev, heads_here, 2, half_dim)
    key_piece = lax.all_gather(key_rows, "sp", axis=0, tiled=True)
    value_piece = lax.all_gather(value_rows, "sp", axis=0, tiled=True)
    piece_len = key_piece.shape[0]
    key_heads = key_piece.reshape(piece_len, heads_here, 2, half_dim)
    value_heads = value_piece.reshape(piece_len, heads_here, head_dim)
    scores = (
        jnp.einsum("qhmd,khmd->mhqk", query_heads, key_heads, preferred_element_type=jnp.float32)
        * score_scale
    )
    key_pos = jnp.arange(piece_len, dtype=jnp.int32)
    visible = key_pos[None, :] <= query_pos[:, None]
    scores = jnp.where(visible, scores, masked_score)
    run_max = jnp.full((2, heads_here, seq_dev), masked_score, jnp.float32)
    new_max = jnp.maximum(run_max, jnp.max(scores, axis=-1))
    expo = jnp.where(visible, jnp.exp(scores - new_max[..., None]), 0.0)
    new_sum = jnp.sum(expo, axis=-1)
    product = jnp.einsum(
        "mhqk,khd->mhqd", expo.astype(jnp.bfloat16), value_heads, preferred_element_type=jnp.float32
    )
    summed = product / new_sum[..., None]
    diff_out = summed[0] - map_weight[:, None, None] * summed[1]
    head_out = rms_scale(diff_out, head_gain).astype(jnp.bfloat16)
    head_out = jnp.transpose(head_out, (1, 0, 2)).reshape(seq_dev, heads_here * head_dim)
    attn = jnp.dot(
        lax.all_gather(head_out, "tp", axis=1, tiled=True),
        out_proj,
        preferred_element_type=jnp.float32,
    )
    hidden_state = (residual_in.astype(jnp.float32) + attn).astype(jnp.bfloat16)
    full_rows = lax.all_gather(hidden_state, "tp", axis=1, tiled=True)
    normed = rms_scale(full_rows.astype(jnp.float32), norm_gain).astype(jnp.bfloat16)
    shared_gate_part = jnp.einsum(
        "rd,fd->rf", normed, shared_gate, preferred_element_type=jnp.float32
    )
    shared_up_part = jnp.einsum("rd,fd->rf", normed, shared_up, preferred_element_type=jnp.float32)
    shared_hidden = (jax.nn.silu(shared_gate_part) * shared_up_part).astype(jnp.bfloat16)
    slot_ids = block_slots(route_ids, experts_all, capacity)
    token_of = jnp.repeat(jnp.arange(seq_dev, dtype=jnp.int32), topk_count)
    slot_token = (
        jnp.full((experts_all * capacity,), seq_dev, jnp.int32)
        .at[slot_ids.reshape(-1)]
        .set(token_of)
    )
    own_cols = lax.dynamic_slice_in_dim(normed, lax.axis_index("tp") * col_dev, col_dev, 1)
    padded = jnp.concatenate([own_cols, jnp.zeros((1, col_dev), jnp.bfloat16)], axis=0)
    outgoing = jnp.take(padded, slot_token, axis=0).reshape(experts_all, capacity, col_dev)
    arrived = lax.all_to_all(outgoing, "sp", split_axis=0, concat_axis=1, tiled=True)
    arrived_rows = arrived.shape[1]
    pieces = lax.all_gather(arrived, "tp", axis=2, tiled=True)
    gate_add = jnp.einsum("erd,efd->erf", pieces, expert_gate, preferred_element_type=jnp.float32)
    up_add = jnp.einsum("erd,efd->erf", pieces, expert_up, preferred_element_type=jnp.float32)
    expert_hidden = (jax.nn.silu(gate_add) * up_add).astype(jnp.bfloat16)
    expert_flat = expert_hidden.reshape(exp_here * arrived_rows, expert_hidden.shape[2])
    pieces = (
        lax.all_gather(shared_hidden, "tp", axis=1, tiled=True),
        lax.all_gather(expert_flat, "tp", axis=1, tiled=True),
    )
    piece_width = pieces[0].shape[1]
    routed_piece = pieces[1].reshape(exp_here, arrived_rows, piece_width)
    shared_add = jnp.dot(pieces[0], shared_down, preferred_element_type=jnp.float32)
    expert_add = jnp.einsum(
        "erf,efd->erd", routed_piece, expert_down, preferred_element_type=jnp.float32
    )
    returned_rows = lax.all_to_all(
        expert_add.astype(jnp.bfloat16), "sp", split_axis=1, concat_axis=0, tiled=True
    )
    returned_flat = returned_rows.reshape(experts_all * capacity, col_dev)
    picked = (
        jnp.take(returned_flat, slot_ids.reshape(-1), axis=0)
        .reshape(seq_dev, topk_count, col_dev)
        .astype(jnp.float32)
    )
    routed = jnp.sum(picked * route_weights[:, :, None], axis=1)
    return (hidden_state.astype(jnp.float32) + shared_add + routed).astype(jnp.bfloat16)


def lane_iota(rows):
    return lax.broadcasted_iota(jnp.int32, (rows, 128), 1)


def roll_half(values):
    return pltpu.roll(values, 64, 1)


def contract_last(a, b):
    return lax.dot_general(a, b, (((1,), (1,)), ((), ())), preferred_element_type=jnp.float32)


def layer_kernel(
    n_sp,
    n_tp,
    q_hbm,
    k_hbm,
    v_hbm,
    res_hbm,
    map_w_hbm,
    head_g_hbm,
    norm_g_hbm,
    ids_hbm,
    route_w_hbm,
    out_proj,
    exp_gate,
    exp_up,
    exp_down,
    sh_gate,
    sh_up,
    sh_down,
    out_ref,
    w_out,
    w_gate,
    w_up,
    w_down,
    w_sgate,
    w_sup,
    w_sdown,
    kv_out,
    q_out,
    kv_buf,
    q_buf,
    o_out,
    ho_buf,
    hid_buf,
    disp_out,
    arr_buf,
    sh_buf,
    eh_buf,
    res_out,
    ret_buf,
    spread_buf,
    pick_buf,
    weight_buf,
    w_sem,
    s_sem,
    kv_recv,
    q_recv,
    o_recv,
    d_recv,
    r_recv,
    g_recv,
    p_recv,
    peer_out,
    shared_sum,
    q_in,
    k_in,
    v_in,
    res_in,
    map_w,
    head_g,
    norm_g,
    ids_in,
    route_w,
    in_sem,
    t_gate,
    t_up,
    t_sgate,
    t_sup,
):
    me_s = lax.axis_index("sp")
    me_t = lax.axis_index("tp")
    sib = me_t + 1 - 2 * lax.rem(me_t, 2)
    peers = n_tp // 2 - 1
    rows = res_in.shape[0]
    col_dev = res_in.shape[1]
    half = rows // 2
    quarter = rows // 4
    cap = arr_buf.shape[2]
    half_dim = 32
    bf16 = jnp.bfloat16
    f32 = jnp.float32

    def across(k):
        other = me_s
        for b in range(n_sp.bit_length() - 1):
            if k >> b & 1:
                bit = lax.rem(me_s // (1 << b), 2)
                other = other + (1 << b) * (1 - 2 * bit)
        return other

    barrier = pltpu.get_barrier_semaphore()
    for d in range(1, n_sp):
        pl.semaphore_signal(
            barrier, inc=1, device_id={"sp": lax.rem(me_s + d, n_sp)}, device_id_type=MESH
        )
    for d in range(1, n_tp):
        pl.semaphore_signal(
            barrier, inc=1, device_id={"tp": lax.rem(me_t + d, n_tp)}, device_id_type=MESH
        )

    inputs = []
    for i, (src, dst) in enumerate(
        (
            (q_hbm, q_in),
            (k_hbm, k_in),
            (v_hbm, v_in),
            (res_hbm, res_in),
            (map_w_hbm, map_w),
            (head_g_hbm, head_g),
            (norm_g_hbm, norm_g),
            (ids_hbm, ids_in),
            (route_w_hbm, route_w),
        )
    ):
        copy = pltpu.make_async_copy(src, dst, in_sem.at[max(0, i - 2)])
        copy.start()
        inputs.append(copy)

    loads = []
    for i, (src, dst) in enumerate(
        (
            (out_proj, w_out),
            (sh_gate, w_sgate),
            (sh_up, w_sup),
            (exp_gate.at[0], w_gate),
            (exp_up.at[0], w_up),
            (exp_down.at[0], w_down),
            (sh_down, w_sdown),
        )
    ):
        copy = pltpu.make_async_copy(src, dst, w_sem.at[i])
        copy.start()
        loads.append(copy)

    def send(src, dst, ssem, rsem, device):
        pltpu.make_async_remote_copy(
            src_ref=src,
            dst_ref=dst,
            send_sem=ssem,
            recv_sem=rsem,
            device_id=device,
            device_id_type=MESH,
        ).start()

    def waiter(ref, ssem, rsem):
        return pltpu.make_async_remote_copy(
            src_ref=ref,
            dst_ref=ref,
            send_sem=ssem,
            recv_sem=rsem,
            device_id={"tp": sib},
            device_id_type=MESH,
        )

    def wait_recv(ref, rsem):
        waiter(ref, s_sem.at[0], rsem).wait_recv()

    def peer(k):
        return lax.rem(me_t + 2 * k, n_tp)

    def origin(k):
        return lax.rem(me_t - 2 * k + n_tp, n_tp)

    def channel(i, k):
        return g_recv.at[i * (peers + 1) + k]

    def pass_on(i, kind, block):
        send(block, block, s_sem.at[kind], channel(i, 0), {"tp": sib})

    def gather_start(i, kind, get):
        for k in range(1, peers + 1):
            send(get(me_t), get(me_t), s_sem.at[kind], channel(i, k), {"tp": peer(k)})
        pass_on(i, kind, get(me_t))

    def gather_relay(i, kind, get):
        for k in range(1, peers + 1):
            wait_recv(get(origin(k)), channel(i, k))
            pass_on(i, kind, get(origin(k)))

    def gather_finish(i, get):
        wait_recv(get(pl.ds(0, peers + 1)), channel(i, 0))

    pltpu.make_async_copy(kv_buf.at[0:6], kv_buf.at[0:6], in_sem.at[0]).wait()
    low_rows = lane_iota(rows) < 64
    low_quarter = lane_iota(quarter) < 64
    for j in range(n_sp // 4):
        pair = slice(j * 128, (j + 1) * 128)
        keys = k_in[:, pair].astype(f32)
        vals = v_in[:, pair].astype(f32)
        kv_out[2 * j] = jnp.where(low_rows, keys, roll_half(vals)).astype(bf16)
        kv_out[2 * j + 1] = jnp.where(low_rows, roll_half(keys), vals).astype(bf16)
        for p in range(2):
            first = q_in[p * half : p * half + quarter, pair].astype(f32)
            second = q_in[p * half + quarter : (p + 1) * half, pair].astype(f32)
            q_out[4 * j + p] = jnp.where(low_quarter, first, roll_half(second)).astype(bf16)
            q_out[4 * j + 2 + p] = jnp.where(low_quarter, roll_half(first), second).astype(bf16)

    pl.semaphore_wait(barrier, n_sp + n_tp - 2)

    for d in (6, 4, 2, 1):
        dst = across(d)
        send(kv_out.at[dst // 2], kv_buf.at[me_s], s_sem.at[0], kv_recv.at[d // 2], {"sp": dst})

    def send_queries(ds):
        for d in ds:
            dst = across(d)
            send(q_out.at[dst], q_buf.at[me_s], s_sem.at[1], q_recv.at[0], {"sp": dst})

    upper = me_s // (n_sp // 2)
    inner = lax.rem(me_s // 2 + upper, 2)
    send_queries((2, 3, 1))
    kv_buf[me_s] = kv_out[me_s // 2]
    q_buf[me_s] = q_out[me_s]
    for copy in inputs[3:]:
        copy.wait()
    eye = lax.broadcasted_iota(jnp.int32, (rows, rows), 0)
    eye_lane = lax.broadcasted_iota(jnp.int32, (rows, rows), 1)
    same = eye == eye_lane
    before_col = eye_lane < eye
    before_row = eye < eye_lane

    def as_column(row):
        return jnp.sum(jnp.where(same, row, 0.0), axis=1, keepdims=True)

    ids_row = [jnp.bitwise_xor(ids_in[c : c + 1, :], me_s).astype(f32) for c in range(2)]
    ids_col = [as_column(row) for row in ids_row]
    weight_col = [as_column(route_w[c : c + 1, :]) for c in range(2)]
    slot_row = []
    slot_col = []
    for c in range(2):
        hit = (ids_row[0] == ids_col[c]) | (ids_row[1] == ids_col[c])
        count = jnp.sum(jnp.where(hit & before_col, 1.0, 0.0), axis=1, keepdims=True)
        slot_col.append(ids_col[c] * cap + count)
        hit = (ids_col[0] == ids_row[c]) | (ids_col[1] == ids_row[c])
        count = jnp.sum(jnp.where(hit & before_row, 1.0, 0.0), axis=0, keepdims=True)
        slot_row.append(ids_row[c] * cap + count)
    slots = n_sp * cap
    slot_iota = lax.broadcasted_iota(jnp.int32, (slots, rows), 0).astype(f32)
    chosen = (slot_iota == slot_row[0]) | (slot_iota == slot_row[1])
    spread_buf[...] = jnp.where(chosen, 1.0, 0.0).astype(bf16)
    col_iota = lax.broadcasted_iota(jnp.int32, (rows, slots), 1).astype(f32)
    for c in range(2):
        pick_buf[c] = jnp.where(col_iota == slot_col[c], 1.0, 0.0).astype(bf16)
        weight_buf[c] = jnp.broadcast_to(weight_col[c], (rows, 128))
    head_lane = lax.broadcasted_iota(jnp.int32, map_w.shape, 1)
    map_here = jnp.sum(
        jnp.where(head_lane == me_s // 2, map_w[...], 0.0), axis=1, keepdims=True
    )
    gain_here = jnp.concatenate([jnp.zeros((1, 64), f32), head_g[...]], axis=1)

    parity = lax.rem(me_s, 2)
    lane_q = lane_iota(quarter)
    scale = half_dim ** (-0.5) * log2_e
    ones_lane = lane_iota(rows) == 0
    one = jnp.ones((rows, 128), bf16)
    row_in = lax.broadcasted_iota(jnp.int32, (half, rows), 0) + parity * half
    visible_half = lax.broadcasted_iota(jnp.int32, (half, rows), 1) <= row_in
    visible = jnp.concatenate([visible_half.astype(f32)] * 2, axis=0) > 0.5
    high_lanes = lane_iota(half) >= 64
    zero_q = jnp.zeros((quarter, 128), f32)
    first_map = lane_q < 32
    second_map = (lane_q >= 32) & (lane_q < 64)
    batch = n_sp // 2
    for d in (6, 4, 2):
        src = across(d)
        wait_recv(kv_buf.at[src], kv_recv.at[d // 2])
        send(kv_buf.at[src], kv_buf.at[src], s_sem.at[0], kv_recv.at[0], {"sp": across(1)})
        if d == 6:
            send_queries((6, 7, 4, 5))
    for i, (src, dst) in ((3, (w_gate, t_gate)), (4, (w_up, t_up))):
        loads[i].wait()
        dst[...] = src[...].T
    wait_recv(kv_buf.at[0 : n_sp // 2], kv_recv.at[0])
    wait_recv(q_buf.at[0 : n_sp - 1], q_recv.at[0])
    def send_rows(s, k):
        far = lax.rem(s // batch + upper, 2)
        send(
            o_out.at[s],
            ho_buf.at[me_t, me_s],
            s_sem.at[2],
            o_recv.at[2 * k + far],
            {"sp": s, "tp": peer(k)},
        )

    def attend(start):
        steps = range(start, start + batch)
        queries = {}
        for s in steps:
            packed = q_buf[s].astype(f32)
            rolled = roll_half(packed)
            queries[s] = jnp.concatenate(
                [
                    jnp.where(first_map, packed, zero_q),
                    jnp.where(first_map, rolled, zero_q),
                    jnp.where(second_map, packed, zero_q),
                    jnp.where(second_map, rolled, zero_q),
                ],
                axis=0,
            ).astype(bf16)
        keys = {s: kv_buf[0 : s + 1].reshape((s + 1) * rows, 128) for s in steps}
        blocks = [jnp.where(ones_lane, one, kv_buf[s]) for s in range(start + batch)]
        values = {s: jnp.concatenate(blocks[: s + 1], axis=0) for s in steps}
        scores = {}
        for s in steps:
            raw = contract_last(queries[s], keys[s])
            diag = jnp.where(visible, raw[:, s * rows :], masked_score)
            scores[s] = jnp.concatenate([raw[:, : s * rows], diag], axis=1) if s else diag
        row_max = {s: jnp.max(scores[s], axis=1, keepdims=True) for s in steps}
        expo = {s: jnp.exp2(scores[s] * scale - row_max[s] * scale).astype(bf16) for s in steps}
        acc = {s: jnp.dot(expo[s], values[s], preferred_element_type=f32) for s in steps}
        diff = {}
        for s in steps:
            summed = acc[s] / acc[s][:, 0:1]
            raw = summed[0:half] - map_here * summed[half:rows]
            diff[s] = jnp.where(high_lanes, raw, 0.0)
        for s in steps:
            squares = jnp.sum(diff[s] * diff[s], axis=1, keepdims=True) * (1.0 / 64.0)
            head = diff[s] * lax.rsqrt(squares + epsilon) * gain_here
            o_out[s] = (roll_half(head[0:quarter]) + head[quarter:half]).astype(bf16)

        for s in steps:

            @pl.when(me_s != s)
            def _():
                for k in range(peers + 1):
                    send_rows(s, k)

            @pl.when(me_s == s)
            def _():
                ho_buf[me_t, s] = o_out[s]


    @pl.when(upper == 1)
    def _():
        attend(0)
        attend(batch)

    @pl.when(upper == 0)
    def _():
        attend(batch)
        attend(0)

    split = n_sp // 2
    base = me_s // split * split

    def get_near(t):
        return ho_buf.at[t, pl.ds(base, split)]

    def get_far(t):
        return ho_buf.at[t, pl.ds(split - base, split)]

    for i, (src, dst) in ((1, (w_sgate, t_sgate)), (2, (w_sup, t_sup))):
        loads[i].wait()
        dst[...] = src[...].T
    for k in range(1, peers + 1):
        block = ho_buf.at[me_t, me_s]
        send(block, block, s_sem.at[3], o_recv.at[2 * k], {"tp": peer(k)})

    for k in range(peers + 1):
        wait_recv(get_far(origin(k)), o_recv.at[2 * k + 1])
        pass_on(0, 4, get_far(origin(k)))
    for k in range(peers + 1):
        wait_recv(ho_buf.at[origin(k), 0 : split - (k == 0)], o_recv.at[2 * k])
        pass_on(1, 4, get_near(origin(k)))
    def project(j):
        blocks = []
        for p in range(2):
            for u in range(2):
                parts = []
                for t in range(n_tp):
                    even = ho_buf[t, 4 * j + p].astype(f32)
                    odd = ho_buf[t, 4 * j + 2 + p].astype(f32)
                    if u == 0:
                        part = jnp.where(low_quarter, even, roll_half(odd))
                    else:
                        part = jnp.where(low_quarter, roll_half(even), odd)
                    parts.append(part.astype(bf16))
                blocks.append(jnp.concatenate(parts, axis=1))
        heads = jnp.concatenate(blocks, axis=0)
        wide = n_sp // 4 * 128
        weights = jnp.concatenate(
            [w_out[pl.ds(pl.multiple_of(t * wide + j * 128, 128), 128), :] for t in range(n_tp)],
            axis=0,
        )
        return jnp.dot(heads, weights, preferred_element_type=f32)

    loads[0].wait()
    gather_finish(0, get_far)
    attn = project(1 - upper)
    gather_finish(1, get_near)
    attn = attn + project(upper)
    hidden = (res_in[...].astype(f32) + attn).astype(bf16)
    hid_buf[me_t] = hidden

    def get_hid(t):
        return hid_buf.at[t]

    gather_start(2, 5, get_hid)

    near = n_sp // 2

    def spread(lo, hi, cols):
        picked = jnp.dot(spread_buf[lo * cap : hi * cap], cols, preferred_element_type=f32)
        return picked.astype(bf16).reshape(hi - lo, cap, col_dev)

    def slot_at(d):
        return d if d < near else near + 2 * inner + 1 - d % 2

    def offset_of(e):
        if e < near:
            return e
        return (6 - 2 * inner if e < 6 else 4 + 2 * inner) + 1 - e % 2

    def source(e):
        if e < near:
            return across(e)
        side = me_s % 2 if e % 2 else 1 - me_s % 2
        return 2 * (3 * (1 - upper) if e < 6 else 2 - upper) + side

    def dispatch(d):
        e = slot_at(d)
        send(disp_out.at[d], arr_buf.at[me_t, e], s_sem.at[6], d_recv.at[e], {"sp": across(d)})

    def dispatch_peer(d, k):
        i = (k - 1) * (near - 1) + d - 1
        send(
            peer_out.at[i], arr_buf.at[peer(k), d], s_sem.at[7], p_recv.at[i], {"sp": across(d)}
        )

    def get_arr(d):
        return lambda t: arr_buf.at[t, d]

    def normalise(pieces):
        full = [piece.astype(f32) for piece in pieces]
        squares = sum(jnp.sum(piece * piece, axis=1, keepdims=True) for piece in full)
        factor = lax.rsqrt(squares * (1.0 / (n_tp * col_dev)) + epsilon)
        return jnp.concatenate(
            [
                (piece * factor * norm_g[:, t * col_dev : (t + 1) * col_dev]).astype(bf16)
                for t, piece in enumerate(full)
            ],
            axis=1,
        )

    def gated(normed, gate, up):
        gate_part = jnp.dot(normed, gate[...], preferred_element_type=f32)
        up_part = jnp.dot(normed, up[...], preferred_element_type=f32)
        return (gate_part / (1.0 + jnp.exp(-gate_part)) * up_part).astype(bf16)

    def arrive(e):
        wait_recv(arr_buf.at[me_t, e], d_recv.at[e])
        gather_start(2 + e, 8, get_arr(e))

    def relay(e):
        gather_relay(2 + e, 8, get_arr(e))

    def arrive_near(d):
        wait_recv(arr_buf.at[me_t, d], d_recv.at[d])
        pass_on(2 + d, 9, arr_buf.at[me_t, d])

    def arrive_peer(d):
        for k in range(1, peers + 1):
            wait_recv(arr_buf.at[peer(k), d], p_recv.at[(k - 1) * (near - 1) + d - 1])
            pass_on(2 + d, 9, arr_buf.at[peer(k), d])

    def get_sh(t):
        return sh_buf.at[t]

    def get_eh(lo, hi):
        return lambda t: eh_buf.at[t, pl.ds(lo, hi - lo)]

    piece_sh = 2 + n_sp
    piece_eh = 3 + n_sp

    def expert_up(lo, hi):
        for d in range(lo, hi):
            if d:
                gather_finish(2 + d, get_arr(d))
        count = (hi - lo) * cap
        normed = normalise([arr_buf[t, lo:hi].reshape(count, col_dev) for t in range(n_tp)])
        hidden_units = gated(normed, t_gate, t_up)
        eh_buf[me_t, lo:hi] = hidden_units.reshape(hi - lo, cap, hidden_units.shape[1])

    def start_eh(lo, hi):
        gather_start(piece_eh + lo, 10, get_eh(lo, hi))

    def relay_eh(lo, hi):
        gather_relay(piece_eh + lo, 10, get_eh(lo, hi))

    def expert_out(lo, hi):
        gather_finish(piece_eh + lo, get_eh(lo, hi))
        count = (hi - lo) * cap
        joined = jnp.concatenate(
            [eh_buf[t, lo:hi].reshape(count, eh_buf.shape[3]) for t in range(n_tp)], axis=1
        )
        result = jnp.dot(joined, w_down[...], preferred_element_type=f32).astype(bf16)
        res_out[lo:hi] = result.reshape(hi - lo, cap, col_dev)
        for d in range(lo, hi):
            if d == 0:
                ret_buf[0] = res_out[0]
            else:
                send(
                    res_out.at[d],
                    ret_buf.at[offset_of(d)],
                    s_sem.at[11],
                    r_recv.at[0],
                    {"sp": source(d)},
                )

    def shared_up():
        normed_own = normalise([hid_buf[t] for t in range(n_tp)])
        sh_buf[me_t] = gated(normed_own, t_sgate, t_sup)

    def shared_down():
        shared_all = jnp.concatenate([sh_buf[t] for t in range(n_tp)], axis=1)
        shared_sum[...] = hid_buf[me_t].astype(f32) + jnp.dot(
            shared_all, w_sdown[...], preferred_element_type=f32
        )

    def own_rows():
        for t in range(n_tp):
            arr_buf[t, 0] = jnp.dot(
                spread_buf[0:cap], hid_buf[t], preferred_element_type=f32
            ).astype(bf16)

    def wait_loads():
        for copy in loads[5:]:
            copy.wait()

    def send_own():
        for d in (4, 6, 5, 7):
            disp_out[d : d + 1] = spread(d, d + 1, hidden)
            dispatch(d)
        disp_out[1:near] = spread(1, near, hidden)
        for d in range(1, near):
            dispatch(d)

    def peer_cols():
        for k in range(1, peers + 1):
            other = lax.rem(me_t + 2 * k, n_tp)
            peer_out[(k - 1) * (near - 1) : k * (near - 1)] = spread(1, near, hid_buf[other])
            for d in range(1, near):
                dispatch_peer(d, k)

    send_own()
    arrive(5)
    gather_relay(2, 5, get_hid)
    peer_cols()
    gather_finish(2, get_hid)
    arrive(4)
    relay(5)
    wait_loads()
    shared_up()
    expert_up(5, 6)
    start_eh(5, 6)
    own_rows()
    arrive(7)
    relay(4)
    expert_up(4, 5)
    start_eh(4, 5)
    relay_eh(5, 6)
    arrive(6)
    arrive_near(1)
    arrive_near(2)
    arrive_near(3)
    arrive_peer(1)
    expert_out(5, 6)
    arrive_peer(2)
    arrive_peer(3)
    relay(7)
    expert_up(0, 2)
    start_eh(0, 2)
    relay_eh(4, 5)
    expert_up(7, 8)
    start_eh(7, 8)
    expert_out(4, 5)
    relay(6)
    expert_up(2, 4)
    start_eh(2, 4)
    expert_up(6, 7)
    start_eh(6, 7)
    gather_start(piece_sh, 12, get_sh)
    relay_eh(0, 2)
    relay_eh(7, 8)
    expert_out(0, 2)
    expert_out(7, 8)
    relay_eh(2, 4)
    relay_eh(6, 7)
    expert_out(6, 7)
    expert_out(2, 4)
    gather_relay(piece_sh, 12, get_sh)
    gather_finish(piece_sh, get_sh)
    shared_down()
    result = shared_sum[...]
    wait_recv(ret_buf.at[0 : n_sp - 1], r_recv.at[0])
    returned = ret_buf[...].reshape(slots, col_dev)
    for c in range(2):
        picked = jnp.dot(pick_buf[c], returned, preferred_element_type=f32)
        result = result + weight_buf[c][:, 0:1] * picked
    out_ref[...] = result.astype(out_ref.dtype)

    hops = 2 * peers + 1
    for i, ref in enumerate(
        (
            kv_buf.at[0 : n_sp - 1],
            q_buf.at[0 : n_sp - 1],
            ho_buf.at[0 : peers + 1, 0 : n_sp - 1],
            ho_buf.at[0:peers, 0],
            ho_buf.at[0 : peers + 1],
            hid_buf.at[0:hops],
            disp_out.at[1:n_sp],
            peer_out,
            arr_buf.at[0:hops, near:n_sp],
            arr_buf.at[0 : peers + 1, 1:near],
            eh_buf.at[0:hops],
            ret_buf.at[1:n_sp],
            sh_buf.at[0:hops],
        )
    ):
        waiter(ref, s_sem.at[i], kv_recv.at[0]).wait_send()


def fused_body(
    residual_in,
    query_rows,
    key_rows,
    value_rows,
    map_weight,
    head_gain,
    out_proj,
    norm_gain,
    route_ids,
    route_weights,
    expert_gate,
    expert_up,
    expert_down,
    shared_gate,
    shared_up,
    shared_down,
):
    n_sp = lax.axis_size("sp")
    n_tp = lax.axis_size("tp")
    rows, col_dev = residual_in.shape
    topk = route_ids.shape[1]
    capacity = 5 * rows * topk // (4 * n_sp)
    cap = (capacity + 15) // 16 * 16
    hid_units = shared_gate.shape[0]
    bf16 = jnp.bfloat16
    peer_slots = (n_tp // 2 - 1) * (n_sp // 2 - 1)
    dma = pltpu.SemaphoreType.DMA
    vmem = pl.BlockSpec(memory_space=pltpu.VMEM)
    hbm = pl.BlockSpec(memory_space=pl.ANY)
    return pl.pallas_call(
        functools.partial(layer_kernel, n_sp, n_tp),
        out_shape=pltpu.VMEM((rows, col_dev), bf16),
        in_specs=[hbm] * 16,
        out_specs=vmem,
        scratch_shapes=[
            pltpu.VMEM(out_proj.shape, bf16),
            pltpu.VMEM(expert_gate.shape[1:], bf16),
            pltpu.VMEM(expert_up.shape[1:], bf16),
            pltpu.VMEM(expert_down.shape[1:], bf16),
            pltpu.VMEM(shared_gate.shape, bf16),
            pltpu.VMEM(shared_up.shape, bf16),
            pltpu.VMEM(shared_down.shape, bf16),
            pltpu.VMEM((n_sp // 2, rows, 128), bf16),
            pltpu.VMEM((n_sp, rows // 4, 128), bf16),
            pltpu.VMEM((n_sp, rows, 128), bf16),
            pltpu.VMEM((n_sp, rows // 4, 128), bf16),
            pltpu.VMEM((n_sp, rows // 4, 128), bf16),
            pltpu.VMEM((n_tp, n_sp, rows // 4, 128), bf16),
            pltpu.VMEM((n_tp, rows, col_dev), bf16),
            pltpu.VMEM((n_sp, cap, col_dev), bf16),
            pltpu.VMEM((n_tp, n_sp, cap, col_dev), bf16),
            pltpu.VMEM((n_tp, rows, hid_units), bf16),
            pltpu.VMEM((n_tp, n_sp, cap, hid_units), bf16),
            pltpu.VMEM((n_sp, cap, col_dev), bf16),
            pltpu.VMEM((n_sp, cap, col_dev), bf16),
            pltpu.VMEM((n_sp * cap, rows), bf16),
            pltpu.VMEM((2, rows, n_sp * cap), bf16),
            pltpu.VMEM((2, rows, 128), jnp.float32),
            dma((7,)),
            dma((13,)),
            dma((n_sp // 2,)),
            dma((1,)),
            dma((n_tp,)),
            dma((n_sp,)),
            dma((1,)),
            dma(((3 + 2 * n_sp) * (n_tp // 2),)),
            dma((peer_slots,)),
            pltpu.VMEM((peer_slots, cap, col_dev), bf16),
            pltpu.VMEM((rows, col_dev), jnp.float32),
            pltpu.VMEM(query_rows.shape, bf16),
            pltpu.VMEM(key_rows.shape, bf16),
            pltpu.VMEM(value_rows.shape, bf16),
            pltpu.VMEM(residual_in.shape, bf16),
            pltpu.VMEM((1,) + map_weight.shape, jnp.float32),
            pltpu.VMEM((1,) + head_gain.shape, jnp.float32),
            pltpu.VMEM((1,) + norm_gain.shape, jnp.float32),
            pltpu.VMEM((topk, rows), jnp.int32),
            pltpu.VMEM((topk, rows), jnp.float32),
            dma((7,)),
            pltpu.VMEM(expert_gate.shape[:0:-1], bf16),
            pltpu.VMEM(expert_up.shape[:0:-1], bf16),
            pltpu.VMEM(shared_gate.shape[::-1], bf16),
            pltpu.VMEM(shared_up.shape[::-1], bf16),
        ],
        compiler_params=pltpu.CompilerParams(collective_id=0, has_side_effects=True),
    )(
        query_rows,
        key_rows,
        value_rows,
        residual_in,
        map_weight[None, :],
        head_gain[None, :],
        norm_gain[None, :],
        route_ids.T,
        route_weights.T,
        out_proj,
        expert_gate,
        expert_up,
        expert_down,
        shared_gate,
        shared_up,
        shared_down,
    )


def layer(*args):
    residual_in, map_weight, head_gain, route_ids = args[0], args[4], args[5], args[8]
    fits = (
        2 * map_weight.shape[0] == lax.axis_size("sp") == 8
        and map_weight.shape[0] % 2 == 0
        and head_gain.shape[0] == 64
        and route_ids.shape[1] == 2
        and args[10].shape[0] == 1
        and residual_in.shape[0] % 64 == 0
        and residual_in.shape[1] % 128 == 0
        and args[13].shape[0] % 128 == 0
        and lax.axis_size("tp") in (4, 8)
    )
    return (fused_body if fits else body)(*args)


def solution(mesh):
    in_specs = (
        P("sp", "tp"),
        P("sp", "tp"),
        P("sp", "tp"),
        P("sp", "tp"),
        P("tp"),
        P(),
        P(None, "tp"),
        P(),
        P("sp", None),
        P("sp", None),
        P("sp", "tp", None),
        P("sp", "tp", None),
        P("sp", None, "tp"),
        P("tp", None),
        P("tp", None),
        P(None, "tp"),
    )
    out_specs = P("sp", "tp")
    return jax.shard_map(layer, mesh=mesh, in_specs=in_specs, out_specs=out_specs, check_vma=False)
```

```python
import functools

import jax
import jax.numpy as jnp
from jax import lax
from jax.experimental import pallas as pl
from jax.experimental.pallas import tpu as pltpu
from jax.sharding import PartitionSpec as P

epsilon = 1e-06
masked_score = -1e30
log2_e = 1.4426950408889634
MESH = pl.DeviceIdType.MESH


def rms_scale(values, gain_vec):
    squares = jnp.mean(values * values, axis=-1, keepdims=True)
    return values * lax.rsqrt(squares + epsilon) * gain_vec


def block_slots(route_block, experts_all, capacity):
    flat_ids = route_block.reshape(-1)
    one_hot = (flat_ids[:, None] == jnp.arange(experts_all, dtype=jnp.int32)[None, :]).astype(
        jnp.int32
    )
    earlier = jnp.cumsum(one_hot, axis=0) - one_hot
    position = jnp.sum(earlier * one_hot, axis=1)
    return (flat_ids * capacity + position).reshape(route_block.shape)


def body(
    residual_in,
    query_rows,
    key_rows,
    value_rows,
    map_weight,
    head_gain,
    out_proj,
    norm_gain,
    route_ids,
    route_weights,
    expert_gate,
    expert_up,
    expert_down,
    shared_gate,
    shared_up,
    shared_down,
):
    seq_dev = residual_in.shape[0]
    col_dev = residual_in.shape[1]
    heads_here = map_weight.shape[0]
    head_dim = head_gain.shape[0]
    half_dim = head_dim // 2
    topk_count = route_ids.shape[1]
    exp_here = expert_gate.shape[0]
    experts_all = exp_here * lax.axis_size("sp")
    capacity = 5 * seq_dev * topk_count // (4 * experts_all)
    score_scale = half_dim ** (-0.5)
    query_pos = lax.axis_index("sp") * seq_dev + jnp.arange(seq_dev, dtype=jnp.int32)
    query_heads = query_rows.reshape(seq_dev, heads_here, 2, half_dim)
    key_piece = lax.all_gather(key_rows, "sp", axis=0, tiled=True)
    value_piece = lax.all_gather(value_rows, "sp", axis=0, tiled=True)
    piece_len = key_piece.shape[0]
    key_heads = key_piece.reshape(piece_len, heads_here, 2, half_dim)
    value_heads = value_piece.reshape(piece_len, heads_here, head_dim)
    scores = (
        jnp.einsum("qhmd,khmd->mhqk", query_heads, key_heads, preferred_element_type=jnp.float32)
        * score_scale
    )
    key_pos = jnp.arange(piece_len, dtype=jnp.int32)
    visible = key_pos[None, :] <= query_pos[:, None]
    scores = jnp.where(visible, scores, masked_score)
    run_max = jnp.full((2, heads_here, seq_dev), masked_score, jnp.float32)
    new_max = jnp.maximum(run_max, jnp.max(scores, axis=-1))
    expo = jnp.where(visible, jnp.exp(scores - new_max[..., None]), 0.0)
    new_sum = jnp.sum(expo, axis=-1)
    product = jnp.einsum(
        "mhqk,khd->mhqd", expo.astype(jnp.bfloat16), value_heads, preferred_element_type=jnp.float32
    )
    summed = product / new_sum[..., None]
    diff_out = summed[0] - map_weight[:, None, None] * summed[1]
    head_out = rms_scale(diff_out, head_gain).astype(jnp.bfloat16)
    head_out = jnp.transpose(head_out, (1, 0, 2)).reshape(seq_dev, heads_here * head_dim)
    attn = jnp.dot(
        lax.all_gather(head_out, "tp", axis=1, tiled=True),
        out_proj,
        preferred_element_type=jnp.float32,
    )
    hidden_state = (residual_in.astype(jnp.float32) + attn).astype(jnp.bfloat16)
    full_rows = lax.all_gather(hidden_state, "tp", axis=1, tiled=True)
    normed = rms_scale(full_rows.astype(jnp.float32), norm_gain).astype(jnp.bfloat16)
    shared_gate_part = jnp.einsum(
        "rd,fd->rf", normed, shared_gate, preferred_element_type=jnp.float32
    )
    shared_up_part = jnp.einsum("rd,fd->rf", normed, shared_up, preferred_element_type=jnp.float32)
    shared_hidden = (jax.nn.silu(shared_gate_part) * shared_up_part).astype(jnp.bfloat16)
    slot_ids = block_slots(route_ids, experts_all, capacity)
    token_of = jnp.repeat(jnp.arange(seq_dev, dtype=jnp.int32), topk_count)
    slot_token = (
        jnp.full((experts_all * capacity,), seq_dev, jnp.int32)
        .at[slot_ids.reshape(-1)]
        .set(token_of)
    )
    own_cols = lax.dynamic_slice_in_dim(normed, lax.axis_index("tp") * col_dev, col_dev, 1)
    padded = jnp.concatenate([own_cols, jnp.zeros((1, col_dev), jnp.bfloat16)], axis=0)
    outgoing = jnp.take(padded, slot_token, axis=0).reshape(experts_all, capacity, col_dev)
    arrived = lax.all_to_all(outgoing, "sp", split_axis=0, concat_axis=1, tiled=True)
    arrived_rows = arrived.shape[1]
    pieces = lax.all_gather(arrived, "tp", axis=2, tiled=True)
    gate_add = jnp.einsum("erd,efd->erf", pieces, expert_gate, preferred_element_type=jnp.float32)
    up_add = jnp.einsum("erd,efd->erf", pieces, expert_up, preferred_element_type=jnp.float32)
    expert_hidden = (jax.nn.silu(gate_add) * up_add).astype(jnp.bfloat16)
    expert_flat = expert_hidden.reshape(exp_here * arrived_rows, expert_hidden.shape[2])
    pieces = (
        lax.all_gather(shared_hidden, "tp", axis=1, tiled=True),
        lax.all_gather(expert_flat, "tp", axis=1, tiled=True),
    )
    piece_width = pieces[0].shape[1]
    routed_piece = pieces[1].reshape(exp_here, arrived_rows, piece_width)
    shared_add = jnp.dot(pieces[0], shared_down, preferred_element_type=jnp.float32)
    expert_add = jnp.einsum(
        "erf,efd->erd", routed_piece, expert_down, preferred_element_type=jnp.float32
    )
    returned_rows = lax.all_to_all(
        expert_add.astype(jnp.bfloat16), "sp", split_axis=1, concat_axis=0, tiled=True
    )
    returned_flat = returned_rows.reshape(experts_all * capacity, col_dev)
    picked = (
        jnp.take(returned_flat, slot_ids.reshape(-1), axis=0)
        .reshape(seq_dev, topk_count, col_dev)
        .astype(jnp.float32)
    )
    routed = jnp.sum(picked * route_weights[:, :, None], axis=1)
    return (hidden_state.astype(jnp.float32) + shared_add + routed).astype(jnp.bfloat16)


def lane_iota(rows):
    return lax.broadcasted_iota(jnp.int32, (rows, 128), 1)


def roll_half(values):
    return pltpu.roll(values, 64, 1)


def contract_last(a, b):
    return lax.dot_general(a, b, (((1,), (1,)), ((), ())), preferred_element_type=jnp.float32)


def layer_kernel(
    n_sp,
    n_tp,
    q_hbm,
    k_hbm,
    v_hbm,
    res_hbm,
    map_w_hbm,
    head_g_hbm,
    norm_g_hbm,
    ids_hbm,
    route_w_hbm,
    out_proj,
    exp_gate,
    exp_up,
    exp_down,
    sh_gate,
    sh_up,
    sh_down,
    out_ref,
    w_out,
    w_gate,
    w_up,
    w_down,
    w_sgate,
    w_sup,
    w_sdown,
    kv_out,
    q_out,
    kv_buf,
    q_buf,
    o_out,
    ho_buf,
    hid_buf,
    disp_out,
    arr_buf,
    sh_buf,
    eh_buf,
    res_out,
    ret_buf,
    spread_buf,
    pick_buf,
    weight_buf,
    w_sem,
    s_sem,
    kv_recv,
    q_recv,
    o_recv,
    d_recv,
    r_recv,
    g_recv,
    p_recv,
    peer_out,
    shared_sum,
    q_in,
    k_in,
    v_in,
    res_in,
    map_w,
    head_g,
    norm_g,
    ids_in,
    route_w,
    in_sem,
    t_gate,
    t_up,
    t_sgate,
    t_sup,
):
    me_s = lax.axis_index("sp")
    me_t = lax.axis_index("tp")
    sib = me_t + 1 - 2 * lax.rem(me_t, 2)
    peers = n_tp // 2 - 1
    rows = res_in.shape[0]
    col_dev = res_in.shape[1]
    half = rows // 2
    quarter = rows // 4
    cap = arr_buf.shape[2]
    half_dim = 32
    bf16 = jnp.bfloat16
    f32 = jnp.float32

    def across(k):
        other = me_s
        for b in range(n_sp.bit_length() - 1):
            if k >> b & 1:
                bit = lax.rem(me_s // (1 << b), 2)
                other = other + (1 << b) * (1 - 2 * bit)
        return other

    barrier = pltpu.get_barrier_semaphore()
    for d in range(1, n_sp):
        pl.semaphore_signal(
            barrier, inc=1, device_id={"sp": lax.rem(me_s + d, n_sp)}, device_id_type=MESH
        )
    for d in range(1, n_tp):
        pl.semaphore_signal(
            barrier, inc=1, device_id={"tp": lax.rem(me_t + d, n_tp)}, device_id_type=MESH
        )

    inputs = []
    for i, (src, dst) in enumerate(
        (
            (q_hbm, q_in),
            (k_hbm, k_in),
            (v_hbm, v_in),
            (res_hbm, res_in),
            (map_w_hbm, map_w),
            (head_g_hbm, head_g),
            (norm_g_hbm, norm_g),
            (ids_hbm, ids_in),
            (route_w_hbm, route_w),
        )
    ):
        copy = pltpu.make_async_copy(src, dst, in_sem.at[max(0, i - 2)])
        copy.start()
        inputs.append(copy)

    loads = []
    for i, (src, dst) in enumerate(
        (
            (out_proj, w_out),
            (sh_gate, w_sgate),
            (sh_up, w_sup),
            (exp_gate.at[0], w_gate),
            (exp_up.at[0], w_up),
            (exp_down.at[0], w_down),
            (sh_down, w_sdown),
        )
    ):
        copy = pltpu.make_async_copy(src, dst, w_sem.at[i])
        copy.start()
        loads.append(copy)

    def send(src, dst, ssem, rsem, device):
        pltpu.make_async_remote_copy(
            src_ref=src,
            dst_ref=dst,
            send_sem=ssem,
            recv_sem=rsem,
            device_id=device,
            device_id_type=MESH,
        ).start()

    def waiter(ref, ssem, rsem):
        return pltpu.make_async_remote_copy(
            src_ref=ref,
            dst_ref=ref,
            send_sem=ssem,
            recv_sem=rsem,
            device_id={"tp": sib},
            device_id_type=MESH,
        )

    def wait_recv(ref, rsem):
        waiter(ref, s_sem.at[0], rsem).wait_recv()

    def peer(k):
        return lax.rem(me_t + 2 * k, n_tp)

    def origin(k):
        return lax.rem(me_t - 2 * k + n_tp, n_tp)

    def channel(i, k):
        return g_recv.at[i * (peers + 1) + k]

    def pass_on(i, kind, block):
        send(block, block, s_sem.at[kind], channel(i, 0), {"tp": sib})

    def gather_start(i, kind, get):
        for k in range(1, peers + 1):
            send(get(me_t), get(me_t), s_sem.at[kind], channel(i, k), {"tp": peer(k)})
        pass_on(i, kind, get(me_t))

    def gather_relay(i, kind, get):
        for k in range(1, peers + 1):
            wait_recv(get(origin(k)), channel(i, k))
            pass_on(i, kind, get(origin(k)))

    def gather_finish(i, get):
        wait_recv(get(pl.ds(0, peers + 1)), channel(i, 0))

    pltpu.make_async_copy(kv_buf.at[0:6], kv_buf.at[0:6], in_sem.at[0]).wait()
    low_rows = lane_iota(rows) < 64
    low_quarter = lane_iota(quarter) < 64
    for j in range(n_sp // 4):
        pair = slice(j * 128, (j + 1) * 128)
        keys = k_in[:, pair].astype(f32)
        vals = v_in[:, pair].astype(f32)
        kv_out[2 * j] = jnp.where(low_rows, keys, roll_half(vals)).astype(bf16)
        kv_out[2 * j + 1] = jnp.where(low_rows, roll_half(keys), vals).astype(bf16)
        for p in range(2):
            first = q_in[p * half : p * half + quarter, pair].astype(f32)
            second = q_in[p * half + quarter : (p + 1) * half, pair].astype(f32)
            q_out[4 * j + p] = jnp.where(low_quarter, first, roll_half(second)).astype(bf16)
            q_out[4 * j + 2 + p] = jnp.where(low_quarter, roll_half(first), second).astype(bf16)

    pl.semaphore_wait(barrier, n_sp + n_tp - 2)

    for d in (6, 4, 2, 3, 1):
        dst = across(d)
        part = kv_recv.at[0 if d % 2 else d // 2]
        send(kv_out.at[dst // 2], kv_buf.at[me_s], s_sem.at[0], part, {"sp": dst})

    def send_queries(ds):
        for d in ds:
            dst = across(d)
            send(q_out.at[dst], q_buf.at[me_s], s_sem.at[1], q_recv.at[0], {"sp": dst})

    upper = me_s // (n_sp // 2)
    inner = lax.rem(me_s // 2 + upper, 2)
    send_queries((2, 3, 1))
    kv_buf[me_s] = kv_out[me_s // 2]
    q_buf[me_s] = q_out[me_s]
    for copy in inputs[3:]:
        copy.wait()
    eye = lax.broadcasted_iota(jnp.int32, (rows, rows), 0)
    eye_lane = lax.broadcasted_iota(jnp.int32, (rows, rows), 1)
    same = eye == eye_lane
    before_col = eye_lane < eye
    before_row = eye < eye_lane

    def as_column(row):
        return jnp.sum(jnp.where(same, row, 0.0), axis=1, keepdims=True)

    ids_row = [jnp.bitwise_xor(ids_in[c : c + 1, :], me_s).astype(f32) for c in range(2)]
    ids_col = [as_column(row) for row in ids_row]
    weight_col = [as_column(route_w[c : c + 1, :]) for c in range(2)]
    slot_row = []
    slot_col = []
    for c in range(2):
        hit = (ids_row[0] == ids_col[c]) | (ids_row[1] == ids_col[c])
        count = jnp.sum(jnp.where(hit & before_col, 1.0, 0.0), axis=1, keepdims=True)
        slot_col.append(ids_col[c] * cap + count)
        hit = (ids_col[0] == ids_row[c]) | (ids_col[1] == ids_row[c])
        count = jnp.sum(jnp.where(hit & before_row, 1.0, 0.0), axis=0, keepdims=True)
        slot_row.append(ids_row[c] * cap + count)
    slots = n_sp * cap
    slot_iota = lax.broadcasted_iota(jnp.int32, (slots, rows), 0).astype(f32)
    chosen = (slot_iota == slot_row[0]) | (slot_iota == slot_row[1])
    spread_buf[...] = jnp.where(chosen, 1.0, 0.0).astype(bf16)
    col_iota = lax.broadcasted_iota(jnp.int32, (rows, slots), 1).astype(f32)
    for c in range(2):
        pick_buf[c] = jnp.where(col_iota == slot_col[c], 1.0, 0.0).astype(bf16)
        weight_buf[c] = jnp.broadcast_to(weight_col[c], (rows, 128))
    head_lane = lax.broadcasted_iota(jnp.int32, map_w.shape, 1)
    map_here = jnp.sum(
        jnp.where(head_lane == me_s // 2, map_w[...], 0.0), axis=1, keepdims=True
    )
    gain_here = jnp.concatenate([jnp.zeros((1, 64), f32), head_g[...]], axis=1)

    parity = lax.rem(me_s, 2)
    lane_q = lane_iota(quarter)
    scale = half_dim ** (-0.5) * log2_e
    ones_lane = lane_iota(rows) == 0
    one = jnp.ones((rows, 128), bf16)
    row_in = lax.broadcasted_iota(jnp.int32, (half, rows), 0) + parity * half
    visible_half = lax.broadcasted_iota(jnp.int32, (half, rows), 1) <= row_in
    visible = jnp.concatenate([visible_half.astype(f32)] * 2, axis=0) > 0.5
    high_lanes = lane_iota(half) >= 64
    zero_q = jnp.zeros((quarter, 128), f32)
    first_map = lane_q < 32
    second_map = (lane_q >= 32) & (lane_q < 64)
    batch = n_sp // 2
    for d in (6, 4, 2):
        src = across(d)
        wait_recv(kv_buf.at[src], kv_recv.at[d // 2])
        if d > 2:
            send(kv_buf.at[src], kv_buf.at[src], s_sem.at[0], kv_recv.at[0], {"sp": across(1)})
        if d == 6:
            send_queries((6, 7, 4, 5))
    for i, (src, dst) in ((3, (w_gate, t_gate)), (4, (w_up, t_up))):
        loads[i].wait()
        dst[...] = src[...].T
    wait_recv(kv_buf.at[0 : n_sp // 2], kv_recv.at[0])
    wait_recv(q_buf.at[0 : n_sp - 1], q_recv.at[0])
    def send_rows(s, k):
        far = lax.rem(s // batch + upper, 2)
        send(
            o_out.at[s],
            ho_buf.at[me_t, me_s],
            s_sem.at[2],
            o_recv.at[2 * k + far],
            {"sp": s, "tp": peer(k)},
        )

    def attend(start):
        steps = range(start, start + batch)
        queries = {}
        for s in steps:
            packed = q_buf[s].astype(f32)
            rolled = roll_half(packed)
            queries[s] = jnp.concatenate(
                [
                    jnp.where(first_map, packed, zero_q),
                    jnp.where(first_map, rolled, zero_q),
                    jnp.where(second_map, packed, zero_q),
                    jnp.where(second_map, rolled, zero_q),
                ],
                axis=0,
            ).astype(bf16)
        keys = {s: kv_buf[0 : s + 1].reshape((s + 1) * rows, 128) for s in steps}
        blocks = [jnp.where(ones_lane, one, kv_buf[s]) for s in range(start + batch)]
        values = {s: jnp.concatenate(blocks[: s + 1], axis=0) for s in steps}
        scores = {}
        for s in steps:
            raw = contract_last(queries[s], keys[s])
            diag = jnp.where(visible, raw[:, s * rows :], masked_score)
            scores[s] = jnp.concatenate([raw[:, : s * rows], diag], axis=1) if s else diag
        row_max = {s: jnp.max(scores[s], axis=1, keepdims=True) for s in steps}
        expo = {s: jnp.exp2(scores[s] * scale - row_max[s] * scale).astype(bf16) for s in steps}
        acc = {s: jnp.dot(expo[s], values[s], preferred_element_type=f32) for s in steps}
        diff = {}
        for s in steps:
            summed = acc[s] / acc[s][:, 0:1]
            raw = summed[0:half] - map_here * summed[half:rows]
            diff[s] = jnp.where(high_lanes, raw, 0.0)
        for s in steps:
            squares = jnp.sum(diff[s] * diff[s], axis=1, keepdims=True) * (1.0 / 64.0)
            head = diff[s] * lax.rsqrt(squares + epsilon) * gain_here
            o_out[s] = (roll_half(head[0:quarter]) + head[quarter:half]).astype(bf16)

        for s in steps:

            @pl.when(me_s != s)
            def _():
                for k in range(peers + 1):
                    send_rows(s, k)

            @pl.when(me_s == s)
            def _():
                ho_buf[me_t, s] = o_out[s]


    @pl.when(upper == 1)
    def _():
        attend(0)
        attend(batch)

    @pl.when(upper == 0)
    def _():
        attend(batch)
        attend(0)

    split = n_sp // 2
    base = me_s // split * split

    def get_near(t):
        return ho_buf.at[t, pl.ds(base, split)]

    def get_far(t):
        return ho_buf.at[t, pl.ds(split - base, split)]

    for i, (src, dst) in ((1, (w_sgate, t_sgate)), (2, (w_sup, t_sup))):
        loads[i].wait()
        dst[...] = src[...].T
    for k in range(1, peers + 1):
        block = ho_buf.at[me_t, me_s]
        send(block, block, s_sem.at[3], o_recv.at[2 * k], {"tp": peer(k)})

    for k in range(peers + 1):
        wait_recv(get_far(origin(k)), o_recv.at[2 * k + 1])
        pass_on(0, 4, get_far(origin(k)))
    for k in range(peers + 1):
        wait_recv(ho_buf.at[origin(k), 0 : split - (k == 0)], o_recv.at[2 * k])
        pass_on(1, 4, get_near(origin(k)))
    def project(j):
        blocks = []
        for p in range(2):
            for u in range(2):
                parts = []
                for t in range(n_tp):
                    even = ho_buf[t, 4 * j + p].astype(f32)
                    odd = ho_buf[t, 4 * j + 2 + p].astype(f32)
                    if u == 0:
                        part = jnp.where(low_quarter, even, roll_half(odd))
                    else:
                        part = jnp.where(low_quarter, roll_half(even), odd)
                    parts.append(part.astype(bf16))
                blocks.append(jnp.concatenate(parts, axis=1))
        heads = jnp.concatenate(blocks, axis=0)
        wide = n_sp // 4 * 128
        weights = jnp.concatenate(
            [w_out[pl.ds(pl.multiple_of(t * wide + j * 128, 128), 128), :] for t in range(n_tp)],
            axis=0,
        )
        return jnp.dot(heads, weights, preferred_element_type=f32)

    loads[0].wait()
    gather_finish(0, get_far)
    attn = project(1 - upper)
    gather_finish(1, get_near)
    attn = attn + project(upper)
    hidden = (res_in[...].astype(f32) + attn).astype(bf16)
    hid_buf[me_t] = hidden

    def get_hid(t):
        return hid_buf.at[t]

    gather_start(2, 5, get_hid)

    near = n_sp // 2

    def spread(lo, hi, cols):
        picked = jnp.dot(spread_buf[lo * cap : hi * cap], cols, preferred_element_type=f32)
        return picked.astype(bf16).reshape(hi - lo, cap, col_dev)

    def slot_at(d):
        return d if d < near else near + 2 * inner + 1 - d % 2

    def offset_of(e):
        if e < near:
            return e
        return (6 - 2 * inner if e < 6 else 4 + 2 * inner) + 1 - e % 2

    def source(e):
        if e < near:
            return across(e)
        side = me_s % 2 if e % 2 else 1 - me_s % 2
        return 2 * (3 * (1 - upper) if e < 6 else 2 - upper) + side

    def dispatch(d):
        e = slot_at(d)
        send(disp_out.at[d], arr_buf.at[me_t, e], s_sem.at[6], d_recv.at[e], {"sp": across(d)})

    def dispatch_peer(d, k):
        i = (k - 1) * (near - 1) + d - 1
        send(
            peer_out.at[i], arr_buf.at[peer(k), d], s_sem.at[7], p_recv.at[i], {"sp": across(d)}
        )

    def get_arr(d):
        return lambda t: arr_buf.at[t, d]

    def normalise(pieces):
        full = [piece.astype(f32) for piece in pieces]
        squares = sum(jnp.sum(piece * piece, axis=1, keepdims=True) for piece in full)
        factor = lax.rsqrt(squares * (1.0 / (n_tp * col_dev)) + epsilon)
        return jnp.concatenate(
            [
                (piece * factor * norm_g[:, t * col_dev : (t + 1) * col_dev]).astype(bf16)
                for t, piece in enumerate(full)
            ],
            axis=1,
        )

    def gated(normed, gate, up):
        gate_part = jnp.dot(normed, gate[...], preferred_element_type=f32)
        up_part = jnp.dot(normed, up[...], preferred_element_type=f32)
        return (gate_part / (1.0 + jnp.exp(-gate_part)) * up_part).astype(bf16)

    def arrive(e):
        wait_recv(arr_buf.at[me_t, e], d_recv.at[e])
        gather_start(2 + e, 8, get_arr(e))

    def relay(e):
        gather_relay(2 + e, 8, get_arr(e))

    def arrive_near(d):
        wait_recv(arr_buf.at[me_t, d], d_recv.at[d])
        pass_on(2 + d, 9, arr_buf.at[me_t, d])

    def arrive_peer(d):
        for k in range(1, peers + 1):
            wait_recv(arr_buf.at[peer(k), d], p_recv.at[(k - 1) * (near - 1) + d - 1])
            pass_on(2 + d, 9, arr_buf.at[peer(k), d])

    def get_sh(t):
        return sh_buf.at[t]

    def get_eh(lo, hi):
        return lambda t: eh_buf.at[t, pl.ds(lo, hi - lo)]

    piece_sh = 2 + n_sp
    piece_eh = 3 + n_sp

    def expert_up(lo, hi):
        for d in range(lo, hi):
            if d:
                gather_finish(2 + d, get_arr(d))
        count = (hi - lo) * cap
        normed = normalise([arr_buf[t, lo:hi].reshape(count, col_dev) for t in range(n_tp)])
        hidden_units = gated(normed, t_gate, t_up)
        eh_buf[me_t, lo:hi] = hidden_units.reshape(hi - lo, cap, hidden_units.shape[1])

    def start_eh(lo, hi):
        gather_start(piece_eh + lo, 10, get_eh(lo, hi))

    def relay_eh(lo, hi):
        gather_relay(piece_eh + lo, 10, get_eh(lo, hi))

    def expert_out(lo, hi):
        gather_finish(piece_eh + lo, get_eh(lo, hi))
        count = (hi - lo) * cap
        joined = jnp.concatenate(
            [eh_buf[t, lo:hi].reshape(count, eh_buf.shape[3]) for t in range(n_tp)], axis=1
        )
        result = jnp.dot(joined, w_down[...], preferred_element_type=f32).astype(bf16)
        res_out[lo:hi] = result.reshape(hi - lo, cap, col_dev)
        for d in range(lo, hi):
            if d == 0:
                ret_buf[0] = res_out[0]
            else:
                send(
                    res_out.at[d],
                    ret_buf.at[offset_of(d)],
                    s_sem.at[11],
                    r_recv.at[0],
                    {"sp": source(d)},
                )

    def shared_up():
        normed_own = normalise([hid_buf[t] for t in range(n_tp)])
        sh_buf[me_t] = gated(normed_own, t_sgate, t_sup)

    def shared_down():
        shared_all = jnp.concatenate([sh_buf[t] for t in range(n_tp)], axis=1)
        shared_sum[...] = hid_buf[me_t].astype(f32) + jnp.dot(
            shared_all, w_sdown[...], preferred_element_type=f32
        )

    def own_rows():
        for t in range(n_tp):
            arr_buf[t, 0] = jnp.dot(
                spread_buf[0:cap], hid_buf[t], preferred_element_type=f32
            ).astype(bf16)

    def wait_loads():
        for copy in loads[5:]:
            copy.wait()

    def send_own():
        for d in (4, 6, 5, 7):
            disp_out[d : d + 1] = spread(d, d + 1, hidden)
            dispatch(d)
        disp_out[1:near] = spread(1, near, hidden)
        for d in range(1, near):
            dispatch(d)

    def peer_cols():
        for k in range(1, peers + 1):
            other = lax.rem(me_t + 2 * k, n_tp)
            peer_out[(k - 1) * (near - 1) : k * (near - 1)] = spread(1, near, hid_buf[other])
            for d in range(1, near):
                dispatch_peer(d, k)

    send_own()
    arrive(5)
    gather_relay(2, 5, get_hid)
    peer_cols()
    gather_finish(2, get_hid)
    arrive(4)
    relay(5)
    wait_loads()
    shared_up()
    expert_up(5, 6)
    start_eh(5, 6)
    own_rows()
    arrive(7)
    relay(4)
    expert_up(4, 5)
    start_eh(4, 5)
    relay_eh(5, 6)
    arrive(6)
    arrive_near(1)
    arrive_near(2)
    arrive_near(3)
    arrive_peer(1)
    expert_out(5, 6)
    arrive_peer(2)
    arrive_peer(3)
    relay(7)
    expert_up(0, 2)
    start_eh(0, 2)
    relay_eh(4, 5)
    expert_up(7, 8)
    start_eh(7, 8)
    expert_out(4, 5)
    relay(6)
    expert_up(2, 4)
    start_eh(2, 4)
    expert_up(6, 7)
    start_eh(6, 7)
    gather_start(piece_sh, 12, get_sh)
    relay_eh(0, 2)
    relay_eh(7, 8)
    expert_out(0, 2)
    expert_out(7, 8)
    relay_eh(2, 4)
    relay_eh(6, 7)
    expert_out(6, 7)
    expert_out(2, 4)
    gather_relay(piece_sh, 12, get_sh)
    gather_finish(piece_sh, get_sh)
    shared_down()
    result = shared_sum[...]
    wait_recv(ret_buf.at[0 : n_sp - 1], r_recv.at[0])
    returned = ret_buf[...].reshape(slots, col_dev)
    for c in range(2):
        picked = jnp.dot(pick_buf[c], returned, preferred_element_type=f32)
        result = result + weight_buf[c][:, 0:1] * picked
    out_ref[...] = result.astype(out_ref.dtype)

    hops = 2 * peers + 1
    for i, ref in enumerate(
        (
            kv_buf.at[0 : n_sp - 1],
            q_buf.at[0 : n_sp - 1],
            ho_buf.at[0 : peers + 1, 0 : n_sp - 1],
            ho_buf.at[0:peers, 0],
            ho_buf.at[0 : peers + 1],
            hid_buf.at[0:hops],
            disp_out.at[1:n_sp],
            peer_out,
            arr_buf.at[0:hops, near:n_sp],
            arr_buf.at[0 : peers + 1, 1:near],
            eh_buf.at[0:hops],
            ret_buf.at[1:n_sp],
            sh_buf.at[0:hops],
        )
    ):
        waiter(ref, s_sem.at[i], kv_recv.at[0]).wait_send()


def fused_body(
    residual_in,
    query_rows,
    key_rows,
    value_rows,
    map_weight,
    head_gain,
    out_proj,
    norm_gain,
    route_ids,
    route_weights,
    expert_gate,
    expert_up,
    expert_down,
    shared_gate,
    shared_up,
    shared_down,
):
    n_sp = lax.axis_size("sp")
    n_tp = lax.axis_size("tp")
    rows, col_dev = residual_in.shape
    topk = route_ids.shape[1]
    capacity = 5 * rows * topk // (4 * n_sp)
    cap = (capacity + 15) // 16 * 16
    hid_units = shared_gate.shape[0]
    bf16 = jnp.bfloat16
    peer_slots = (n_tp // 2 - 1) * (n_sp // 2 - 1)
    dma = pltpu.SemaphoreType.DMA
    vmem = pl.BlockSpec(memory_space=pltpu.VMEM)
    hbm = pl.BlockSpec(memory_space=pl.ANY)
    return pl.pallas_call(
        functools.partial(layer_kernel, n_sp, n_tp),
        out_shape=pltpu.VMEM((rows, col_dev), bf16),
        in_specs=[hbm] * 16,
        out_specs=vmem,
        scratch_shapes=[
            pltpu.VMEM(out_proj.shape, bf16),
            pltpu.VMEM(expert_gate.shape[1:], bf16),
            pltpu.VMEM(expert_up.shape[1:], bf16),
            pltpu.VMEM(expert_down.shape[1:], bf16),
            pltpu.VMEM(shared_gate.shape, bf16),
            pltpu.VMEM(shared_up.shape, bf16),
            pltpu.VMEM(shared_down.shape, bf16),
            pltpu.VMEM((n_sp // 2, rows, 128), bf16),
            pltpu.VMEM((n_sp, rows // 4, 128), bf16),
            pltpu.VMEM((n_sp, rows, 128), bf16),
            pltpu.VMEM((n_sp, rows // 4, 128), bf16),
            pltpu.VMEM((n_sp, rows // 4, 128), bf16),
            pltpu.VMEM((n_tp, n_sp, rows // 4, 128), bf16),
            pltpu.VMEM((n_tp, rows, col_dev), bf16),
            pltpu.VMEM((n_sp, cap, col_dev), bf16),
            pltpu.VMEM((n_tp, n_sp, cap, col_dev), bf16),
            pltpu.VMEM((n_tp, rows, hid_units), bf16),
            pltpu.VMEM((n_tp, n_sp, cap, hid_units), bf16),
            pltpu.VMEM((n_sp, cap, col_dev), bf16),
            pltpu.VMEM((n_sp, cap, col_dev), bf16),
            pltpu.VMEM((n_sp * cap, rows), bf16),
            pltpu.VMEM((2, rows, n_sp * cap), bf16),
            pltpu.VMEM((2, rows, 128), jnp.float32),
            dma((7,)),
            dma((13,)),
            dma((n_sp // 2,)),
            dma((1,)),
            dma((n_tp,)),
            dma((n_sp,)),
            dma((1,)),
            dma(((3 + 2 * n_sp) * (n_tp // 2),)),
            dma((peer_slots,)),
            pltpu.VMEM((peer_slots, cap, col_dev), bf16),
            pltpu.VMEM((rows, col_dev), jnp.float32),
            pltpu.VMEM(query_rows.shape, bf16),
            pltpu.VMEM(key_rows.shape, bf16),
            pltpu.VMEM(value_rows.shape, bf16),
            pltpu.VMEM(residual_in.shape, bf16),
            pltpu.VMEM((1,) + map_weight.shape, jnp.float32),
            pltpu.VMEM((1,) + head_gain.shape, jnp.float32),
            pltpu.VMEM((1,) + norm_gain.shape, jnp.float32),
            pltpu.VMEM((topk, rows), jnp.int32),
            pltpu.VMEM((topk, rows), jnp.float32),
            dma((7,)),
            pltpu.VMEM(expert_gate.shape[:0:-1], bf16),
            pltpu.VMEM(expert_up.shape[:0:-1], bf16),
            pltpu.VMEM(shared_gate.shape[::-1], bf16),
            pltpu.VMEM(shared_up.shape[::-1], bf16),
        ],
        compiler_params=pltpu.CompilerParams(collective_id=0, has_side_effects=True),
    )(
        query_rows,
        key_rows,
        value_rows,
        residual_in,
        map_weight[None, :],
        head_gain[None, :],
        norm_gain[None, :],
        route_ids.T,
        route_weights.T,
        out_proj,
        expert_gate,
        expert_up,
        expert_down,
        shared_gate,
        shared_up,
        shared_down,
    )


def layer(*args):
    residual_in, map_weight, head_gain, route_ids = args[0], args[4], args[5], args[8]
    fits = (
        2 * map_weight.shape[0] == lax.axis_size("sp") == 8
        and map_weight.shape[0] % 2 == 0
        and head_gain.shape[0] == 64
        and route_ids.shape[1] == 2
        and args[10].shape[0] == 1
        and residual_in.shape[0] % 64 == 0
        and residual_in.shape[1] % 128 == 0
        and args[13].shape[0] % 128 == 0
        and lax.axis_size("tp") in (4, 8)
    )
    return (fused_body if fits else body)(*args)


def solution(mesh):
    in_specs = (
        P("sp", "tp"),
        P("sp", "tp"),
        P("sp", "tp"),
        P("sp", "tp"),
        P("tp"),
        P(),
        P(None, "tp"),
        P(),
        P("sp", None),
        P("sp", None),
        P("sp", "tp", None),
        P("sp", "tp", None),
        P("sp", None, "tp"),
        P("tp", None),
        P("tp", None),
        P(None, "tp"),
    )
    out_specs = P("sp", "tp")
    return jax.shard_map(layer, mesh=mesh, in_specs=in_specs, out_specs=out_specs, check_vma=False)
```

```python
import functools

import jax
import jax.numpy as jnp
from jax import lax
from jax.experimental import pallas as pl
from jax.experimental.pallas import tpu as pltpu
from jax.sharding import PartitionSpec as P

epsilon = 1e-06
masked_score = -1e30
log2_e = 1.4426950408889634
MESH = pl.DeviceIdType.MESH


def rms_scale(values, gain_vec):
    squares = jnp.mean(values * values, axis=-1, keepdims=True)
    return values * lax.rsqrt(squares + epsilon) * gain_vec


def block_slots(route_block, experts_all, capacity):
    flat_ids = route_block.reshape(-1)
    one_hot = (flat_ids[:, None] == jnp.arange(experts_all, dtype=jnp.int32)[None, :]).astype(
        jnp.int32
    )
    earlier = jnp.cumsum(one_hot, axis=0) - one_hot
    position = jnp.sum(earlier * one_hot, axis=1)
    return (flat_ids * capacity + position).reshape(route_block.shape)


def body(
    residual_in,
    query_rows,
    key_rows,
    value_rows,
    map_weight,
    head_gain,
    out_proj,
    norm_gain,
    route_ids,
    route_weights,
    expert_gate,
    expert_up,
    expert_down,
    shared_gate,
    shared_up,
    shared_down,
):
    seq_dev = residual_in.shape[0]
    col_dev = residual_in.shape[1]
    heads_here = map_weight.shape[0]
    head_dim = head_gain.shape[0]
    half_dim = head_dim // 2
    topk_count = route_ids.shape[1]
    exp_here = expert_gate.shape[0]
    experts_all = exp_here * lax.axis_size("sp")
    capacity = 5 * seq_dev * topk_count // (4 * experts_all)
    score_scale = half_dim ** (-0.5)
    query_pos = lax.axis_index("sp") * seq_dev + jnp.arange(seq_dev, dtype=jnp.int32)
    query_heads = query_rows.reshape(seq_dev, heads_here, 2, half_dim)
    key_piece = lax.all_gather(key_rows, "sp", axis=0, tiled=True)
    value_piece = lax.all_gather(value_rows, "sp", axis=0, tiled=True)
    piece_len = key_piece.shape[0]
    key_heads = key_piece.reshape(piece_len, heads_here, 2, half_dim)
    value_heads = value_piece.reshape(piece_len, heads_here, head_dim)
    scores = (
        jnp.einsum("qhmd,khmd->mhqk", query_heads, key_heads, preferred_element_type=jnp.float32)
        * score_scale
    )
    key_pos = jnp.arange(piece_len, dtype=jnp.int32)
    visible = key_pos[None, :] <= query_pos[:, None]
    scores = jnp.where(visible, scores, masked_score)
    run_max = jnp.full((2, heads_here, seq_dev), masked_score, jnp.float32)
    new_max = jnp.maximum(run_max, jnp.max(scores, axis=-1))
    expo = jnp.where(visible, jnp.exp(scores - new_max[..., None]), 0.0)
    new_sum = jnp.sum(expo, axis=-1)
    product = jnp.einsum(
        "mhqk,khd->mhqd", expo.astype(jnp.bfloat16), value_heads, preferred_element_type=jnp.float32
    )
    summed = product / new_sum[..., None]
    diff_out = summed[0] - map_weight[:, None, None] * summed[1]
    head_out = rms_scale(diff_out, head_gain).astype(jnp.bfloat16)
    head_out = jnp.transpose(head_out, (1, 0, 2)).reshape(seq_dev, heads_here * head_dim)
    attn = jnp.dot(
        lax.all_gather(head_out, "tp", axis=1, tiled=True),
        out_proj,
        preferred_element_type=jnp.float32,
    )
    hidden_state = (residual_in.astype(jnp.float32) + attn).astype(jnp.bfloat16)
    full_rows = lax.all_gather(hidden_state, "tp", axis=1, tiled=True)
    normed = rms_scale(full_rows.astype(jnp.float32), norm_gain).astype(jnp.bfloat16)
    shared_gate_part = jnp.einsum(
        "rd,fd->rf", normed, shared_gate, preferred_element_type=jnp.float32
    )
    shared_up_part = jnp.einsum("rd,fd->rf", normed, shared_up, preferred_element_type=jnp.float32)
    shared_hidden = (jax.nn.silu(shared_gate_part) * shared_up_part).astype(jnp.bfloat16)
    slot_ids = block_slots(route_ids, experts_all, capacity)
    token_of = jnp.repeat(jnp.arange(seq_dev, dtype=jnp.int32), topk_count)
    slot_token = (
        jnp.full((experts_all * capacity,), seq_dev, jnp.int32)
        .at[slot_ids.reshape(-1)]
        .set(token_of)
    )
    own_cols = lax.dynamic_slice_in_dim(normed, lax.axis_index("tp") * col_dev, col_dev, 1)
    padded = jnp.concatenate([own_cols, jnp.zeros((1, col_dev), jnp.bfloat16)], axis=0)
    outgoing = jnp.take(padded, slot_token, axis=0).reshape(experts_all, capacity, col_dev)
    arrived = lax.all_to_all(outgoing, "sp", split_axis=0, concat_axis=1, tiled=True)
    arrived_rows = arrived.shape[1]
    pieces = lax.all_gather(arrived, "tp", axis=2, tiled=True)
    gate_add = jnp.einsum("erd,efd->erf", pieces, expert_gate, preferred_element_type=jnp.float32)
    up_add = jnp.einsum("erd,efd->erf", pieces, expert_up, preferred_element_type=jnp.float32)
    expert_hidden = (jax.nn.silu(gate_add) * up_add).astype(jnp.bfloat16)
    expert_flat = expert_hidden.reshape(exp_here * arrived_rows, expert_hidden.shape[2])
    pieces = (
        lax.all_gather(shared_hidden, "tp", axis=1, tiled=True),
        lax.all_gather(expert_flat, "tp", axis=1, tiled=True),
    )
    piece_width = pieces[0].shape[1]
    routed_piece = pieces[1].reshape(exp_here, arrived_rows, piece_width)
    shared_add = jnp.dot(pieces[0], shared_down, preferred_element_type=jnp.float32)
    expert_add = jnp.einsum(
        "erf,efd->erd", routed_piece, expert_down, preferred_element_type=jnp.float32
    )
    returned_rows = lax.all_to_all(
        expert_add.astype(jnp.bfloat16), "sp", split_axis=1, concat_axis=0, tiled=True
    )
    returned_flat = returned_rows.reshape(experts_all * capacity, col_dev)
    picked = (
        jnp.take(returned_flat, slot_ids.reshape(-1), axis=0)
        .reshape(seq_dev, topk_count, col_dev)
        .astype(jnp.float32)
    )
    routed = jnp.sum(picked * route_weights[:, :, None], axis=1)
    return (hidden_state.astype(jnp.float32) + shared_add + routed).astype(jnp.bfloat16)


def lane_iota(rows):
    return lax.broadcasted_iota(jnp.int32, (rows, 128), 1)


def roll_half(values):
    return pltpu.roll(values, 64, 1)


def contract_last(a, b):
    return lax.dot_general(a, b, (((1,), (1,)), ((), ())), preferred_element_type=jnp.float32)


def layer_kernel(
    n_sp,
    n_tp,
    q_hbm,
    k_hbm,
    v_hbm,
    res_hbm,
    map_w_hbm,
    head_g_hbm,
    norm_g_hbm,
    ids_hbm,
    route_w_hbm,
    out_proj,
    exp_gate,
    exp_up,
    exp_down,
    sh_gate,
    sh_up,
    sh_down,
    out_ref,
    w_out,
    w_gate,
    w_up,
    w_down,
    w_sgate,
    w_sup,
    w_sdown,
    kv_out,
    q_out,
    kv_buf,
    q_buf,
    o_out,
    ho_buf,
    hid_buf,
    disp_out,
    arr_buf,
    sh_buf,
    eh_buf,
    res_out,
    ret_buf,
    spread_buf,
    pick_buf,
    weight_buf,
    w_sem,
    s_sem,
    kv_recv,
    q_recv,
    o_recv,
    d_recv,
    r_recv,
    g_recv,
    p_recv,
    peer_out,
    shared_sum,
    q_in,
    k_in,
    v_in,
    res_in,
    map_w,
    head_g,
    norm_g,
    ids_in,
    route_w,
    in_sem,
    t_gate,
    t_up,
    t_sgate,
    t_sup,
):
    me_s = lax.axis_index("sp")
    me_t = lax.axis_index("tp")
    sib = me_t + 1 - 2 * lax.rem(me_t, 2)
    peers = n_tp // 2 - 1
    rows = res_in.shape[0]
    col_dev = res_in.shape[1]
    half = rows // 2
    quarter = rows // 4
    cap = arr_buf.shape[2]
    half_dim = 32
    bf16 = jnp.bfloat16
    f32 = jnp.float32

    def across(k):
        other = me_s
        for b in range(n_sp.bit_length() - 1):
            if k >> b & 1:
                bit = lax.rem(me_s // (1 << b), 2)
                other = other + (1 << b) * (1 - 2 * bit)
        return other

    barrier = pltpu.get_barrier_semaphore()
    for d in range(1, n_sp):
        pl.semaphore_signal(
            barrier, inc=1, device_id={"sp": lax.rem(me_s + d, n_sp)}, device_id_type=MESH
        )
    for d in range(1, n_tp):
        pl.semaphore_signal(
            barrier, inc=1, device_id={"tp": lax.rem(me_t + d, n_tp)}, device_id_type=MESH
        )

    inputs = []
    for i, (src, dst) in enumerate(
        (
            (q_hbm, q_in),
            (k_hbm, k_in),
            (v_hbm, v_in),
            (res_hbm, res_in),
            (map_w_hbm, map_w),
            (head_g_hbm, head_g),
            (norm_g_hbm, norm_g),
            (ids_hbm, ids_in),
            (route_w_hbm, route_w),
        )
    ):
        copy = pltpu.make_async_copy(src, dst, in_sem.at[max(0, i - 2)])
        copy.start()
        inputs.append(copy)

    loads = []
    for i, (src, dst) in enumerate(
        (
            (out_proj, w_out),
            (sh_gate, w_sgate),
            (sh_up, w_sup),
            (exp_gate.at[0], w_gate),
            (exp_up.at[0], w_up),
            (exp_down.at[0], w_down),
            (sh_down, w_sdown),
        )
    ):
        copy = pltpu.make_async_copy(src, dst, w_sem.at[i])
        copy.start()
        loads.append(copy)

    def send(src, dst, ssem, rsem, device):
        pltpu.make_async_remote_copy(
            src_ref=src,
            dst_ref=dst,
            send_sem=ssem,
            recv_sem=rsem,
            device_id=device,
            device_id_type=MESH,
        ).start()

    def waiter(ref, ssem, rsem):
        return pltpu.make_async_remote_copy(
            src_ref=ref,
            dst_ref=ref,
            send_sem=ssem,
            recv_sem=rsem,
            device_id={"tp": sib},
            device_id_type=MESH,
        )

    def wait_recv(ref, rsem):
        waiter(ref, s_sem.at[0], rsem).wait_recv()

    def peer(k):
        return lax.rem(me_t + 2 * k, n_tp)

    def origin(k):
        return lax.rem(me_t - 2 * k + n_tp, n_tp)

    def channel(i, k):
        return g_recv.at[i * (peers + 1) + k]

    def pass_on(i, kind, block):
        send(block, block, s_sem.at[kind], channel(i, 0), {"tp": sib})

    def gather_start(i, kind, get):
        for k in range(1, peers + 1):
            send(get(me_t), get(me_t), s_sem.at[kind], channel(i, k), {"tp": peer(k)})
        pass_on(i, kind, get(me_t))

    def gather_relay(i, kind, get):
        for k in range(1, peers + 1):
            wait_recv(get(origin(k)), channel(i, k))
            pass_on(i, kind, get(origin(k)))

    def gather_finish(i, get):
        wait_recv(get(pl.ds(0, peers + 1)), channel(i, 0))

    pltpu.make_async_copy(kv_buf.at[0:6], kv_buf.at[0:6], in_sem.at[0]).wait()
    low_rows = lane_iota(rows) < 64
    low_quarter = lane_iota(quarter) < 64
    for j in range(n_sp // 4):
        pair = slice(j * 128, (j + 1) * 128)
        keys = k_in[:, pair].astype(f32)
        vals = v_in[:, pair].astype(f32)
        kv_out[2 * j] = jnp.where(low_rows, keys, roll_half(vals)).astype(bf16)
        kv_out[2 * j + 1] = jnp.where(low_rows, roll_half(keys), vals).astype(bf16)
        for p in range(2):
            first = q_in[p * half : p * half + quarter, pair].astype(f32)
            second = q_in[p * half + quarter : (p + 1) * half, pair].astype(f32)
            q_out[4 * j + p] = jnp.where(low_quarter, first, roll_half(second)).astype(bf16)
            q_out[4 * j + 2 + p] = jnp.where(low_quarter, roll_half(first), second).astype(bf16)

    pl.semaphore_wait(barrier, n_sp + n_tp - 2)

    for d in (6, 4, 2, 3, 1):
        dst = across(d)
        part = kv_recv.at[0 if d % 2 else d // 2]
        send(kv_out.at[dst // 2], kv_buf.at[me_s], s_sem.at[0], part, {"sp": dst})

    def send_queries(ds):
        for d in ds:
            dst = across(d)
            send(q_out.at[dst], q_buf.at[me_s], s_sem.at[1], q_recv.at[d // 4], {"sp": dst})

    upper = me_s // (n_sp // 2)
    inner = lax.rem(me_s // 2 + upper, 2)
    send_queries((2, 3, 1))
    kv_buf[me_s] = kv_out[me_s // 2]
    q_buf[me_s] = q_out[me_s]
    for copy in inputs[3:]:
        copy.wait()
    eye = lax.broadcasted_iota(jnp.int32, (rows, rows), 0)
    eye_lane = lax.broadcasted_iota(jnp.int32, (rows, rows), 1)
    same = eye == eye_lane
    before_col = eye_lane < eye
    before_row = eye < eye_lane

    def as_column(row):
        return jnp.sum(jnp.where(same, row, 0.0), axis=1, keepdims=True)

    ids_row = [jnp.bitwise_xor(ids_in[c : c + 1, :], me_s).astype(f32) for c in range(2)]
    ids_col = [as_column(row) for row in ids_row]
    weight_col = [as_column(route_w[c : c + 1, :]) for c in range(2)]
    slot_row = []
    slot_col = []
    for c in range(2):
        hit = (ids_row[0] == ids_col[c]) | (ids_row[1] == ids_col[c])
        count = jnp.sum(jnp.where(hit & before_col, 1.0, 0.0), axis=1, keepdims=True)
        slot_col.append(ids_col[c] * cap + count)
        hit = (ids_col[0] == ids_row[c]) | (ids_col[1] == ids_row[c])
        count = jnp.sum(jnp.where(hit & before_row, 1.0, 0.0), axis=0, keepdims=True)
        slot_row.append(ids_row[c] * cap + count)
    slots = n_sp * cap
    slot_iota = lax.broadcasted_iota(jnp.int32, (slots, rows), 0).astype(f32)
    chosen = (slot_iota == slot_row[0]) | (slot_iota == slot_row[1])
    spread_buf[...] = jnp.where(chosen, 1.0, 0.0).astype(bf16)
    col_iota = lax.broadcasted_iota(jnp.int32, (rows, slots), 1).astype(f32)
    for c in range(2):
        pick_buf[c] = jnp.where(col_iota == slot_col[c], 1.0, 0.0).astype(bf16)
        weight_buf[c] = jnp.broadcast_to(weight_col[c], (rows, 128))
    head_lane = lax.broadcasted_iota(jnp.int32, map_w.shape, 1)
    map_here = jnp.sum(
        jnp.where(head_lane == me_s // 2, map_w[...], 0.0), axis=1, keepdims=True
    )
    gain_here = jnp.concatenate([jnp.zeros((1, 64), f32), head_g[...]], axis=1)

    parity = lax.rem(me_s, 2)
    lane_q = lane_iota(quarter)
    scale = half_dim ** (-0.5) * log2_e
    ones_lane = lane_iota(rows) == 0
    one = jnp.ones((rows, 128), bf16)
    row_in = lax.broadcasted_iota(jnp.int32, (half, rows), 0) + parity * half
    visible_half = lax.broadcasted_iota(jnp.int32, (half, rows), 1) <= row_in
    visible = jnp.concatenate([visible_half.astype(f32)] * 2, axis=0) > 0.5
    high_lanes = lane_iota(half) >= 64
    zero_q = jnp.zeros((quarter, 128), f32)
    first_map = lane_q < 32
    second_map = (lane_q >= 32) & (lane_q < 64)
    batch = n_sp // 2
    for d in (6, 4, 2):
        src = across(d)
        wait_recv(kv_buf.at[src], kv_recv.at[d // 2])
        if d > 2:
            send(kv_buf.at[src], kv_buf.at[src], s_sem.at[0], kv_recv.at[4], {"sp": across(1)})
        if d == 6:
            send_queries((6, 7, 4, 5))
    for i, (src, dst) in ((3, (w_gate, t_gate)), (4, (w_up, t_up))):
        loads[i].wait()
        dst[...] = src[...].T
    wait_recv(kv_buf.at[0:2], kv_recv.at[0])
    wait_recv(q_buf.at[0:3], q_recv.at[0])
    def send_rows(s, k):
        far = lax.rem(s // batch + upper, 2)
        send(
            o_out.at[s],
            ho_buf.at[me_t, me_s],
            s_sem.at[2],
            o_recv.at[2 * k + far],
            {"sp": s, "tp": peer(k)},
        )

    def attend(start):
        steps = range(start, start + batch)
        queries = {}
        for s in steps:
            packed = q_buf[s].astype(f32)
            rolled = roll_half(packed)
            queries[s] = jnp.concatenate(
                [
                    jnp.where(first_map, packed, zero_q),
                    jnp.where(first_map, rolled, zero_q),
                    jnp.where(second_map, packed, zero_q),
                    jnp.where(second_map, rolled, zero_q),
                ],
                axis=0,
            ).astype(bf16)
        keys = {s: kv_buf[0 : s + 1].reshape((s + 1) * rows, 128) for s in steps}
        blocks = [jnp.where(ones_lane, one, kv_buf[s]) for s in range(start + batch)]
        values = {s: jnp.concatenate(blocks[: s + 1], axis=0) for s in steps}
        scores = {}
        for s in steps:
            raw = contract_last(queries[s], keys[s])
            diag = jnp.where(visible, raw[:, s * rows :], masked_score)
            scores[s] = jnp.concatenate([raw[:, : s * rows], diag], axis=1) if s else diag
        row_max = {s: jnp.max(scores[s], axis=1, keepdims=True) for s in steps}
        expo = {s: jnp.exp2(scores[s] * scale - row_max[s] * scale).astype(bf16) for s in steps}
        acc = {s: jnp.dot(expo[s], values[s], preferred_element_type=f32) for s in steps}
        diff = {}
        for s in steps:
            summed = acc[s] / acc[s][:, 0:1]
            raw = summed[0:half] - map_here * summed[half:rows]
            diff[s] = jnp.where(high_lanes, raw, 0.0)
        for s in steps:
            squares = jnp.sum(diff[s] * diff[s], axis=1, keepdims=True) * (1.0 / 64.0)
            head = diff[s] * lax.rsqrt(squares + epsilon) * gain_here
            o_out[s] = (roll_half(head[0:quarter]) + head[quarter:half]).astype(bf16)

        for s in steps:

            @pl.when(me_s != s)
            def _():
                for k in range(peers + 1):
                    send_rows(s, k)

            @pl.when(me_s == s)
            def _():
                ho_buf[me_t, s] = o_out[s]


    def wait_far():
        wait_recv(kv_buf.at[0:2], kv_recv.at[4])
        wait_recv(q_buf.at[0:4], q_recv.at[1])

    @pl.when(upper == 1)
    def _():
        wait_far()
        attend(0)
        attend(batch)

    @pl.when(upper == 0)
    def _():
        attend(0)
        wait_far()
        attend(batch)

    split = n_sp // 2
    base = me_s // split * split

    def get_near(t):
        return ho_buf.at[t, pl.ds(base, split)]

    def get_far(t):
        return ho_buf.at[t, pl.ds(split - base, split)]

    for i, (src, dst) in ((1, (w_sgate, t_sgate)), (2, (w_sup, t_sup))):
        loads[i].wait()
        dst[...] = src[...].T
    for k in range(1, peers + 1):
        block = ho_buf.at[me_t, me_s]
        send(block, block, s_sem.at[3], o_recv.at[2 * k], {"tp": peer(k)})

    for k in range(peers + 1):
        wait_recv(get_far(origin(k)), o_recv.at[2 * k + 1])
        pass_on(0, 4, get_far(origin(k)))
    for k in range(peers + 1):
        wait_recv(ho_buf.at[origin(k), 0 : split - (k == 0)], o_recv.at[2 * k])
        pass_on(1, 4, get_near(origin(k)))
    def project(j):
        blocks = []
        for p in range(2):
            for u in range(2):
                parts = []
                for t in range(n_tp):
                    even = ho_buf[t, 4 * j + p].astype(f32)
                    odd = ho_buf[t, 4 * j + 2 + p].astype(f32)
                    if u == 0:
                        part = jnp.where(low_quarter, even, roll_half(odd))
                    else:
                        part = jnp.where(low_quarter, roll_half(even), odd)
                    parts.append(part.astype(bf16))
                blocks.append(jnp.concatenate(parts, axis=1))
        heads = jnp.concatenate(blocks, axis=0)
        wide = n_sp // 4 * 128
        weights = jnp.concatenate(
            [w_out[pl.ds(pl.multiple_of(t * wide + j * 128, 128), 128), :] for t in range(n_tp)],
            axis=0,
        )
        return jnp.dot(heads, weights, preferred_element_type=f32)

    loads[0].wait()
    gather_finish(0, get_far)
    attn = project(1 - upper)
    gather_finish(1, get_near)
    attn = attn + project(upper)
    hidden = (res_in[...].astype(f32) + attn).astype(bf16)
    hid_buf[me_t] = hidden

    def get_hid(t):
        return hid_buf.at[t]

    gather_start(2, 5, get_hid)

    near = n_sp // 2

    def spread(lo, hi, cols):
        picked = jnp.dot(spread_buf[lo * cap : hi * cap], cols, preferred_element_type=f32)
        return picked.astype(bf16).reshape(hi - lo, cap, col_dev)

    def slot_at(d):
        return d if d < near else near + 2 * inner + 1 - d % 2

    def offset_of(e):
        if e < near:
            return e
        return (6 - 2 * inner if e < 6 else 4 + 2 * inner) + 1 - e % 2

    def source(e):
        if e < near:
            return across(e)
        side = me_s % 2 if e % 2 else 1 - me_s % 2
        return 2 * (3 * (1 - upper) if e < 6 else 2 - upper) + side

    def dispatch(d):
        e = slot_at(d)
        send(disp_out.at[d], arr_buf.at[me_t, e], s_sem.at[6], d_recv.at[e], {"sp": across(d)})

    def dispatch_peer(d, k):
        i = (k - 1) * (near - 1) + d - 1
        send(
            peer_out.at[i], arr_buf.at[peer(k), d], s_sem.at[7], p_recv.at[i], {"sp": across(d)}
        )

    def get_arr(d):
        return lambda t: arr_buf.at[t, d]

    def normalise(pieces):
        full = [piece.astype(f32) for piece in pieces]
        squares = sum(jnp.sum(piece * piece, axis=1, keepdims=True) for piece in full)
        factor = lax.rsqrt(squares * (1.0 / (n_tp * col_dev)) + epsilon)
        return jnp.concatenate(
            [
                (piece * factor * norm_g[:, t * col_dev : (t + 1) * col_dev]).astype(bf16)
                for t, piece in enumerate(full)
            ],
            axis=1,
        )

    def gated(normed, gate, up):
        gate_part = jnp.dot(normed, gate[...], preferred_element_type=f32)
        up_part = jnp.dot(normed, up[...], preferred_element_type=f32)
        return (gate_part / (1.0 + jnp.exp(-gate_part)) * up_part).astype(bf16)

    def arrive(e):
        wait_recv(arr_buf.at[me_t, e], d_recv.at[e])
        gather_start(2 + e, 8, get_arr(e))

    def relay(e):
        gather_relay(2 + e, 8, get_arr(e))

    def arrive_near(d):
        wait_recv(arr_buf.at[me_t, d], d_recv.at[d])
        pass_on(2 + d, 9, arr_buf.at[me_t, d])

    def arrive_peer(d):
        for k in range(1, peers + 1):
            wait_recv(arr_buf.at[peer(k), d], p_recv.at[(k - 1) * (near - 1) + d - 1])
            pass_on(2 + d, 9, arr_buf.at[peer(k), d])

    def get_sh(t):
        return sh_buf.at[t]

    def get_eh(lo, hi):
        return lambda t: eh_buf.at[t, pl.ds(lo, hi - lo)]

    piece_sh = 2 + n_sp
    piece_eh = 3 + n_sp

    def expert_up(lo, hi):
        for d in range(lo, hi):
            if d:
                gather_finish(2 + d, get_arr(d))
        count = (hi - lo) * cap
        normed = normalise([arr_buf[t, lo:hi].reshape(count, col_dev) for t in range(n_tp)])
        hidden_units = gated(normed, t_gate, t_up)
        eh_buf[me_t, lo:hi] = hidden_units.reshape(hi - lo, cap, hidden_units.shape[1])

    def start_eh(lo, hi):
        gather_start(piece_eh + lo, 10, get_eh(lo, hi))

    def relay_eh(lo, hi):
        gather_relay(piece_eh + lo, 10, get_eh(lo, hi))

    def expert_out(lo, hi):
        gather_finish(piece_eh + lo, get_eh(lo, hi))
        count = (hi - lo) * cap
        joined = jnp.concatenate(
            [eh_buf[t, lo:hi].reshape(count, eh_buf.shape[3]) for t in range(n_tp)], axis=1
        )
        result = jnp.dot(joined, w_down[...], preferred_element_type=f32).astype(bf16)
        res_out[lo:hi] = result.reshape(hi - lo, cap, col_dev)
        for d in range(lo, hi):
            if d == 0:
                ret_buf[0] = res_out[0]
            else:
                send(
                    res_out.at[d],
                    ret_buf.at[offset_of(d)],
                    s_sem.at[11],
                    r_recv.at[0],
                    {"sp": source(d)},
                )

    def shared_up():
        normed_own = normalise([hid_buf[t] for t in range(n_tp)])
        sh_buf[me_t] = gated(normed_own, t_sgate, t_sup)

    def shared_down():
        shared_all = jnp.concatenate([sh_buf[t] for t in range(n_tp)], axis=1)
        shared_sum[...] = hid_buf[me_t].astype(f32) + jnp.dot(
            shared_all, w_sdown[...], preferred_element_type=f32
        )

    def own_rows():
        for t in range(n_tp):
            arr_buf[t, 0] = jnp.dot(
                spread_buf[0:cap], hid_buf[t], preferred_element_type=f32
            ).astype(bf16)

    def wait_loads():
        for copy in loads[5:]:
            copy.wait()

    def send_own():
        for d in (4, 6, 5, 7):
            disp_out[d : d + 1] = spread(d, d + 1, hidden)
            dispatch(d)
        disp_out[1:near] = spread(1, near, hidden)
        for d in range(1, near):
            dispatch(d)

    def peer_cols():
        for k in range(1, peers + 1):
            other = lax.rem(me_t + 2 * k, n_tp)
            peer_out[(k - 1) * (near - 1) : k * (near - 1)] = spread(1, near, hid_buf[other])
            for d in range(1, near):
                dispatch_peer(d, k)

    send_own()
    arrive(5)
    gather_relay(2, 5, get_hid)
    peer_cols()
    gather_finish(2, get_hid)
    arrive(4)
    relay(5)
    wait_loads()
    shared_up()
    expert_up(5, 6)
    start_eh(5, 6)
    own_rows()
    arrive(7)
    relay(4)
    expert_up(4, 5)
    start_eh(4, 5)
    relay_eh(5, 6)
    arrive(6)
    arrive_near(1)
    arrive_near(2)
    arrive_near(3)
    arrive_peer(1)
    expert_out(5, 6)
    arrive_peer(2)
    arrive_peer(3)
    relay(7)
    expert_up(0, 2)
    start_eh(0, 2)
    relay_eh(4, 5)
    expert_up(7, 8)
    start_eh(7, 8)
    expert_out(4, 5)
    relay(6)
    expert_up(2, 4)
    start_eh(2, 4)
    expert_up(6, 7)
    start_eh(6, 7)
    gather_start(piece_sh, 12, get_sh)
    relay_eh(0, 2)
    relay_eh(7, 8)
    expert_out(0, 2)
    expert_out(7, 8)
    relay_eh(2, 4)
    relay_eh(6, 7)
    expert_out(2, 4)
    expert_out(6, 7)
    gather_relay(piece_sh, 12, get_sh)
    gather_finish(piece_sh, get_sh)
    shared_down()
    result = shared_sum[...]
    wait_recv(ret_buf.at[0 : n_sp - 1], r_recv.at[0])
    returned = ret_buf[...].reshape(slots, col_dev)
    for c in range(2):
        picked = jnp.dot(pick_buf[c], returned, preferred_element_type=f32)
        result = result + weight_buf[c][:, 0:1] * picked
    out_ref[...] = result.astype(out_ref.dtype)

    hops = 2 * peers + 1
    for i, ref in enumerate(
        (
            kv_buf.at[0 : n_sp - 1],
            q_buf.at[0 : n_sp - 1],
            ho_buf.at[0 : peers + 1, 0 : n_sp - 1],
            ho_buf.at[0:peers, 0],
            ho_buf.at[0 : peers + 1],
            hid_buf.at[0:hops],
            disp_out.at[1:n_sp],
            peer_out,
            arr_buf.at[0:hops, near:n_sp],
            arr_buf.at[0 : peers + 1, 1:near],
            eh_buf.at[0:hops],
            ret_buf.at[1:n_sp],
            sh_buf.at[0:hops],
        )
    ):
        waiter(ref, s_sem.at[i], kv_recv.at[0]).wait_send()


def fused_body(
    residual_in,
    query_rows,
    key_rows,
    value_rows,
    map_weight,
    head_gain,
    out_proj,
    norm_gain,
    route_ids,
    route_weights,
    expert_gate,
    expert_up,
    expert_down,
    shared_gate,
    shared_up,
    shared_down,
):
    n_sp = lax.axis_size("sp")
    n_tp = lax.axis_size("tp")
    rows, col_dev = residual_in.shape
    topk = route_ids.shape[1]
    capacity = 5 * rows * topk // (4 * n_sp)
    cap = (capacity + 15) // 16 * 16
    hid_units = shared_gate.shape[0]
    bf16 = jnp.bfloat16
    peer_slots = (n_tp // 2 - 1) * (n_sp // 2 - 1)
    dma = pltpu.SemaphoreType.DMA
    vmem = pl.BlockSpec(memory_space=pltpu.VMEM)
    hbm = pl.BlockSpec(memory_space=pl.ANY)
    return pl.pallas_call(
        functools.partial(layer_kernel, n_sp, n_tp),
        out_shape=pltpu.VMEM((rows, col_dev), bf16),
        in_specs=[hbm] * 16,
        out_specs=vmem,
        scratch_shapes=[
            pltpu.VMEM(out_proj.shape, bf16),
            pltpu.VMEM(expert_gate.shape[1:], bf16),
            pltpu.VMEM(expert_up.shape[1:], bf16),
            pltpu.VMEM(expert_down.shape[1:], bf16),
            pltpu.VMEM(shared_gate.shape, bf16),
            pltpu.VMEM(shared_up.shape, bf16),
            pltpu.VMEM(shared_down.shape, bf16),
            pltpu.VMEM((n_sp // 2, rows, 128), bf16),
            pltpu.VMEM((n_sp, rows // 4, 128), bf16),
            pltpu.VMEM((n_sp, rows, 128), bf16),
            pltpu.VMEM((n_sp, rows // 4, 128), bf16),
            pltpu.VMEM((n_sp, rows // 4, 128), bf16),
            pltpu.VMEM((n_tp, n_sp, rows // 4, 128), bf16),
            pltpu.VMEM((n_tp, rows, col_dev), bf16),
            pltpu.VMEM((n_sp, cap, col_dev), bf16),
            pltpu.VMEM((n_tp, n_sp, cap, col_dev), bf16),
            pltpu.VMEM((n_tp, rows, hid_units), bf16),
            pltpu.VMEM((n_tp, n_sp, cap, hid_units), bf16),
            pltpu.VMEM((n_sp, cap, col_dev), bf16),
            pltpu.VMEM((n_sp, cap, col_dev), bf16),
            pltpu.VMEM((n_sp * cap, rows), bf16),
            pltpu.VMEM((2, rows, n_sp * cap), bf16),
            pltpu.VMEM((2, rows, 128), jnp.float32),
            dma((7,)),
            dma((13,)),
            dma((n_sp // 2 + 1,)),
            dma((2,)),
            dma((n_tp,)),
            dma((n_sp,)),
            dma((1,)),
            dma(((3 + 2 * n_sp) * (n_tp // 2),)),
            dma((peer_slots,)),
            pltpu.VMEM((peer_slots, cap, col_dev), bf16),
            pltpu.VMEM((rows, col_dev), jnp.float32),
            pltpu.VMEM(query_rows.shape, bf16),
            pltpu.VMEM(key_rows.shape, bf16),
            pltpu.VMEM(value_rows.shape, bf16),
            pltpu.VMEM(residual_in.shape, bf16),
            pltpu.VMEM((1,) + map_weight.shape, jnp.float32),
            pltpu.VMEM((1,) + head_gain.shape, jnp.float32),
            pltpu.VMEM((1,) + norm_gain.shape, jnp.float32),
            pltpu.VMEM((topk, rows), jnp.int32),
            pltpu.VMEM((topk, rows), jnp.float32),
            dma((7,)),
            pltpu.VMEM(expert_gate.shape[:0:-1], bf16),
            pltpu.VMEM(expert_up.shape[:0:-1], bf16),
            pltpu.VMEM(shared_gate.shape[::-1], bf16),
            pltpu.VMEM(shared_up.shape[::-1], bf16),
        ],
        compiler_params=pltpu.CompilerParams(collective_id=0, has_side_effects=True),
    )(
        query_rows,
        key_rows,
        value_rows,
        residual_in,
        map_weight[None, :],
        head_gain[None, :],
        norm_gain[None, :],
        route_ids.T,
        route_weights.T,
        out_proj,
        expert_gate,
        expert_up,
        expert_down,
        shared_gate,
        shared_up,
        shared_down,
    )


def layer(*args):
    residual_in, map_weight, head_gain, route_ids = args[0], args[4], args[5], args[8]
    fits = (
        2 * map_weight.shape[0] == lax.axis_size("sp") == 8
        and map_weight.shape[0] % 2 == 0
        and head_gain.shape[0] == 64
        and route_ids.shape[1] == 2
        and args[10].shape[0] == 1
        and residual_in.shape[0] % 64 == 0
        and residual_in.shape[1] % 128 == 0
        and args[13].shape[0] % 128 == 0
        and lax.axis_size("tp") in (4, 8)
    )
    return (fused_body if fits else body)(*args)


def solution(mesh):
    in_specs = (
        P("sp", "tp"),
        P("sp", "tp"),
        P("sp", "tp"),
        P("sp", "tp"),
        P("tp"),
        P(),
        P(None, "tp"),
        P(),
        P("sp", None),
        P("sp", None),
        P("sp", "tp", None),
        P("sp", "tp", None),
        P("sp", None, "tp"),
        P("tp", None),
        P("tp", None),
        P(None, "tp"),
    )
    out_specs = P("sp", "tp")
    return jax.shard_map(layer, mesh=mesh, in_specs=in_specs, out_specs=out_specs, check_vma=False)
```
